256 devices in a mesh: ep: 64 (over z, y, core), tp: 4 (over x).
Axes of the slice: x: 4, y: 4, z: 8, core: 2. Of those that a mesh axis runs over, the one named last changes fastest.
Arguments:
- resid: bfloat16 [2048, 2048], P('ep'), may hold values from -6 to 6
- mix_gain: bfloat16 [2048], replicated, may hold values from 0.099609375 to 1.8984375
- proj_x: bfloat16 [2048, 512], P(None, 'tp'), may hold values from -0.125 to 0.125
- proj_z: bfloat16 [2048, 512], P(None, 'tp'), may hold values from -0.125 to 0.125
- proj_b: bfloat16 [2048, 512], P(None, 'tp'), may hold values from -0.125 to 0.125
- proj_c: bfloat16 [2048, 512], P(None, 'tp'), may hold values from -0.125 to 0.125
- proj_step: bfloat16 [2048, 8], replicated, may hold values from -0.125 to 0.125
- step_bias: float32 [8], P('tp'), may hold values from -5 to -1
- decay_rate: float32 [8], P('tp'), may hold values from 1 to 16
- conv_taps: bfloat16 [3, 4, 512], P(None, None, 'tp'), may hold values from -3 to 3
- conv_state: bfloat16 [2048, 3, 3, 512], P('ep', None, None, 'tp'), may hold values from -6 to 6
- scan_state: float32 [2048, 8, 64, 128], P('ep', 'tp'), may hold values from -2.5 to 2.5
- inner_gain: bfloat16 [512], P('tp'), may hold values from 0.099609375 to 1.8984375
- proj_out: bfloat16 [512, 2048], P('tp'), may hold values from -0.25 to 0.25
- post_gain: bfloat16 [2048], replicated, may hold values from 0.099609375 to 1.8984375
- ffn_gain: bfloat16 [2048], replicated, may hold values from 0.099609375 to 1.8984375
- group_router: bfloat16 [2048, 2], replicated, may hold values from -0.125 to 0.125
- expert_router: bfloat16 [2048, 64], replicated, may hold values from -0.125 to 0.125
- route_experts: int32 [2048, 4], P('ep'), may hold values from 0 to 63, as said below
- expert_gate: bfloat16 [64, 2048, 1024], P('ep', None, 'tp'), may hold values from -0.125 to 0.125
- expert_up: bfloat16 [64, 2048, 1024], P('ep', None, 'tp'), may hold values from -0.125 to 0.125
- expert_down: bfloat16 [64, 1024, 2048], P('ep', 'tp')
- dense_switch: bfloat16 [2048], replicated, may hold values from -0.125 to 0.125
- dense_gate: bfloat16 [2048, 2048], P('ep', 'tp'), may hold values from -0.125 to 0.125
- dense_up: bfloat16 [2048, 2048], P('ep', 'tp'), may hold values from -0.125 to 0.125
- dense_down: bfloat16 [2048, 2048], P('ep', 'tp')
- out_gain: bfloat16 [2048], P('tp'), may hold values from 0.099609375 to 1.8984375
Outputs:
- layer_out: bfloat16 [2048, 2048], P('ep', 'tp')
- new_state: float32 [2048, 8, 64, 128], P('ep', 'tp')
- new_conv: bfloat16 [2048, 3, 3, 512], P('ep', None, None, 'tp')
The draws below stay inside these ranges and needn't reach their ends.
Inputs may be any that keep to these rules, and one draw needn't show every extreme that they name: `route_experts`: each row names 4 different experts, all from one group of 32 consecutive expert numbers. Within each aligned block of 32 rows (the rows of one index of ep) no expert is named more than 4 times, and one expert, the same in every block, is named exactly 4 times in every block.
All inputs are finite; a program needn't handle non-finite values.
Results may differ from the reference program's by a relative error of at most 0.019.
Values may be sent and summed in bfloat16 or wider, within the bound.
A program may use at most 64 MiB of HBM per device.

```python
import math
import jax
import jax.numpy as jnp
from jax import lax

MODEL_WIDTH = 2048
HEAD_COUNT = 8
HEAD_DIM = 64
STATE_DIM = 128
STATE_GROUPS = 4
CONV_TAPS = 4
EXPERT_WIDTH = 1024
DENSE_WIDTH = 2048
ROUTE_GROUPS = 2
ROUTE_PICKS = 4
SEQ_DEV = 32
INNER_WIDTH = 512
EXPERTS = 64
GROUP_EXPERTS = 32
CAPACITY = 4
TOKENS = 2048
N_TP = 4


def draw_route_experts(key, part):
    blocks = TOKENS // SEQ_DEV
    hot_key, block_key = jax.random.split(jax.random.fold_in(key, 11))
    hot = jax.random.randint(hot_key, (), 0, EXPERTS)
    hot_group = hot // GROUP_EXPERTS
    hot_local = hot % GROUP_EXPERTS
    needed = (CAPACITY - 1) * GROUP_EXPERTS // ROUTE_PICKS + 1

    def one_block(index):
        keys = jax.random.split(jax.random.fold_in(block_key, index), 5)
        hot_rows = jax.random.randint(keys[0], (), needed, SEQ_DEV + 1)
        other = jax.random.randint(keys[1], (SEQ_DEV,), 0, ROUTE_GROUPS - 1)
        other = other + (other >= hot_group).astype(jnp.int32)
        position = jnp.arange(SEQ_DEV)
        group_of = jnp.where(position < hot_rows, hot_group, other)
        group_of = jax.random.permutation(keys[2], group_of)
        member = (group_of[:, None] == jnp.arange(ROUTE_GROUPS)[None, :]).astype(jnp.int32)
        rank = jnp.sum((jnp.cumsum(member, axis=0) - member) * member, axis=1)
        orders = jax.vmap(lambda inner: jax.random.permutation(inner, GROUP_EXPERTS))(jax.random.split(keys[3], ROUTE_GROUPS))
        offsets = jax.random.randint(keys[4], (ROUTE_GROUPS,), 0, GROUP_EXPERTS)
        hot_place = jnp.argmax((orders[hot_group] == hot_local).astype(jnp.int32))
        offsets = offsets.at[hot_group].set(hot_place)
        order_rows = orders[group_of]
        places = (offsets[group_of][:, None] + rank[:, None] * ROUTE_PICKS + jnp.arange(ROUTE_PICKS)[None, :]) % GROUP_EXPERTS
        local = jnp.take_along_axis(order_rows, places, axis=1)
        return (group_of[:, None] * GROUP_EXPERTS + local).astype(jnp.int32)
    return jax.vmap(one_block)(jnp.arange(blocks)).reshape(TOKENS, ROUTE_PICKS)


def column_ramp(width):
    ramp = jnp.arange(width, dtype=jnp.float32) / width
    return 0.5 * jnp.power(10.0, ramp)


def draw_expert_down(key, part):
    base = jax.random.truncated_normal(jax.random.fold_in(key, 21), -6.0, 6.0, (EXPERTS, EXPERT_WIDTH, MODEL_WIDTH), jnp.float32)
    base = base * EXPERT_WIDTH ** (-0.5)
    return (base * column_ramp(MODEL_WIDTH)[None, None, :]).astype(jnp.bfloat16)


def draw_dense_down(key, part):
    base = jax.random.truncated_normal(jax.random.fold_in(key, 31), -6.0, 6.0, (DENSE_WIDTH, MODEL_WIDTH), jnp.float32)
    base = base * DENSE_WIDTH ** (-0.5)
    return (base * column_ramp(MODEL_WIDTH)[None, :]).astype(jnp.bfloat16)


def shard_levels(own_key, shape, shards, smallest, top_value):
    level, own = 1.0, jax.random.fold_in(own_key, 6)
    for dim, blocks in shards:
        heights = jnp.exp(jax.random.uniform(jax.random.fold_in(own, dim), (blocks,), jnp.float32, smallest / len(shards), top_value / len(shards)))
        level = level * jnp.repeat(heights, shape[dim] // blocks).reshape([-1 if axis == dim else 1 for axis in range(len(shape))])
    return level


def normal_values(stream_key, extent, scale, limit, shards=(), held_as=jnp.bfloat16):
    values = jax.random.normal(stream_key, extent, jnp.float32) * scale
    if len(shards) > 0:
        values = shard_levels(stream_key, extent, shards, -0.22, 0.18) * values
    return jnp.clip(values, min=-limit, max=limit).astype(held_as)


def setup_inputs(seed: int = 0) -> dict:
    key_of = jax.random.split(jax.random.key(seed), 28)
    resid = normal_values(key_of[0], (TOKENS, MODEL_WIDTH), 1.0, 6.0, ((0, 64),))
    mix_gain = jnp.clip(1.0 + 0.18 * jax.random.normal(key_of[1], (MODEL_WIDTH,), jnp.float32), 0.099609375, 1.8984375).astype(jnp.bfloat16)
    proj_x = normal_values(key_of[2], (MODEL_WIDTH, INNER_WIDTH), MODEL_WIDTH ** -0.5, 0.125, ((1, 4),))
    proj_z = normal_values(key_of[3], (MODEL_WIDTH, INNER_WIDTH), MODEL_WIDTH ** -0.5, 0.125, ((1, 4),))
    proj_b = normal_values(key_of[4], (MODEL_WIDTH, STATE_GROUPS * STATE_DIM), MODEL_WIDTH ** -0.5, 0.125, ((1, 4),))
    proj_c = normal_values(key_of[5], (MODEL_WIDTH, STATE_GROUPS * STATE_DIM), MODEL_WIDTH ** -0.5, 0.125, ((1, 4),))
    proj_step = normal_values(key_of[6], (MODEL_WIDTH, HEAD_COUNT), MODEL_WIDTH ** -0.5, 0.125)
    step_bias = jnp.clip(-5.0 + 4.0 * jax.random.uniform(key_of[7], (HEAD_COUNT,), jnp.float32) ** shard_levels(key_of[7], (HEAD_COUNT,), ((0, 4),), -0.2, 0.2), -5.0, -1.0)
    decay_rate = jnp.clip(jnp.exp(math.log(16.0) - 2.7725887 * jax.random.uniform(key_of[8], (HEAD_COUNT,), jnp.float32) ** shard_levels(key_of[8], (HEAD_COUNT,), ((0, 4),), -0.2, 0.2)), 1.0, 16.0)
    conv_taps = normal_values(key_of[9], (3, CONV_TAPS, INNER_WIDTH), CONV_TAPS ** -0.5, 3.0, ((2, 4),))
    conv_state = normal_values(key_of[10], (TOKENS, 3, CONV_TAPS - 1, INNER_WIDTH), 1.0, 6.0, ((0, 64), (3, 4)))
    scan_state = normal_values(key_of[11], (TOKENS, HEAD_COUNT, HEAD_DIM, STATE_DIM), 0.3, 2.5, ((0, 64), (1, 4)), jnp.float32)
    inner_gain = jnp.clip(1.0 + 0.18 * jax.random.normal(key_of[12], (INNER_WIDTH,), jnp.float32), 0.099609375, 1.8984375).astype(jnp.bfloat16)
    proj_out = normal_values(key_of[13], (INNER_WIDTH, MODEL_WIDTH), INNER_WIDTH ** -0.5, 0.25, ((0, 4),))
    post_gain = jnp.clip(1.0 + 0.18 * jax.random.normal(key_of[14], (MODEL_WIDTH,), jnp.float32), 0.099609375, 1.8984375).astype(jnp.bfloat16)
    ffn_gain = jnp.clip(1.0 + 0.18 * jax.random.normal(key_of[15], (MODEL_WIDTH,), jnp.float32), 0.099609375, 1.8984375).astype(jnp.bfloat16)
    group_router = normal_values(key_of[16], (MODEL_WIDTH, ROUTE_GROUPS), MODEL_WIDTH ** -0.5, 0.125)
    expert_router = normal_values(key_of[17], (MODEL_WIDTH, EXPERTS), MODEL_WIDTH ** -0.5, 0.125)
    route_experts = draw_route_experts(jax.random.fold_in(key_of[27], 71), 0)
    expert_gate = normal_values(key_of[19], (EXPERTS, MODEL_WIDTH, EXPERT_WIDTH), MODEL_WIDTH ** -0.5, 0.125, ((0, 64), (2, 4)))
    expert_up = normal_values(key_of[20], (EXPERTS, MODEL_WIDTH, EXPERT_WIDTH), MODEL_WIDTH ** -0.5, 0.125, ((0, 64), (2, 4)))
    expert_down = draw_expert_down(jax.random.fold_in(key_of[27], 71), 0)
    dense_switch = normal_values(key_of[22], (MODEL_WIDTH,), MODEL_WIDTH ** -0.5, 0.125)
    dense_gate = normal_values(key_of[23], (DENSE_WIDTH, MODEL_WIDTH), MODEL_WIDTH ** -0.5, 0.125, ((0, 64), (1, 4)))
    dense_up = normal_values(key_of[24], (DENSE_WIDTH, MODEL_WIDTH), MODEL_WIDTH ** -0.5, 0.125, ((0, 64), (1, 4)))
    dense_down = draw_dense_down(jax.random.fold_in(key_of[27], 71), 0)
    out_gain = jnp.clip(1.0 + 0.18 * jax.random.normal(key_of[26], (MODEL_WIDTH,), jnp.float32), 0.099609375, 1.8984375).astype(jnp.bfloat16)
    return dict(resid=resid, mix_gain=mix_gain, proj_x=proj_x, proj_z=proj_z, proj_b=proj_b, proj_c=proj_c, proj_step=proj_step, step_bias=step_bias, decay_rate=decay_rate, conv_taps=conv_taps, conv_state=conv_state, scan_state=scan_state, inner_gain=inner_gain, proj_out=proj_out, post_gain=post_gain, ffn_gain=ffn_gain, group_router=group_router, expert_router=expert_router, route_experts=route_experts, expert_gate=expert_gate, expert_up=expert_up, expert_down=expert_down, dense_switch=dense_switch, dense_gate=dense_gate, dense_up=dense_up, dense_down=dense_down, out_gain=out_gain)


norm_eps = 1e-06

def scaled_rows(values, gain):
    values = values.astype(jnp.float32)
    mean_square = lax.optimization_barrier(jnp.mean(values * values, axis=-1, keepdims=True))
    return values * lax.rsqrt(mean_square + norm_eps) * gain.astype(jnp.float32)

def softmax_plain(logits):
    weights = jnp.exp(logits)
    return weights / lax.optimization_barrier(jnp.sum(weights, axis=-1, keepdims=True))

def state_block(pieces):
    old_state, keep, driven, b_heads, c_heads = pieces
    updated = keep[:, :, None, None] * old_state + driven[:, :, :, None] * b_heads[:, :, None, :]
    read = lax.optimization_barrier(jnp.sum(updated * c_heads[:, :, None, :], axis=3))
    return (updated, read)

def expert_block(pieces):
    rows, gate_weight, up_weight, down_weight = pieces
    gate_value = jnp.dot(rows, gate_weight, preferred_element_type=jnp.float32)
    up_value = jnp.dot(rows, up_weight, preferred_element_type=jnp.float32)
    hidden = (jax.nn.silu(gate_value) * up_value).astype(jnp.bfloat16)
    share = hidden.shape[1] // N_TP
    parts = jnp.einsum('rqf,qfd->qrd', hidden.reshape(rows.shape[0], N_TP, share).astype(jnp.float32), down_weight.reshape(N_TP, share, down_weight.shape[1]).astype(jnp.float32))
    parts = lax.optimization_barrier(parts.astype(jnp.bfloat16))
    return lax.optimization_barrier(jnp.sum(parts.astype(jnp.float32), axis=0)).astype(jnp.bfloat16)

def reference(resid, mix_gain, proj_x, proj_z, proj_b, proj_c, proj_step, step_bias, decay_rate, conv_taps, conv_state, scan_state, inner_gain, proj_out, post_gain, ffn_gain, group_router, expert_router, route_experts, expert_gate, expert_up, expert_down, dense_switch, dense_gate, dense_up, dense_down, out_gain):
    normed = scaled_rows(resid, mix_gain).astype(jnp.bfloat16)
    fresh = jnp.stack([jnp.dot(normed, proj_x, preferred_element_type=jnp.float32), jnp.dot(normed, proj_b, preferred_element_type=jnp.float32), jnp.dot(normed, proj_c, preferred_element_type=jnp.float32)], axis=1).astype(jnp.bfloat16)
    gate_z = jnp.dot(normed, proj_z, preferred_element_type=jnp.float32)
    step_raw = jnp.dot(normed, proj_step, preferred_element_type=jnp.float32)
    history = jnp.concatenate([conv_state, fresh[:, :, None, :]], axis=2)
    activated = jax.nn.silu(lax.optimization_barrier(jnp.sum(history.astype(jnp.float32) * conv_taps.astype(jnp.float32)[None], axis=2)))
    repeat = HEAD_COUNT // STATE_GROUPS
    xs_heads = activated[:, 0].reshape(TOKENS, HEAD_COUNT, HEAD_DIM)
    b_heads = jnp.repeat(activated[:, 1].reshape(TOKENS, STATE_GROUPS, STATE_DIM), repeat, axis=1)
    c_heads = jnp.repeat(activated[:, 2].reshape(TOKENS, STATE_GROUPS, STATE_DIM), repeat, axis=1)
    step = jax.nn.softplus(step_raw + step_bias)
    keep = jnp.exp(-decay_rate * step)
    driven = step[:, :, None] * xs_heads
    blocks = TOKENS // SEQ_DEV

    def by_block(array):
        return array.reshape((blocks, SEQ_DEV) + array.shape[1:])
    new_state, read = lax.map(state_block, (by_block(scan_state), by_block(keep), by_block(driven), by_block(b_heads), by_block(c_heads)))
    new_state = new_state.reshape(scan_state.shape)
    read = read.reshape(TOKENS, INNER_WIDTH)
    gated = (read * jax.nn.silu(gate_z) * inner_gain.astype(jnp.float32)).astype(jnp.bfloat16)
    mixed = jnp.dot(gated, proj_out, preferred_element_type=jnp.float32)
    stream = (resid.astype(jnp.float32) + scaled_rows(mixed, post_gain)).astype(jnp.bfloat16)
    feed = scaled_rows(stream, ffn_gain).astype(jnp.bfloat16)
    group_prob = softmax_plain(jnp.dot(feed, group_router, preferred_element_type=jnp.float32))
    expert_logits = jnp.dot(feed, expert_router, preferred_element_type=jnp.float32)
    matches = route_experts[:, :, None] == jnp.arange(EXPERTS, dtype=jnp.int32)[None, None, :]
    pick_logits = lax.optimization_barrier(jnp.sum(jnp.where(matches, expert_logits[:, None, :], 0.0), axis=2))
    chosen_group = route_experts[:, 0] // GROUP_EXPERTS
    group_weight = lax.optimization_barrier(jnp.sum(jnp.where(chosen_group[:, None] == jnp.arange(ROUTE_GROUPS, dtype=jnp.int32)[None, :], group_prob, 0.0), axis=1))
    pick_weight = softmax_plain(pick_logits) * group_weight[:, None]
    flat_picks = route_experts.reshape(blocks, SEQ_DEV * ROUTE_PICKS)
    one_hot = (flat_picks[:, :, None] == jnp.arange(EXPERTS, dtype=jnp.int32)[None, None, :]).astype(jnp.int32)
    slot = lax.optimization_barrier(jnp.sum((jnp.cumsum(one_hot, axis=1) - one_hot) * one_hot, axis=2))
    block_ids = jnp.arange(blocks, dtype=jnp.int32)[:, None]
    target = ((flat_picks * blocks + block_ids) * CAPACITY + slot).reshape(-1).astype(jnp.int32)
    repeated = jnp.repeat(feed, ROUTE_PICKS, axis=0)
    buffer = jnp.zeros((EXPERTS * blocks * CAPACITY, MODEL_WIDTH), jnp.bfloat16).at[target].set(repeated)
    served = lax.map(expert_block, (buffer.reshape(EXPERTS, blocks * CAPACITY, MODEL_WIDTH), expert_gate, expert_up, expert_down))
    expert_out = served.reshape(-1, MODEL_WIDTH)[target].reshape(TOKENS, ROUTE_PICKS, MODEL_WIDTH)
    routed = lax.optimization_barrier(jnp.sum(expert_out.astype(jnp.float32) * pick_weight[:, :, None], axis=1))
    dense_pre_gate = jnp.dot(feed, dense_gate.T, preferred_element_type=jnp.float32)
    dense_pre_up = jnp.dot(feed, dense_up.T, preferred_element_type=jnp.float32)
    dense_hidden = (jax.nn.silu(dense_pre_gate) * dense_pre_up).astype(jnp.bfloat16)
    dense_out = jnp.dot(dense_hidden, dense_down, preferred_element_type=jnp.float32)
    switch = jax.nn.sigmoid(jnp.dot(feed, dense_switch, preferred_element_type=jnp.float32))
    combined = routed + switch[:, None] * dense_out
    layer_out = (stream.astype(jnp.float32) + scaled_rows(combined, out_gain)).astype(jnp.bfloat16)
    new_conv = history[:, :, 1:, :]
    return (layer_out, new_state, new_conv)
```

```python
import functools

import jax
import jax.numpy as jnp
from jax import lax
from jax.experimental import pallas as pl
from jax.experimental.pallas import tpu as pltpu
from jax.sharding import Mesh
from jax.sharding import PartitionSpec as P

EP = ("ep_0", "ep_1", "ep_2")
MESH = pl.DeviceIdType.MESH
norm_eps = 1e-06
CAPACITY = 4
LANES = 128


def dot(a, b):
    return jnp.dot(a, b, preferred_element_type=jnp.float32)


def dot_nt(a, b):
    return lax.dot_general(a, b, (((1,), (1,)), ((), ())), preferred_element_type=jnp.float32)


def in_row(gain_ref):
    gain = gain_ref[...].astype(jnp.float32)
    return jnp.concatenate([gain[i : i + 1] for i in range(gain.shape[0])], axis=1)


def iota(shape, dim):
    return lax.broadcasted_iota(jnp.int32, shape, dim)


def shift_of(count):
    return count.bit_length() - 1


def root_mean(values):
    return values * lax.rsqrt(jnp.mean(values * values, axis=-1, keepdims=True) + norm_eps)


def rest_of_layer(
    sizes,
    gated,
    proj_out,
    resid,
    post_gain,
    ffn_gain,
    switch_row,
    group_rows,
    expert_rows,
    route,
    expert_gate,
    expert_up,
    expert_down,
    dense_gate,
    dense_up,
    dense_down,
    out_gain,
    layer_out,
    w_gate,
    w_up,
    w_down,
    d_gate,
    d_up,
    d_down,
    mixed_f,
    mixed_b,
    mixed_in,
    feed_out,
    feed_in,
    stream_out,
    stream_in,
    pick_in,
    pick_z,
    code_z,
    feed_z,
    rows_out,
    rows_in,
    rows_x,
    pre_out,
    pre_in,
    hidden_x,
    sum_out,
    sum_in,
    back_out,
    back_in,
    last_out,
    last_in,
    square_x,
    send_sem,
    recv_sem,
    local_sem,
):
    nz, ny, nc, nx, cap = sizes
    np_ = ny * nc
    z, y, c, x = (lax.axis_index(a) for a in ("ep_0", "ep_1", "ep_2", "tp"))
    place = y * nc + c
    toks = gated.shape[0]
    own = toks // nx
    width = proj_out.shape[1]
    quarter = width // nx
    all_toks = nz * toks
    rows = np_ * nz * cap
    half = np_ // 2

    def z_dev(r):
        return {"ep_0": lax.rem(z + r, nz)}

    def p_dev(q):
        to = lax.rem(place + q, np_)
        return {"ep_1": to // nc, "ep_2": lax.rem(to, nc)}

    def x_dev(r):
        return {"tp": lax.rem(x + r, nx)}

    used = [0]
    started = []

    def send(src, dst, device):
        k = used[0]
        used[0] += 1
        copy = pltpu.make_async_remote_copy(
            src_ref=src,
            dst_ref=dst,
            send_sem=send_sem.at[k],
            recv_sem=recv_sem.at[k],
            device_id=device,
            device_id_type=MESH,
        )
        copy.start()
        started.append(copy)
        return copy

    local = []

    def fetch(src, dst):
        copy = pltpu.make_async_copy(src, dst, local_sem.at[len(local)])
        copy.start()
        local.append(copy)
        return copy

    def arrive(copies):
        for copy in copies:
            copy.wait_recv()

    barrier = pltpu.get_barrier_semaphore()
    peers = (
        [x_dev(r) for r in range(1, nx)]
        + [p_dev(q) for q in range(1, np_)]
        + [z_dev(r) for r in range(1, nz)]
    )
    for device in peers:
        pl.semaphore_signal(barrier, inc=1, device_id=device, device_id_type=MESH)

    own_dense = [
        fetch(dense_gate, d_gate.at[0]),
        fetch(dense_up, d_up.at[0]),
        fetch(dense_down, d_down.at[0]),
    ]
    own_expert = [fetch(expert_gate, w_gate), fetch(expert_up, w_up)]
    own_expert += [
        fetch(expert_down.at[:, pl.ds(j * quarter, quarter)], w_down.at[j]) for j in range(nx)
    ]

    route_t = route[...]
    picks = route_t.shape[0]
    expert_ids = iota((LANES, toks), 0)
    named = jnp.zeros((LANES, toks), jnp.float32)
    for k in range(picks):
        named += jnp.where(expert_ids == route_t[k : k + 1, :], 1.0, 0.0)
    named_b = named.astype(jnp.bfloat16)
    before = jnp.where(iota((toks, toks), 0) < iota((toks, toks), 1), 1.0, 0.0).astype(jnp.bfloat16)
    code_t = (named * (dot(named_b, before) + 1.0)).astype(jnp.bfloat16)
    eye = jnp.where(iota((toks, toks), 0) == iota((toks, toks), 1), 1.0, 0.0).astype(jnp.bfloat16)
    code_z[0] = dot_nt(eye, code_t).astype(jnp.bfloat16)

    share = dot(gated[...], proj_out[...]).reshape(nx, own, width)
    mixed_f[...] = share
    mixed_b[...] = share.astype(jnp.bfloat16)

    pl.semaphore_wait(barrier, len(peers))

    copies = [
        send(mixed_b.at[lax.rem(x + r, nx)], mixed_in.at[r - 1], x_dev(r)) for r in range(1, nx)
    ]
    code_copies = [send(code_z.at[0], code_z.at[r], z_dev(r)) for r in range(1, nz)]
    dense_copies = []
    for src, dst in ((dense_gate, d_gate), (dense_up, d_up), (dense_down, d_down)):
        dense_copies += [send(src, dst.at[q], p_dev(q)) for q in range(1, np_)]

    arrive(copies)
    mixed = mixed_f[x]
    for r in range(1, nx):
        mixed += mixed_in[r - 1].astype(jnp.float32)
    stream = (resid[x].astype(jnp.float32) + root_mean(mixed) * in_row(post_gain)).astype(
        jnp.bfloat16
    )
    feed = (root_mean(stream.astype(jnp.float32)) * in_row(ffn_gain)).astype(jnp.bfloat16)
    for j in range(nx):
        feed_out[j] = feed[:, j * quarter : (j + 1) * quarter]
        stream_out[j] = stream[:, j * quarter : (j + 1) * quarter]
    feed_in[x] = feed_out[x]
    feed_copies = [
        send(feed_out.at[lax.rem(x + r, nx)], feed_in.at[x], x_dev(r)) for r in range(1, nx)
    ]

    feed_f = feed.astype(jnp.float32)
    experts = expert_rows.shape[0]
    groups = group_rows.shape[0]
    group_size = experts // groups
    token_pick = jnp.where(iota((own, toks), 1) == iota((own, toks), 0) + x * own, 1.0, 0.0)
    own_route = dot_nt(token_pick.astype(jnp.bfloat16), route_t.astype(jnp.bfloat16))
    logits = dot_nt(feed, expert_rows[...])
    lanes = iota((own, experts), 1).astype(jnp.float32)
    weights = []
    for k in range(picks):
        chosen = jnp.sum(
            jnp.where(lanes == own_route[:, k : k + 1], logits, 0.0), axis=1, keepdims=True
        )
        weights.append(jnp.exp(chosen))
    total = functools.reduce(jnp.add, weights)
    group_f = group_rows[...].astype(jnp.float32)
    group_exp = [
        jnp.exp(jnp.sum(feed_f * group_f[g : g + 1], axis=1, keepdims=True)) for g in range(groups)
    ]
    group_total = functools.reduce(jnp.add, group_exp)
    first = own_route[:, 0:1]
    group_weight = jnp.zeros((own, 1), jnp.float32)
    for g in range(groups):
        here = (first >= g * group_size) & (first < (g + 1) * group_size)
        group_weight += jnp.where(here, group_exp[g] / group_total, 0.0)
    switch = jax.nn.sigmoid(jnp.sum(feed_f * in_row(switch_row), axis=1, keepdims=True))
    all_lanes = iota((own, LANES), 1).astype(jnp.float32)
    pick_table = jnp.where(all_lanes < experts, 0.0, switch)
    for k in range(picks):
        pick_table += jnp.where(
            all_lanes == own_route[:, k : k + 1], weights[k] / total * group_weight, 0.0
        )
    pick_in[x] = pick_table

    arrive(feed_copies)
    feed_z[0] = feed_in[...].astype(jnp.float32).reshape(toks, quarter).astype(jnp.bfloat16)
    feed_copies = [send(feed_z.at[0], feed_z.at[r], z_dev(r)) for r in range(1, nz)]
    pick_copies = [send(pick_in.at[x], pick_in.at[x], x_dev(r)) for r in range(1, nx)]
    stream_in[x] = stream_out[x]
    stream_copies = [
        send(stream_out.at[lax.rem(x + r, nx)], stream_in.at[x], x_dev(r)) for r in range(1, nx)
    ]

    arrive(code_copies)
    codes = code_z[...].reshape(all_toks, LANES)
    step = shift_of(nz * cap)

    def expert_of(j):
        return z * np_ + ((place + (j >> step)) & (np_ - 1))

    def block_of(j):
        return (j & (nz * cap - 1)) >> shift_of(cap)

    def slot_of(j):
        return ((j & (cap - 1)) + 1).astype(jnp.float32)

    choose_t = jnp.where(
        iota((rows, LANES), 1) == expert_of(iota((rows, LANES), 0)), 1.0, 0.0
    ).astype(jnp.bfloat16)
    choose = jnp.where(
        iota((LANES, rows), 0) == expert_of(iota((LANES, rows), 1)), 1.0, 0.0
    ).astype(jnp.bfloat16)
    j_row = iota((rows, all_toks), 0)
    t_col = iota((rows, all_toks), 1)
    put = jnp.where(
        (dot_nt(choose_t, codes) == slot_of(j_row)) & (block_of(j_row) == t_col >> shift_of(toks)),
        1.0,
        0.0,
    ).astype(jnp.bfloat16)

    arrive(pick_copies)
    pick_z[0] = pick_in[...].reshape(toks, LANES)
    pick_copies = [send(pick_z.at[0], pick_z.at[r], z_dev(r)) for r in range(1, nz)]

    arrive(feed_copies)
    feeds = feed_z[...].reshape(all_toks, quarter)
    rows_out[...] = dot(put, feeds).astype(jnp.bfloat16).reshape(rows_out.shape)
    rows_in[0] = rows_out[0]
    row_copies = [None] + [send(rows_out.at[q], rows_in.at[q], p_dev(q)) for q in range(1, np_)]

    for copy in own_dense:
        copy.wait()
    arrive(dense_copies)
    hidden_here = d_gate.shape[0] * d_gate.shape[1]
    for k, weight in enumerate((d_gate, d_up)):
        part = dot_nt(feeds, weight[...].reshape(hidden_here, quarter)).astype(jnp.bfloat16)
        pre_out[:, :, k * hidden_here : (k + 1) * hidden_here] = part.reshape(
            nx, all_toks // nx, hidden_here
        )
    pre_copies = [
        send(pre_out.at[lax.rem(x + r, nx)], pre_in.at[r - 1], x_dev(r)) for r in range(1, nx)
    ]

    from_left, from_right, from_far = [], [], []
    for q in range(np_):
        if q:
            row_copies[q].wait_recv()
        from_left.append(send(rows_in.at[q], rows_x.at[0, q], x_dev(1)))
        from_right.append(send(rows_in.at[q], rows_x.at[1, q], x_dev(nx - 1)))

    arrive(pre_copies)
    pre = pre_out[x].astype(jnp.float32)
    for r in range(1, nx):
        pre += pre_in[r - 1].astype(jnp.float32)
    hidden_x[x] = (jax.nn.silu(pre[:, :hidden_here]) * pre[:, hidden_here:]).astype(jnp.bfloat16)
    hidden_copies = [send(hidden_x.at[x], hidden_x.at[x], x_dev(r)) for r in range(1, nx)]

    for q in range(half):
        from_left[q].wait_recv()
        from_far.append(send(rows_x.at[0, q], rows_x.at[2, q], x_dev(1)))
        from_right[half + q].wait_recv()
        from_far.append(send(rows_x.at[1, half + q], rows_x.at[2, half + q], x_dev(nx - 1)))
    for copy in own_expert:
        copy.wait()

    def of_share(taken, share):
        taken = taken.reshape(rows, quarter)
        return dot(taken, w_gate[share]), dot(taken, w_up[share])

    gate_value, up_value = of_share(rows_in[...], x)
    arrive(from_left[half:])
    more = of_share(rows_x[0], lax.rem(x + nx - 1, nx))
    gate_value, up_value = gate_value + more[0], up_value + more[1]
    arrive(from_right[:half])
    more = of_share(rows_x[1], lax.rem(x + 1, nx))
    gate_value, up_value = gate_value + more[0], up_value + more[1]
    arrive(from_far)
    more = of_share(rows_x[2], lax.rem(x + 2, nx))
    gate_value, up_value = gate_value + more[0], up_value + more[1]
    hidden = (jax.nn.silu(gate_value) * up_value).astype(jnp.bfloat16)

    cut = rows // 2
    low, high = hidden[:cut], hidden[cut:]
    right, left, far = lax.rem(x + 1, nx), lax.rem(x + nx - 1, nx), lax.rem(x + 2, nx)

    def put_out(k, values, device):
        sum_out[k] = values.astype(jnp.bfloat16)
        return send(sum_out.at[k], sum_in.at[k], device)

    to_right, to_left = x_dev(1), x_dev(nx - 1)
    sums = [
        put_out(0, dot(low, w_down[far]), to_right),
        put_out(1, dot(high, w_down[far]), to_left),
        put_out(2, dot(high, w_down[right]), to_right),
        put_out(3, dot(low, w_down[left]), to_left),
    ]
    value = dot(low, w_down[right])
    sums[0].wait_recv()
    sums.append(put_out(4, value + sum_in[0].astype(jnp.float32), to_right))
    value = dot(high, w_down[left])
    sums[1].wait_recv()
    sums.append(put_out(5, value + sum_in[1].astype(jnp.float32), to_left))

    arrive(hidden_copies)
    down = d_down[...].reshape(hidden_here, quarter)
    dense_part = dot(hidden_x[...].reshape(all_toks, hidden_here), down)
    arrive(pick_copies)
    table = pick_z[...].reshape(all_toks, LANES)
    dense_part = dense_part * table[:, experts : experts + 1]
    table_hi = table.astype(jnp.bfloat16)
    table_lo = (table - table_hi.astype(jnp.float32)).astype(jnp.bfloat16)
    j_col = iota((all_toks, rows), 1)
    take = (dot(codes, choose) == slot_of(j_col)) & (
        block_of(j_col) == iota((all_toks, rows), 0) >> shift_of(toks)
    )
    take_hi = jnp.where(take, dot(table_hi, choose), 0.0).astype(jnp.bfloat16)
    take_lo = jnp.where(take, dot(table_lo, choose), 0.0).astype(jnp.bfloat16)

    done_low = dot(low, w_down[x])
    done_high = dot(high, w_down[x])
    sums[3].wait_recv()
    sums[4].wait_recv()
    done_low += sum_in[3].astype(jnp.float32) + sum_in[4].astype(jnp.float32)
    back_out[:half] = done_low.astype(jnp.bfloat16).reshape(half, nz * cap, quarter)
    back_in[0] = back_out[0]
    back = [None] + [
        send(back_out.at[q], back_in.at[q], p_dev(np_ - q)) for q in range(1, half)
    ]
    sums[2].wait_recv()
    sums[5].wait_recv()
    done_high += sum_in[2].astype(jnp.float32) + sum_in[5].astype(jnp.float32)
    back_out[half:] = done_high.astype(jnp.bfloat16).reshape(half, nz * cap, quarter)
    back += [send(back_out.at[q], back_in.at[q], p_dev(np_ - q)) for q in range(half, np_)]

    arrive(back[1:])
    results = back_in[...].reshape(rows, quarter)
    part = dot(take_hi, results) + dot(take_lo, results) + dense_part
    last_out[...] = part.astype(jnp.bfloat16).reshape(nz, toks, quarter)
    last = [send(last_out.at[r], last_in.at[r - 1], z_dev(nz - r)) for r in range(1, nz)]
    combined = part[:toks]
    gain = in_row(out_gain)
    arrive(stream_copies)
    stream_part = stream_in[...].astype(jnp.float32).reshape(toks, quarter)
    arrive(last)
    for r in range(1, nz):
        combined += last_in[r - 1].astype(jnp.float32)

    square = jnp.sum(combined * combined, axis=1, keepdims=True)
    on_lane = iota((toks, LANES), 0) == iota((toks, LANES), 1)
    as_row = jnp.sum(jnp.where(on_lane, square, 0.0), axis=0, keepdims=True)
    square_x[0] = jnp.broadcast_to(as_row, square_x.shape[1:])
    square_copies = [send(square_x.at[0], square_x.at[r], x_dev(r)) for r in range(1, nx)]
    combined = combined * gain
    arrive(square_copies)
    all_rows = square_x[0]
    for r in range(1, nx):
        all_rows += square_x[r]
    total_square = jnp.sum(jnp.where(on_lane, all_rows[0:1], 0.0), axis=1, keepdims=True)
    scale = lax.rsqrt(total_square / width + norm_eps)
    layer_out[...] = (stream_part + combined * scale).astype(jnp.bfloat16)

    for copy in started:
        copy.wait_send()


def copies_of(nz, np_, nx):
    x_copies = 3 * (nx - 1) + 3 * (nx - 1) + (nx - 1) + 2 * np_ + np_ + 6
    return x_copies + 4 * (nz - 1) + 5 * (np_ - 1)


def after_mixer(sizes, gated, resid, params):
    nz, ny, nc, nx, cap = sizes
    np_ = ny * nc
    toks, width = resid.shape
    own, quarter = toks // nx, width // nx
    rows = np_ * nz * cap
    all_toks = nz * toks
    bf16, f32 = jnp.bfloat16, jnp.float32
    share = params["expert_gate"].shape[2]
    hid = params["dense_gate"].shape[0]
    tall = lambda a: a.reshape(-1, LANES)
    operands = (
        gated,
        params["proj_out"],
        resid.reshape(nx, own, width),
        tall(params["post_gain"]),
        tall(params["ffn_gain"]),
        tall(params["dense_switch"]),
        params["group_router"].T,
        params["expert_router"].T,
        params["route_experts"].T,
        params["expert_gate"].reshape(nx, quarter, share),
        params["expert_up"].reshape(nx, quarter, share),
        params["expert_down"].reshape(share, width),
        params["dense_gate"],
        params["dense_up"],
        params["dense_down"],
        tall(params["out_gain"]),
    )
    vmem = pl.BlockSpec(memory_space=pltpu.VMEM)
    anyw = pl.BlockSpec(memory_space=pl.ANY)
    in_specs = [vmem] * 9 + [anyw] * 6 + [vmem]
    scratch = [
        pltpu.VMEM((nx, quarter, share), bf16),
        pltpu.VMEM((nx, quarter, share), bf16),
        pltpu.VMEM((nx, share, quarter), bf16),
        pltpu.VMEM((np_, hid, quarter), bf16),
        pltpu.VMEM((np_, hid, quarter), bf16),
        pltpu.VMEM((np_, hid, quarter), bf16),
        pltpu.VMEM((nx, own, width), f32),
        pltpu.VMEM((nx, own, width), bf16),
        pltpu.VMEM((nx - 1, own, width), bf16),
        pltpu.VMEM((nx, own, quarter), bf16),
        pltpu.VMEM((nx, own, quarter), bf16),
        pltpu.VMEM((nx, own, quarter), bf16),
        pltpu.VMEM((nx, own, quarter), bf16),
        pltpu.VMEM((nx, own, LANES), f32),
        pltpu.VMEM((nz, toks, LANES), f32),
        pltpu.VMEM((nz, toks, LANES), bf16),
        pltpu.VMEM((nz, toks, quarter), bf16),
        pltpu.VMEM((np_, nz * cap, quarter), bf16),
        pltpu.VMEM((np_, nz * cap, quarter), bf16),
        pltpu.VMEM((3, np_, nz * cap, quarter), bf16),
        pltpu.VMEM((nx, all_toks // nx, 2 * np_ * hid), bf16),
        pltpu.VMEM((nx - 1, all_toks // nx, 2 * np_ * hid), bf16),
        pltpu.VMEM((nx, all_toks // nx, np_ * hid), bf16),
        pltpu.VMEM((6, rows // 2, quarter), bf16),
        pltpu.VMEM((6, rows // 2, quarter), bf16),
        pltpu.VMEM((np_, nz * cap, quarter), bf16),
        pltpu.VMEM((np_, nz * cap, quarter), bf16),
        pltpu.VMEM((nz, toks, quarter), bf16),
        pltpu.VMEM((nz - 1, toks, quarter), bf16),
        pltpu.VMEM((nx, 8, LANES), f32),
        pltpu.SemaphoreType.DMA((copies_of(nz, np_, nx),)),
        pltpu.SemaphoreType.DMA((copies_of(nz, np_, nx),)),
        pltpu.SemaphoreType.DMA((5 + nx,)),
    ]
    return pl.pallas_call(
        functools.partial(rest_of_layer, sizes),
        out_shape=jax.ShapeDtypeStruct((toks, quarter), bf16),
        in_specs=in_specs,
        out_specs=vmem,
        scratch_shapes=scratch,
        compiler_params=pltpu.CompilerParams(
            collective_id=0, has_side_effects=True, vmem_limit_bytes=56 * 1024 * 1024
        ),
        name="rest_of_layer",
    )(*operands)


def scaled_rows(values, gain):
    values = values.astype(jnp.float32)
    mean_square = jnp.mean(values * values, axis=-1, keepdims=True)
    return values * lax.rsqrt(mean_square + norm_eps) * gain.astype(jnp.float32)


def mixer(p):
    tp_index = lax.axis_index("tp")
    resid, scan_state, conv_state = p["resid"], p["scan_state"], p["conv_state"]
    seqs = resid.shape[0]
    heads_here, head_dim, state_dim = scan_state.shape[1:]
    channels = conv_state.shape[3]
    repeat = heads_here // (channels // state_dim)
    normed = scaled_rows(resid, p["mix_gain"]).astype(jnp.bfloat16)
    fresh = jnp.stack([dot(normed, p["proj_x"]), dot(normed, p["proj_b"]), dot(normed, p["proj_c"])], axis=1).astype(jnp.bfloat16)
    gate_z = dot(normed, p["proj_z"])
    step_all = dot(normed, p["proj_step"])
    step_raw = lax.dynamic_slice_in_dim(step_all, tp_index * heads_here, heads_here, 1)
    history = jnp.concatenate([conv_state, fresh[:, :, None, :]], axis=2)
    activated = jax.nn.silu(
        jnp.sum(history.astype(jnp.float32) * p["conv_taps"].astype(jnp.float32)[None], axis=2)
    )
    xs_heads = activated[:, 0].reshape(seqs, heads_here, head_dim)
    b_heads = jnp.repeat(activated[:, 1].reshape(seqs, -1, state_dim), repeat, axis=1)
    c_heads = jnp.repeat(activated[:, 2].reshape(seqs, -1, state_dim), repeat, axis=1)
    step = jax.nn.softplus(step_raw + p["step_bias"])
    keep = jnp.exp(-p["decay_rate"] * step)
    driven = step[:, :, None] * xs_heads
    new_state = keep[:, :, None, None] * scan_state + driven[:, :, :, None] * b_heads[:, :, None, :]
    read = jnp.sum(new_state * c_heads[:, :, None, :], axis=3).reshape(seqs, channels)
    gated = (read * jax.nn.silu(gate_z) * p["inner_gain"].astype(jnp.float32)).astype(jnp.bfloat16)
    return gated, new_state, history[:, :, 1:, :]


NAMES = (
    "resid",
    "mix_gain",
    "proj_x",
    "proj_z",
    "proj_b",
    "proj_c",
    "proj_step",
    "step_bias",
    "decay_rate",
    "conv_taps",
    "conv_state",
    "scan_state",
    "inner_gain",
    "proj_out",
    "post_gain",
    "ffn_gain",
    "group_router",
    "expert_router",
    "route_experts",
    "expert_gate",
    "expert_up",
    "expert_down",
    "dense_switch",
    "dense_gate",
    "dense_up",
    "dense_down",
    "out_gain",
)


def on_device(*arrays):
    params = dict(zip(NAMES, arrays))
    sizes = tuple(lax.axis_size(a) for a in EP) + (lax.axis_size("tp"), CAPACITY)
    gated, new_state, new_conv = mixer(params)
    layer_out = after_mixer(sizes, gated, params["resid"], params)
    return layer_out, new_state, new_conv


TORUS = (8, 4, 2)


def solution(mesh):
    torus = Mesh(mesh.devices.reshape(*TORUS, mesh.shape["tp"]), EP + ("tp",))
    in_specs = (
        P(EP, None),
        P(),
        P(None, "tp"),
        P(None, "tp"),
        P(None, "tp"),
        P(None, "tp"),
        P(),
        P("tp"),
        P("tp"),
        P(None, None, "tp"),
        P(EP, None, None, "tp"),
        P(EP, "tp", None, None),
        P("tp"),
        P("tp", None),
        P(),
        P(),
        P(),
        P(),
        P(EP, None),
        P(EP, None, "tp"),
        P(EP, None, "tp"),
        P(EP, "tp", None),
        P(),
        P(EP, "tp"),
        P(EP, "tp"),
        P(EP, "tp"),
        P("tp"),
    )
    out_specs = (P(EP, "tp"), P(EP, "tp", None, None), P(EP, None, None, "tp"))
    return jax.shard_map(
        on_device, mesh=torus, in_specs=in_specs, out_specs=out_specs, check_vma=False
    )
```

```python
import functools

import jax
import jax.numpy as jnp
from jax import lax
from jax.experimental import pallas as pl
from jax.experimental.pallas import tpu as pltpu
from jax.sharding import Mesh
from jax.sharding import PartitionSpec as P

EP = ("ep_0", "ep_1", "ep_2")
MESH = pl.DeviceIdType.MESH
norm_eps = 1e-06
CAPACITY = 4
LANES = 128


def dot(a, b):
    return jnp.dot(a, b, preferred_element_type=jnp.float32)


def dot_nt(a, b):
    return lax.dot_general(a, b, (((1,), (1,)), ((), ())), preferred_element_type=jnp.float32)


def in_row(gain_ref):
    gain = gain_ref[...].astype(jnp.float32)
    return jnp.concatenate([gain[i : i + 1] for i in range(gain.shape[0])], axis=1)


def iota(shape, dim):
    return lax.broadcasted_iota(jnp.int32, shape, dim)


def shift_of(count):
    return count.bit_length() - 1


def root_mean(values):
    return values * lax.rsqrt(jnp.mean(values * values, axis=-1, keepdims=True) + norm_eps)


OPERANDS = (
    "resid",
    "mix_gain",
    "proj_x",
    "proj_b",
    "proj_c",
    "proj_z",
    "proj_step",
    "conv_taps",
    "conv_state",
    "step_bias",
    "decay_rate",
    "scan_state",
    "inner_gain",
    "proj_out",
    "route_experts",
    "dense_gate",
    "dense_up",
    "dense_down",
    "post_gain",
    "ffn_gain",
    "expert_router",
    "group_router",
    "dense_switch",
    "out_gain",
    "expert_gate",
    "expert_up",
    "expert_down",
)


def near_first(nz):
    return sorted(range(nz), key=lambda r: (min(r, nz - r), r))


def layer(sizes, plan, *refs):
    nz, ny, nc, nx, cap = sizes
    np_ = ny * nc
    given = dict(zip(OPERANDS, refs))
    layer_out, state_rows, fresh_out = refs[len(OPERANDS) : len(OPERANDS) + 3]
    s = dict(zip(plan, refs[len(OPERANDS) + 3 :]))
    send_sem, recv_sem, local_sem = s["send_sem"], s["recv_sem"], s["local_sem"]
    z, y, c, x = (lax.axis_index(a) for a in ("ep_0", "ep_1", "ep_2", "tp"))
    place = y * nc + c
    own, width = given["resid"].shape[1:]
    toks = own * nx
    quarter = width // nx
    hz = nz // 2
    half_toks = hz * toks
    chunk = hz * cap
    rows = np_ * chunk
    half = np_ // 2
    order = near_first(nz)

    def z_dev(r):
        return {"ep_0": lax.rem(z + r, nz)}

    def p_dev(q):
        to = lax.rem(place + q, np_)
        return {"ep_1": to // nc, "ep_2": lax.rem(to, nc)}

    def x_dev(r):
        return {"tp": lax.rem(x + r, nx)}

    used = [0]
    started = []

    def send(src, dst, device):
        k = used[0]
        used[0] += 1
        copy = pltpu.make_async_remote_copy(
            src_ref=src,
            dst_ref=dst,
            send_sem=send_sem.at[k],
            recv_sem=recv_sem.at[k],
            device_id=device,
            device_id_type=MESH,
        )
        copy.start()
        started.append(copy)
        return copy

    local_used = [0]

    def fetch(src, dst):
        copy = pltpu.make_async_copy(src, dst, local_sem.at[local_used[0]])
        local_used[0] += 1
        copy.start()
        return copy

    def arrive(copies):
        for copy in copies:
            copy.wait_recv()

    barrier = pltpu.get_barrier_semaphore()
    peers = (
        [x_dev(r) for r in range(1, nx)]
        + [p_dev(q) for q in range(1, np_)]
        + [z_dev(r) for r in range(1, nz)]
    )
    for device in peers:
        pl.semaphore_signal(barrier, inc=1, device_id=device, device_id_type=MESH)

    fetched = {}
    for name in OPERANDS:
        src = given[name]
        if name in ("proj_x", "proj_b", "proj_c", "proj_z"):
            k = ("proj_x", "proj_b", "proj_c", "proj_z").index(name)
            wide = src.shape[1]
            fetched[name] = [fetch(src, s["proj"].at[:, pl.ds(k * wide, wide)])]
        elif name in ("dense_gate", "dense_up", "dense_down"):
            fetched[name] = [fetch(src, s[name].at[0])]
        elif name == "expert_down":
            fetched[name] = [
                fetch(src.at[:, pl.ds(j * quarter, quarter)], s[name].at[j]) for j in range(nx)
            ]
        else:
            fetched[name] = [fetch(src, s[name])]

    def held(name):
        for copy in fetched.pop(name, ()):
            copy.wait()
        return s[name]

    route_t = held("route_experts")[...]
    picks = route_t.shape[0]
    expert_ids = iota((LANES, toks), 0)
    named = jnp.zeros((LANES, toks), jnp.float32)
    for k in range(picks):
        named += jnp.where(expert_ids == route_t[k : k + 1, :], 1.0, 0.0)
    named_b = named.astype(jnp.bfloat16)
    before = jnp.where(iota((toks, toks), 0) < iota((toks, toks), 1), 1.0, 0.0).astype(jnp.bfloat16)
    code_t = (named * (dot(named_b, before) + 1.0)).astype(jnp.bfloat16)
    eye = jnp.where(iota((toks, toks), 0) == iota((toks, toks), 1), 1.0, 0.0).astype(jnp.bfloat16)
    code_z = s["code_z"]
    code_z[0] = dot_nt(eye, code_t).astype(jnp.bfloat16)

    resid = held("resid")
    gain = in_row(held("mix_gain"))
    normed = root_mean(resid[...].astype(jnp.float32).reshape(toks, width)) * gain
    normed = normed.astype(jnp.bfloat16)
    for name in ("proj_x", "proj_b", "proj_c", "proj_z"):
        for copy in fetched.pop(name):
            copy.wait()
    projected = dot(normed, s["proj"][...])
    step_all = dot_nt(normed, held("proj_step")[...])
    taps = held("conv_taps")[...].astype(jnp.float32)
    old_conv = held("conv_state")
    channels = taps.shape[2]
    acts = []
    fresh_ref = s["fresh"]
    for k in range(3):
        fresh = projected[:, k * channels : (k + 1) * channels].astype(jnp.bfloat16)
        fresh_ref[k] = fresh
        mixed_in = fresh.astype(jnp.float32) * taps[k, 3:4]
        for i in range(3):
            mixed_in += old_conv[k, i].astype(jnp.float32) * taps[k, i : i + 1]
        acts.append(jax.nn.silu(mixed_in))
    xs, bs, cs = acts
    gate_z = projected[:, 3 * channels :]
    bias, rate = held("step_bias")[...], held("decay_rate")[...]
    heads_here = bias.shape[1]
    head_dim = channels // heads_here
    head_of = iota((toks, channels), 1) >> shift_of(head_dim)
    head_col = iota(step_all.shape, 1)
    step = jnp.zeros((toks, channels), jnp.float32)
    keep = jnp.zeros((toks, channels), jnp.float32)
    for h in range(heads_here):
        raw = jnp.sum(
            jnp.where(head_col == x * heads_here + h, step_all, 0.0), axis=1, keepdims=True
        )
        one = jax.nn.softplus(raw + bias[:, h : h + 1])
        step = jnp.where(head_of == h, one, step)
        keep = jnp.where(head_of == h, jnp.exp(-rate[:, h : h + 1] * one), keep)
    driven = step * xs
    rows_ref = s["rows_ref"]
    rows_ref[0] = keep
    rows_ref[1] = driven
    rows_ref[2] = bs
    small_out = [fetch(rows_ref, state_rows), fetch(fresh_ref, fresh_out)]
    c_ref, old_read = s["c_ref"], s["old_read"]
    c_ref[...] = cs
    diag = iota((channels, channels), 0) == iota((channels, channels), 1)
    old_state = held("scan_state")

    @pl.loop(0, toks // 8)
    def _(i):
        at = pl.multiple_of(i * 8, 8)
        c8 = c_ref[pl.ds(at, 8), :]
        out = []
        for t in range(8):
            sums = jnp.sum(old_state[at + t] * c8[t : t + 1], axis=1, keepdims=True)
            out.append(jnp.sum(jnp.where(diag, sums, 0.0), axis=0, keepdims=True))
        old_read[pl.ds(at, 8), :] = jnp.concatenate(out, axis=0)

    read = keep * old_read[...] + driven * jnp.sum(bs * cs, axis=1, keepdims=True)
    gated = (read * jax.nn.silu(gate_z) * in_row(held("inner_gain"))).astype(jnp.bfloat16)

    mixed_f, mixed_b, mixed_in = s["mixed_f"], s["mixed_b"], s["mixed_in"]
    share = dot(gated, held("proj_out")[...]).reshape(nx, own, width)
    mixed_f[...] = share
    mixed_b[...] = share.astype(jnp.bfloat16)

    pl.semaphore_wait(barrier, len(peers))

    copies = [
        send(mixed_b.at[lax.rem(x + r, nx)], mixed_in.at[r - 1], x_dev(r)) for r in range(1, nx)
    ]
    code_copies = [send(code_z.at[0], code_z.at[k], z_dev(order[k])) for k in range(1, nz)]
    dense_copies = []
    for name in ("dense_gate", "dense_up", "dense_down"):
        dense_copies += [send(given[name], s[name].at[q], p_dev(q)) for q in range(1, np_)]

    post_gain, ffn_gain = in_row(held("post_gain")), in_row(held("ffn_gain"))
    resid_own = resid[x].astype(jnp.float32)
    arrive(copies)
    mixed = mixed_f[x]
    for r in range(1, nx):
        mixed += mixed_in[r - 1].astype(jnp.float32)
    stream = (resid_own + root_mean(mixed) * post_gain).astype(jnp.bfloat16)
    feed = (root_mean(stream.astype(jnp.float32)) * ffn_gain).astype(jnp.bfloat16)
    feed_out, feed_in = s["feed_out"], s["feed_in"]
    stream_out, stream_in = s["stream_out"], s["stream_in"]
    for j in range(nx):
        feed_out[j] = feed[:, j * quarter : (j + 1) * quarter]
    feed_in[x] = feed_out[x]
    feed_copies = [
        send(feed_out.at[lax.rem(x + r, nx)], feed_in.at[x], x_dev(r)) for r in range(1, nx)
    ]
    for j in range(nx):
        stream_out[j] = stream[:, j * quarter : (j + 1) * quarter]

    feed_f = feed.astype(jnp.float32)
    expert_rows, group_rows = held("expert_router"), held("group_router")
    experts = expert_rows.shape[0]
    groups = group_rows.shape[0]
    group_size = experts // groups
    token_pick = jnp.where(iota((own, toks), 1) == iota((own, toks), 0) + x * own, 1.0, 0.0)
    own_route = dot_nt(token_pick.astype(jnp.bfloat16), route_t.astype(jnp.bfloat16))
    logits = dot_nt(feed, expert_rows[...])
    lanes = iota((own, experts), 1).astype(jnp.float32)
    weights = []
    for k in range(picks):
        chosen = jnp.sum(
            jnp.where(lanes == own_route[:, k : k + 1], logits, 0.0), axis=1, keepdims=True
        )
        weights.append(jnp.exp(chosen))
    total = functools.reduce(jnp.add, weights)
    group_f = group_rows[...].astype(jnp.float32)
    group_exp = [
        jnp.exp(jnp.sum(feed_f * group_f[g : g + 1], axis=1, keepdims=True)) for g in range(groups)
    ]
    group_total = functools.reduce(jnp.add, group_exp)
    first = own_route[:, 0:1]
    group_weight = jnp.zeros((own, 1), jnp.float32)
    for g in range(groups):
        here = (first >= g * group_size) & (first < (g + 1) * group_size)
        group_weight += jnp.where(here, group_exp[g] / group_total, 0.0)
    switch_row = in_row(held("dense_switch"))
    switch = jax.nn.sigmoid(jnp.sum(feed_f * switch_row, axis=1, keepdims=True))
    all_lanes = iota((own, LANES), 1).astype(jnp.float32)
    pick_table = jnp.where(all_lanes < experts, 0.0, switch)
    for k in range(picks):
        pick_table += jnp.where(
            all_lanes == own_route[:, k : k + 1], weights[k] / total * group_weight, 0.0
        )
    pick_in, pick_z = s["pick_in"], s["pick_z"]
    pick_in[x] = pick_table

    arrive(feed_copies)
    feed_z = s["feed_z"]
    feed_z[0] = feed_in[...].astype(jnp.float32).reshape(toks, quarter).astype(jnp.bfloat16)
    feed_copies = [None] + [
        send(feed_z.at[0], feed_z.at[k], z_dev(order[k])) for k in range(1, nz)
    ]
    pick_copies = [send(pick_in.at[x], pick_in.at[x], x_dev(r)) for r in range(1, nx)]
    stream_in[x] = stream_out[x]
    stream_copies = [
        send(stream_out.at[lax.rem(x + r, nx)], stream_in.at[x], x_dev(r)) for r in range(1, nx)
    ]

    def expert_of(j):
        return z * np_ + ((place + (j >> shift_of(chunk))) & (np_ - 1))

    def block_of(j):
        return (j & (chunk - 1)) >> shift_of(cap)

    def slot_of(j):
        return ((j & (cap - 1)) + 1).astype(jnp.float32)

    arrive(code_copies)
    codes = [
        code_z[h * hz : (h + 1) * hz].reshape(half_toks, LANES) for h in range(2)
    ]
    choose_t = jnp.where(
        iota((rows, LANES), 1) == expert_of(iota((rows, LANES), 0)), 1.0, 0.0
    ).astype(jnp.bfloat16)
    choose = jnp.where(
        iota((LANES, rows), 0) == expert_of(iota((LANES, rows), 1)), 1.0, 0.0
    ).astype(jnp.bfloat16)
    j_row = iota((rows, half_toks), 0)
    same_block = block_of(j_row) == iota((rows, half_toks), 1) >> shift_of(toks)
    put = [
        jnp.where((dot_nt(choose_t, k) == slot_of(j_row)) & same_block, 1.0, 0.0).astype(
            jnp.bfloat16
        )
        for k in codes
    ]

    arrive(pick_copies)
    pick_z[0] = pick_in[...].reshape(toks, LANES)
    pick_copies = [send(pick_z.at[0], pick_z.at[k], z_dev(order[k])) for k in range(1, nz)]

    rows_out, rows_in, rows_x = s["rows_out"], s["rows_in"], s["rows_x"]
    pre_out, pre_in, hidden_x = s["pre_out"], s["pre_in"], s["hidden_x"]
    hidden_here = s["dense_gate"].shape[0] * s["dense_gate"].shape[1]
    row_copies, pre_copies = [], []
    from_left, from_right, from_far = ([], []), ([], []), ([], [])

    def rows_to_experts(h):
        arrive(feed_copies[max(1, h * hz) : (h + 1) * hz])
        feeds = feed_z[h * hz : (h + 1) * hz].reshape(half_toks, quarter)
        rows_out[h] = dot(put[h], feeds).astype(jnp.bfloat16).reshape(np_, chunk, quarter)
        rows_in[h, 0] = rows_out[h, 0]
        row_copies.append(
            [None] + [send(rows_out.at[h, q], rows_in.at[h, q], p_dev(q)) for q in range(1, np_)]
        )
        return feeds

    def dense_sums(h, feeds):
        for k, name in enumerate(("dense_gate", "dense_up")):
            part = dot_nt(feeds, held(name)[...].reshape(hidden_here, quarter))
            part = part.reshape(hz, nx, own, hidden_here).swapaxes(0, 1)
            part = part.reshape(nx, hz * own, hidden_here).astype(jnp.bfloat16)
            pre_out[h, :, :, k * hidden_here : (k + 1) * hidden_here] = part
        pre_copies.append(
            [
                send(pre_out.at[h, lax.rem(x + r, nx)], pre_in.at[h, r - 1], x_dev(r))
                for r in range(1, nx)
            ]
        )

    def rows_over_x(h):
        for q in range(np_):
            if q:
                row_copies[h][q].wait_recv()
            from_left[h].append(send(rows_in.at[h, q], rows_x.at[h, 0, q], x_dev(1)))
            from_right[h].append(send(rows_in.at[h, q], rows_x.at[h, 1, q], x_dev(nx - 1)))

    def pass_on(h):
        for q in range(half):
            from_left[h][q].wait_recv()
            from_far[h].append(send(rows_x.at[h, 0, q], rows_x.at[h, 2, q], x_dev(1)))
            k = half + q
            from_right[h][k].wait_recv()
            from_far[h].append(send(rows_x.at[h, 1, k], rows_x.at[h, 2, k], x_dev(nx - 1)))

    w_gate, w_up, w_down = s["expert_gate"], s["expert_up"], s["expert_down"]

    def of_share(taken, share):
        taken = taken.reshape(rows, quarter)
        return dot(taken, w_gate[share]), dot(taken, w_up[share])

    right, left, far = lax.rem(x + 1, nx), lax.rem(x + nx - 1, nx), lax.rem(x + 2, nx)

    def expert_hidden(h):
        gate_value, up_value = of_share(rows_in[h], x)
        arrive(from_left[h][half:])
        more = of_share(rows_x[h, 0], left)
        gate_value, up_value = gate_value + more[0], up_value + more[1]
        arrive(from_right[h][:half])
        more = of_share(rows_x[h, 1], right)
        gate_value, up_value = gate_value + more[0], up_value + more[1]
        arrive(from_far[h])
        more = of_share(rows_x[h, 2], far)
        gate_value, up_value = gate_value + more[0], up_value + more[1]
        return (jax.nn.silu(gate_value) * up_value).astype(jnp.bfloat16)

    sum_out, sum_in = s["sum_out"], s["sum_in"]
    to_right, to_left = x_dev(1), x_dev(nx - 1)
    cut = rows // 2

    def put_out(h, k, values, device):
        sum_out[h, k] = values.astype(jnp.bfloat16)
        return send(sum_out.at[h, k], sum_in.at[h, k], device)

    def sums_start(h, hidden):
        low, high = hidden[:cut], hidden[cut:]
        return [
            put_out(h, 0, dot(low, w_down[far]), to_right),
            put_out(h, 1, dot(high, w_down[far]), to_left),
            put_out(h, 2, dot(high, w_down[right]), to_right),
            put_out(h, 3, dot(low, w_down[left]), to_left),
        ]

    def sums_pass_on(h, hidden, sums):
        low, high = hidden[:cut], hidden[cut:]
        value = dot(low, w_down[right])
        sums[0].wait_recv()
        sums.append(put_out(h, 4, value + sum_in[h, 0].astype(jnp.float32), to_right))
        value = dot(high, w_down[left])
        sums[1].wait_recv()
        sums.append(put_out(h, 5, value + sum_in[h, 1].astype(jnp.float32), to_left))

    back_out, back_in = s["back_out"], s["back_in"]

    def sums_end(h, hidden, sums):
        done = dot(hidden, w_down[x])
        back = [None]
        for k, (a, b) in enumerate(((3, 4), (2, 5))):
            sums[a].wait_recv()
            sums[b].wait_recv()
            total = done[k * cut : (k + 1) * cut]
            total += sum_in[h, a].astype(jnp.float32) + sum_in[h, b].astype(jnp.float32)
            back_out[h, k * half : (k + 1) * half] = total.astype(jnp.bfloat16).reshape(
                half, chunk, quarter
            )
            if k == 0:
                back_in[h, 0] = back_out[h, 0]
            back += [
                send(back_out.at[h, q], back_in.at[h, q], p_dev(np_ - q))
                for q in range(max(1, k * half), (k + 1) * half)
            ]
        return back[1:]

    def dense_hidden(h):
        arrive(pre_copies[h])
        pre = pre_out[h, x].astype(jnp.float32)
        for r in range(1, nx):
            pre += pre_in[h, r - 1].astype(jnp.float32)
        value = jax.nn.silu(pre[:, :hidden_here]) * pre[:, hidden_here:]
        hidden_x[h, x] = value.astype(jnp.bfloat16)
        return [send(hidden_x.at[h, x], hidden_x.at[h, x], x_dev(r)) for r in range(1, nx)]

    feeds = rows_to_experts(0)
    arrive(dense_copies)
    dense_sums(0, feeds)
    rows_over_x(0)
    feeds = rows_to_experts(1)
    dense_sums(1, feeds)
    pass_on(0)
    rows_over_x(1)
    hidden_copies = [dense_hidden(0)]
    held("expert_gate")
    held("expert_up")
    held("expert_down")
    hidden0 = expert_hidden(0)
    sums0 = sums_start(0, hidden0)
    pass_on(1)
    sums_pass_on(0, hidden0, sums0)
    hidden_copies.append(dense_hidden(1))
    hidden1 = expert_hidden(1)
    sums1 = sums_start(1, hidden1)
    backs = [sums_end(0, hidden0, sums0)]
    sums_pass_on(1, hidden1, sums1)

    arrive(pick_copies)
    j_col = iota((half_toks, rows), 1)
    same_block = block_of(j_col) == iota((half_toks, rows), 0) >> shift_of(toks)
    take, dense_part = [], []
    down = held("dense_down")[...].reshape(hidden_here, quarter)
    for h in range(2):
        table = pick_z[h * hz : (h + 1) * hz].reshape(half_toks, LANES)
        table_hi = table.astype(jnp.bfloat16)
        table_lo = (table - table_hi.astype(jnp.float32)).astype(jnp.bfloat16)
        here = (dot(codes[h], choose) == slot_of(j_col)) & same_block
        take.append(
            [
                jnp.where(here, dot(k, choose), 0.0).astype(jnp.bfloat16)
                for k in (table_hi, table_lo)
            ]
        )
        arrive(hidden_copies[h])
        value = hidden_x[h].astype(jnp.float32).reshape(nx, hz, own, hidden_here)
        value = value.swapaxes(0, 1).reshape(half_toks, hidden_here).astype(jnp.bfloat16)
        dense_part.append(dot(value, down) * table[:, experts : experts + 1])

    last_out, last_in = s["last_out"], s["last_in"]
    last, parts = [], []

    def give_back(h):
        arrive(backs[h])
        results = back_in[h].reshape(rows, quarter)
        part = dot(take[h][0], results) + dot(take[h][1], results) + dense_part[h]
        last_out[h * hz : (h + 1) * hz] = part.astype(jnp.bfloat16).reshape(hz, toks, quarter)
        last.extend(
            send(last_out.at[k], last_in.at[k - 1], z_dev(nz - order[k]))
            for k in range(max(1, h * hz), (h + 1) * hz)
        )
        return part

    combined = give_back(0)[:toks]
    backs.append(sums_end(1, hidden1, sums1))
    give_back(1)
    gain = in_row(held("out_gain"))
    arrive(stream_copies)
    stream_part = stream_in[...].astype(jnp.float32).reshape(toks, quarter)
    for k in range(1, nz):
        last[k - 1].wait_recv()
        combined += last_in[k - 1].astype(jnp.float32)

    square_x = s["square_x"]
    square = jnp.sum(combined * combined, axis=1, keepdims=True)
    on_lane = iota((toks, LANES), 0) == iota((toks, LANES), 1)
    as_row = jnp.sum(jnp.where(on_lane, square, 0.0), axis=0, keepdims=True)
    square_x[0] = jnp.broadcast_to(as_row, square_x.shape[1:])
    square_copies = [send(square_x.at[0], square_x.at[r], x_dev(r)) for r in range(1, nx)]
    combined = combined * gain
    arrive(square_copies)
    all_rows = square_x[0]
    for r in range(1, nx):
        all_rows += square_x[r]
    total_square = jnp.sum(jnp.where(on_lane, all_rows[0:1], 0.0), axis=1, keepdims=True)
    scale = lax.rsqrt(total_square / width + norm_eps)
    layer_out[...] = (stream_part + combined * scale).astype(jnp.bfloat16)

    for copy in started:
        copy.wait_send()
    for copy in small_out:
        copy.wait()


def copies_of(nz, np_, nx):
    x_copies = 6 * (nx - 1) + 4 * (nx - 1) + 4 * np_ + 2 * np_ + 12
    return x_copies + 4 * (nz - 1) + 7 * (np_ - 1)


def run_layer(sizes, p):
    nz, ny, nc, nx, cap = sizes
    np_ = ny * nc
    toks, width = p["resid"].shape
    own, quarter = toks // nx, width // nx
    hz = nz // 2
    bf16, f32 = jnp.bfloat16, jnp.float32
    share = p["expert_gate"].shape[2]
    hid = p["dense_gate"].shape[0]
    channels = p["conv_state"].shape[3]
    state_dim = p["scan_state"].shape[3]

    def tall(a):
        return a.reshape(-1, LANES)

    given = dict(p)
    for name in ("mix_gain", "post_gain", "ffn_gain", "dense_switch", "inner_gain", "out_gain"):
        given[name] = tall(p[name])
    for name in ("proj_step", "expert_router", "group_router", "route_experts"):
        given[name] = p[name].T
    given["resid"] = p["resid"].reshape(nx, own, width)
    given["conv_state"] = p["conv_state"].transpose(1, 2, 0, 3)
    given["scan_state"] = p["scan_state"].reshape(toks, channels, state_dim)
    for name in ("step_bias", "decay_rate"):
        given[name] = p[name].reshape(1, -1)
    given["expert_gate"] = p["expert_gate"].reshape(nx, quarter, share)
    given["expert_up"] = p["expert_up"].reshape(nx, quarter, share)
    given["expert_down"] = p["expert_down"].reshape(share, width)
    operands = [given[name] for name in OPERANDS]
    scratch = {}
    for name in OPERANDS:
        if name not in ("proj_x", "proj_b", "proj_c", "proj_z"):
            scratch[name] = (given[name].shape, given[name].dtype)
    for name in ("dense_gate", "dense_up", "dense_down"):
        scratch[name] = ((np_, hid, quarter), bf16)
    scratch["expert_down"] = ((nx, share, quarter), bf16)
    scratch["proj"] = ((width, 4 * channels), bf16)
    scratch["fresh"] = ((3, toks, channels), bf16)
    scratch["rows_ref"] = ((3, toks, channels), f32)
    scratch["c_ref"] = ((toks, channels), f32)
    scratch["old_read"] = ((toks, channels), f32)
    scratch["mixed_f"] = ((nx, own, width), f32)
    scratch["mixed_b"] = ((nx, own, width), bf16)
    scratch["mixed_in"] = ((nx - 1, own, width), bf16)
    for name in ("feed_out", "feed_in", "stream_out", "stream_in"):
        scratch[name] = ((nx, own, quarter), bf16)
    scratch["pick_in"] = ((nx, own, LANES), f32)
    scratch["pick_z"] = ((nz, toks, LANES), f32)
    scratch["code_z"] = ((nz, toks, LANES), bf16)
    scratch["feed_z"] = ((nz, toks, quarter), bf16)
    for name in ("rows_out", "rows_in", "back_out", "back_in"):
        scratch[name] = ((2, np_, hz * cap, quarter), bf16)
    scratch["rows_x"] = ((2, 3, np_, hz * cap, quarter), bf16)
    scratch["pre_out"] = ((2, nx, hz * own, 2 * np_ * hid), bf16)
    scratch["pre_in"] = ((2, nx - 1, hz * own, 2 * np_ * hid), bf16)
    scratch["hidden_x"] = ((2, nx, hz * own, np_ * hid), bf16)
    for name in ("sum_out", "sum_in"):
        scratch[name] = ((2, 6, np_ * hz * cap // 2, quarter), bf16)
    scratch["last_out"] = ((nz, toks, quarter), bf16)
    scratch["last_in"] = ((nz - 1, toks, quarter), bf16)
    scratch["square_x"] = ((nx, 8, LANES), f32)
    plan = tuple(scratch) + ("send_sem", "recv_sem", "local_sem")
    shapes = [pltpu.VMEM(*scratch[name]) for name in scratch]
    copies = copies_of(nz, np_, nx)
    shapes += [
        pltpu.SemaphoreType.DMA((copies,)),
        pltpu.SemaphoreType.DMA((copies,)),
        pltpu.SemaphoreType.DMA((len(OPERANDS) + nx + 1,)),
    ]
    anyw = pl.BlockSpec(memory_space=pl.ANY)
    return pl.pallas_call(
        functools.partial(layer, sizes, plan),
        out_shape=(
            jax.ShapeDtypeStruct((toks, quarter), bf16),
            jax.ShapeDtypeStruct((3, toks, channels), f32),
            jax.ShapeDtypeStruct((3, toks, channels), bf16),
        ),
        in_specs=[anyw] * len(operands),
        out_specs=(pl.BlockSpec(memory_space=pltpu.VMEM), anyw, anyw),
        scratch_shapes=shapes,
        compiler_params=pltpu.CompilerParams(
            collective_id=0, has_side_effects=True, vmem_limit_bytes=56 * 1024 * 1024
        ),
        name="layer",
    )(*operands)


def finish_step(rows, fresh, conv, result, state, new_state, new_conv, layer_out):
    @pl.when(pl.program_id(0) == 0)
    def _():
        layer_out[...] = result[...]
        new_conv[:, 0:2] = conv[:, 1:3]
        new_conv[:, 2] = fresh[...]

    keep, driven, bs = rows[0], rows[1], rows[2]
    channels = keep.shape[1]
    diag = iota((channels, channels), 0) == iota((channels, channels), 1)
    for t in range(state.shape[0]):
        at = slice(t, t + 1)
        keep_col = jnp.sum(jnp.where(diag, keep[at], 0.0), axis=1, keepdims=True)
        driven_col = jnp.sum(jnp.where(diag, driven[at], 0.0), axis=1, keepdims=True)
        new_state[t] = keep_col * state[t] + driven_col * bs[at]


def finish(rows, fresh, result, p):
    toks, heads, head_dim, state_dim = p["scan_state"].shape
    channels = heads * head_dim
    conv = p["conv_state"].transpose(1, 2, 0, 3)
    state = p["scan_state"].reshape(toks, channels, state_dim)
    block = 8
    whole = pl.BlockSpec(memory_space=pltpu.VMEM)
    piece = pl.BlockSpec((block, channels, state_dim), lambda i: (i, 0, 0))
    new_state, new_conv, layer_out = pl.pallas_call(
        finish_step,
        grid=(toks // block,),
        out_shape=(
            jax.ShapeDtypeStruct(state.shape, state.dtype),
            jax.ShapeDtypeStruct(conv.shape, conv.dtype),
            jax.ShapeDtypeStruct(result.shape, result.dtype),
        ),
        in_specs=[
            pl.BlockSpec((3, block, channels), lambda i: (0, i, 0)),
            whole,
            whole,
            whole,
            piece,
        ],
        out_specs=(piece, whole, whole),
        name="finish",
    )(rows, fresh, conv, result, state)
    return (
        layer_out,
        new_state.reshape(p["scan_state"].shape),
        new_conv.transpose(2, 0, 1, 3),
    )


NAMES = (
    "resid",
    "mix_gain",
    "proj_x",
    "proj_z",
    "proj_b",
    "proj_c",
    "proj_step",
    "step_bias",
    "decay_rate",
    "conv_taps",
    "conv_state",
    "scan_state",
    "inner_gain",
    "proj_out",
    "post_gain",
    "ffn_gain",
    "group_router",
    "expert_router",
    "route_experts",
    "expert_gate",
    "expert_up",
    "expert_down",
    "dense_switch",
    "dense_gate",
    "dense_up",
    "dense_down",
    "out_gain",
)


def on_device(*arrays):
    params = dict(zip(NAMES, arrays))
    sizes = tuple(lax.axis_size(a) for a in EP) + (lax.axis_size("tp"), CAPACITY)
    result, rows, fresh = run_layer(sizes, params)
    return finish(rows, fresh, result, params)


TORUS = (8, 4, 2)


def solution(mesh):
    torus = Mesh(mesh.devices.reshape(*TORUS, mesh.shape["tp"]), EP + ("tp",))
    in_specs = (
        P(EP, None),
        P(),
        P(None, "tp"),
        P(None, "tp"),
        P(None, "tp"),
        P(None, "tp"),
        P(),
        P("tp"),
        P("tp"),
        P(None, None, "tp"),
        P(EP, None, None, "tp"),
        P(EP, "tp", None, None),
        P("tp"),
        P("tp", None),
        P(),
        P(),
        P(),
        P(),
        P(EP, None),
        P(EP, None, "tp"),
        P(EP, None, "tp"),
        P(EP, "tp", None),
        P(),
        P(EP, "tp"),
        P(EP, "tp"),
        P(EP, "tp"),
        P("tp"),
    )
    out_specs = (P(EP, "tp"), P(EP, "tp", None, None), P(EP, None, None, "tp"))
    return jax.shard_map(
        on_device, mesh=torus, in_specs=in_specs, out_specs=out_specs, check_vma=False
    )
```

```python
import functools
from types import SimpleNamespace

import jax
import jax.numpy as jnp
from jax import lax
from jax.experimental import pallas as pl
from jax.experimental.pallas import tpu as pltpu
from jax.sharding import Mesh
from jax.sharding import PartitionSpec as P

EP = ("ep_0", "ep_1", "ep_2")
MESH = pl.DeviceIdType.MESH
norm_eps = 1e-06
CAPACITY = 4
LANES = 128


def dot(a, b):
    return jnp.dot(a, b, preferred_element_type=jnp.float32)


def dot_nt(a, b):
    return lax.dot_general(a, b, (((1,), (1,)), ((), ())), preferred_element_type=jnp.float32)


def in_row(gain_ref):
    gain = gain_ref[...].astype(jnp.float32)
    return jnp.concatenate([gain[i : i + 1] for i in range(gain.shape[0])], axis=1)


def iota(shape, dim):
    return lax.broadcasted_iota(jnp.int32, shape, dim)


def shift_of(count):
    return count.bit_length() - 1


def root_mean(values):
    return values * lax.rsqrt(jnp.mean(values * values, axis=-1, keepdims=True) + norm_eps)


def far_first(nz):
    return sorted(range(nz), key=lambda r: (-min(r, nz - r), r))


def layer(sizes, plan, *refs):
    nz, ny, nc, nx, cap = sizes
    np_ = ny * nc
    names, scratch = plan
    given = SimpleNamespace(**dict(zip(names, refs)))
    layer_out, state_rows, state_cols, fresh_out = refs[len(names) :][:4]
    send_sem, recv_sem, local_sem = refs[len(names) + 4 :][:3]
    s = SimpleNamespace(**dict(zip(scratch, refs[len(names) + 7 :])))
    z, y, c, x = (lax.axis_index(a) for a in ("ep_0", "ep_1", "ep_2", "tp"))
    place = y * nc + c
    own, width = given.resid.shape[1:]
    toks = own * nx
    quarter = width // nx
    hz = nz // 2
    half_toks = hz * toks
    chunk = hz * cap
    rows = np_ * chunk
    half = np_ // 2
    order = far_first(nz)
    here = order.index(0)
    others = [k for k in range(nz) if k != here]

    def z_dev(r):
        return {"ep_0": lax.rem(z + r, nz)}

    def p_dev(q):
        to = lax.rem(place + q, np_)
        return {"ep_1": to // nc, "ep_2": lax.rem(to, nc)}

    def x_dev(r):
        return {"tp": lax.rem(x + r, nx)}

    used = [0]
    started = []

    def send(src, dst, device):
        k = used[0]
        used[0] += 1
        copy = pltpu.make_async_remote_copy(
            src_ref=src,
            dst_ref=dst,
            send_sem=send_sem.at[k],
            recv_sem=recv_sem.at[k],
            device_id=device,
            device_id_type=MESH,
        )
        copy.start()
        started.append(copy)
        return copy

    local_used = [0]

    def fetch(src, dst):
        copy = pltpu.make_async_copy(src, dst, local_sem.at[local_used[0]])
        local_used[0] += 1
        copy.start()
        return copy

    def arrive(copies):
        for copy in copies:
            copy.wait_recv()

    barrier = pltpu.get_barrier_semaphore()
    peers = (
        [x_dev(r) for r in range(1, nx)]
        + [p_dev(q) for q in range(1, np_)]
        + [z_dev(r) for r in range(1, nz)]
    )
    for device in peers:
        pl.semaphore_signal(barrier, inc=1, device_id=device, device_id_type=MESH)

    def bring(*pairs):
        coming = [fetch(src, dst) for src, dst in pairs]

        def get():
            while coming:
                coming.pop().wait()
            return pairs[0][1]

        return get

    g, ready = given, SimpleNamespace()
    ready.route_experts = bring((g.route_experts, s.route_experts))
    ready.resid = bring((g.resid, s.resid))
    ready.mix_gain = bring((g.mix_gain, s.mix_gain))
    wide = g.proj_x.shape[1]
    ready.proj = bring(
        *(
            (one, s.proj.at[:, pl.ds(k * wide, wide)])
            for k, one in enumerate((g.proj_x, g.proj_b, g.proj_c, g.proj_z))
        )
    )
    ready.proj_step = bring((g.proj_step, s.proj_step))
    ready.conv_taps = bring((g.conv_taps, s.conv_taps))
    ready.conv_state = bring((g.conv_state, s.conv_state))
    ready.step_bias = bring((g.step_bias, s.step_bias))
    ready.decay_rate = bring((g.decay_rate, s.decay_rate))
    ready.scan_state = bring((g.scan_state, s.scan_state))
    ready.inner_gain = bring((g.inner_gain, s.inner_gain))
    ready.proj_out = bring((g.proj_out, s.proj_out))
    ready.post_gain = bring((g.post_gain, s.post_gain))
    ready.ffn_gain = bring((g.ffn_gain, s.ffn_gain))
    ready.expert_router = bring((g.expert_router, s.expert_router))
    ready.group_router = bring((g.group_router, s.group_router))
    ready.dense_switch = bring((g.dense_switch, s.dense_switch))
    ready.out_gain = bring((g.out_gain, s.out_gain))
    ready.dense_gate = bring((g.dense_gate, s.dense_gate.at[0]))
    ready.dense_up = bring((g.dense_up, s.dense_up.at[0]))
    ready.dense_down = bring((g.dense_down, s.dense_down.at[0]))
    ready.expert_gate = bring((g.expert_gate, s.expert_gate))
    ready.expert_up = bring((g.expert_up, s.expert_up))
    ready.expert_down = bring(
        *((g.expert_down.at[:, pl.ds(j * quarter, quarter)], s.expert_down.at[j]) for j in range(nx))
    )

    route_t = ready.route_experts()[...]
    picks = route_t.shape[0]
    expert_ids = iota((LANES, toks), 0)
    named = jnp.zeros((LANES, toks), jnp.float32)
    for k in range(picks):
        named += jnp.where(expert_ids == route_t[k : k + 1, :], 1.0, 0.0)
    named_b = named.astype(jnp.bfloat16)
    before = jnp.where(iota((toks, toks), 0) < iota((toks, toks), 1), 1.0, 0.0).astype(jnp.bfloat16)
    code_t = (named * (dot(named_b, before) + 1.0)).astype(jnp.bfloat16)
    eye = jnp.where(iota((toks, toks), 0) == iota((toks, toks), 1), 1.0, 0.0).astype(jnp.bfloat16)
    code_z = s.code_z
    code_z[here] = dot_nt(eye, code_t).astype(jnp.bfloat16)

    resid = ready.resid()
    gain = in_row(ready.mix_gain())
    normed = root_mean(resid[...].astype(jnp.float32).reshape(toks, width)) * gain
    normed = normed.astype(jnp.bfloat16)
    ready.proj()
    projected = dot(normed, s.proj[...])
    step_all = dot_nt(normed, ready.proj_step()[...])
    taps = ready.conv_taps()[...].astype(jnp.float32)
    old_conv = ready.conv_state()
    channels = taps.shape[2]
    acts = []
    fresh_ref = s.fresh
    for k in range(3):
        fresh = projected[:, k * channels : (k + 1) * channels].astype(jnp.bfloat16)
        fresh_ref[k] = fresh
        mixed_in = fresh.astype(jnp.float32) * taps[k, 3:4]
        for i in range(3):
            mixed_in += old_conv[k, i].astype(jnp.float32) * taps[k, i : i + 1]
        acts.append(jax.nn.silu(mixed_in))
    xs, bs, cs = acts
    gate_z = projected[:, 3 * channels :]
    bias, rate = ready.step_bias()[...], ready.decay_rate()[...]
    heads_here = bias.shape[1]
    head_dim = channels // heads_here
    head_of = iota((toks, channels), 1) >> shift_of(head_dim)
    head_col = iota(step_all.shape, 1)
    step = jnp.zeros((toks, channels), jnp.float32)
    keep = jnp.zeros((toks, channels), jnp.float32)
    rows_ref = s.rows_ref
    for h in range(heads_here):
        raw = jnp.sum(
            jnp.where(head_col == x * heads_here + h, step_all, 0.0), axis=1, keepdims=True
        )
        one = jax.nn.softplus(raw + bias[:, h : h + 1])
        step = jnp.where(head_of == h, one, step)
        kept = jnp.exp(-rate[:, h : h + 1] * one)
        keep = jnp.where(head_of == h, kept, keep)
        rows_ref[h] = jnp.broadcast_to(kept, (toks, channels))
    driven = step * xs
    rows_ref[heads_here] = bs
    s.cols_ref[...] = jnp.concatenate([driven] * (channels // toks), axis=0).T
    small_out = [
        fetch(rows_ref, state_rows),
        fetch(s.cols_ref, state_cols),
        fetch(fresh_ref, fresh_out),
    ]
    c_ref, old_read = s.c_ref, s.old_read
    c_ref[...] = cs
    diag = iota((channels, channels), 0) == iota((channels, channels), 1)
    old_state = ready.scan_state()

    @pl.loop(0, toks // 8)
    def _(i):
        at = pl.multiple_of(i * 8, 8)
        c8 = c_ref[pl.ds(at, 8), :]
        out = []
        for t in range(8):
            sums = jnp.sum(old_state[at + t] * c8[t : t + 1], axis=1, keepdims=True)
            out.append(jnp.sum(jnp.where(diag, sums, 0.0), axis=0, keepdims=True))
        old_read[pl.ds(at, 8), :] = jnp.concatenate(out, axis=0)

    read = keep * old_read[...] + driven * jnp.sum(bs * cs, axis=1, keepdims=True)
    gated = (read * jax.nn.silu(gate_z) * in_row(ready.inner_gain())).astype(jnp.bfloat16)

    mixed_f, mixed_b, mixed_in = s.mixed_f, s.mixed_b, s.mixed_in
    share = dot(gated, ready.proj_out()[...]).reshape(nx, own, width)
    mixed_f[...] = share
    mixed_b[...] = share.astype(jnp.bfloat16)

    pl.semaphore_wait(barrier, len(peers))

    copies = [
        send(mixed_b.at[lax.rem(x + r, nx)], mixed_in.at[r - 1], x_dev(r)) for r in range(1, nx)
    ]
    code_copies = [send(code_z.at[here], code_z.at[k], z_dev(order[k])) for k in others]
    dense_copies = []
    for one, all_here in (
        (g.dense_gate, s.dense_gate),
        (g.dense_up, s.dense_up),
        (g.dense_down, s.dense_down),
    ):
        dense_copies += [send(one, all_here.at[q], p_dev(q)) for q in range(1, np_)]

    post_gain, ffn_gain = in_row(ready.post_gain()), in_row(ready.ffn_gain())
    resid_own = resid[x].astype(jnp.float32)
    arrive(copies)
    mixed = mixed_f[x]
    for r in range(1, nx):
        mixed += mixed_in[r - 1].astype(jnp.float32)
    stream = (resid_own + root_mean(mixed) * post_gain).astype(jnp.bfloat16)
    feed = (root_mean(stream.astype(jnp.float32)) * ffn_gain).astype(jnp.bfloat16)
    feed_out, feed_in = s.feed_out, s.feed_in
    stream_out, stream_in = s.stream_out, s.stream_in
    for j in range(nx):
        feed_out[j] = feed[:, j * quarter : (j + 1) * quarter]
    feed_in[x] = feed_out[x]
    feed_copies = [
        send(feed_out.at[lax.rem(x + r, nx)], feed_in.at[x], x_dev(r)) for r in range(1, nx)
    ]
    for j in range(nx):
        stream_out[j] = stream[:, j * quarter : (j + 1) * quarter]

    feed_f = feed.astype(jnp.float32)
    expert_rows, group_rows = ready.expert_router(), ready.group_router()
    experts = expert_rows.shape[0]
    groups = group_rows.shape[0]
    group_size = experts // groups
    token_pick = jnp.where(iota((own, toks), 1) == iota((own, toks), 0) + x * own, 1.0, 0.0)
    own_route = dot_nt(token_pick.astype(jnp.bfloat16), route_t.astype(jnp.bfloat16))
    logits = dot_nt(feed, expert_rows[...])
    lanes = iota((own, experts), 1).astype(jnp.float32)
    weights = []
    for k in range(picks):
        chosen = jnp.sum(
            jnp.where(lanes == own_route[:, k : k + 1], logits, 0.0), axis=1, keepdims=True
        )
        weights.append(jnp.exp(chosen))
    total = functools.reduce(jnp.add, weights)
    group_f = group_rows[...].astype(jnp.float32)
    group_exp = [
        jnp.exp(jnp.sum(feed_f * group_f[g : g + 1], axis=1, keepdims=True)) for g in range(groups)
    ]
    group_total = functools.reduce(jnp.add, group_exp)
    first = own_route[:, 0:1]
    group_weight = jnp.zeros((own, 1), jnp.float32)
    for g in range(groups):
        in_group = (first >= g * group_size) & (first < (g + 1) * group_size)
        group_weight += jnp.where(in_group, group_exp[g] / group_total, 0.0)
    switch_row = in_row(ready.dense_switch())
    switch = jax.nn.sigmoid(jnp.sum(feed_f * switch_row, axis=1, keepdims=True))
    all_lanes = iota((own, LANES), 1).astype(jnp.float32)
    pick_table = jnp.where(all_lanes < experts, 0.0, switch)
    for k in range(picks):
        pick_table += jnp.where(
            all_lanes == own_route[:, k : k + 1], weights[k] / total * group_weight, 0.0
        )
    pick_in, pick_z = s.pick_in, s.pick_z
    pick_in[x] = pick_table

    arrive(feed_copies)
    feed_z = s.feed_z
    feed_z[here] = feed_in[...].astype(jnp.float32).reshape(toks, quarter).astype(jnp.bfloat16)
    feed_copies = [send(feed_z.at[here], feed_z.at[k], z_dev(order[k])) for k in others]
    pick_copies = [send(pick_in.at[x], pick_in.at[x], x_dev(r)) for r in range(1, nx)]
    stream_in[x] = stream_out[x]
    stream_copies = [
        send(stream_out.at[lax.rem(x + r, nx)], stream_in.at[x], x_dev(r)) for r in range(1, nx)
    ]

    def expert_of(j):
        return z * np_ + ((place + (j >> shift_of(chunk))) & (np_ - 1))

    def block_of(j):
        return (j & (chunk - 1)) >> shift_of(cap)

    def slot_of(j):
        return ((j & (cap - 1)) + 1).astype(jnp.float32)

    arrive(code_copies)
    codes = [
        code_z[h * hz : (h + 1) * hz].reshape(half_toks, LANES) for h in range(2)
    ]
    choose_t = jnp.where(
        iota((rows, LANES), 1) == expert_of(iota((rows, LANES), 0)), 1.0, 0.0
    ).astype(jnp.bfloat16)
    choose = jnp.where(
        iota((LANES, rows), 0) == expert_of(iota((LANES, rows), 1)), 1.0, 0.0
    ).astype(jnp.bfloat16)
    j_row = iota((rows, half_toks), 0)
    same_block = block_of(j_row) == iota((rows, half_toks), 1) >> shift_of(toks)
    put = [
        jnp.where((dot_nt(choose_t, k) == slot_of(j_row)) & same_block, 1.0, 0.0).astype(
            jnp.bfloat16
        )
        for k in codes
    ]

    arrive(pick_copies)
    pick_z[here] = pick_in[...].reshape(toks, LANES)
    pick_copies = [send(pick_z.at[here], pick_z.at[k], z_dev(order[k])) for k in others]

    rows_out, rows_in, rows_x = s.rows_out, s.rows_in, s.rows_x
    pre_out, pre_in, hidden_x = s.pre_out, s.pre_in, s.hidden_x
    hidden_here = s.dense_gate.shape[0] * s.dense_gate.shape[1]
    row_copies, pre_copies = [], []
    from_left, from_right, from_far = ([], []), ([], []), ([], [])

    def rows_to_experts(h):
        arrive(feed_copies[h * hz : (h + 1) * hz])
        feeds = feed_z[h * hz : (h + 1) * hz].reshape(half_toks, quarter)
        rows_out[h] = dot(put[h], feeds).astype(jnp.bfloat16).reshape(np_, chunk, quarter)
        rows_in[h, 0] = rows_out[h, 0]
        row_copies.append(
            [None] + [send(rows_out.at[h, q], rows_in.at[h, q], p_dev(q)) for q in range(1, np_)]
        )
        return feeds

    def dense_sums(h, feeds):
        ready.dense_gate()
        ready.dense_up()
        for k, weight in enumerate((s.dense_gate, s.dense_up)):
            part = dot_nt(feeds, weight[...].reshape(hidden_here, quarter))
            part = part.reshape(hz, nx, own, hidden_here).swapaxes(0, 1)
            part = part.reshape(nx, hz * own, hidden_here).astype(jnp.bfloat16)
            pre_out[h, :, :, k * hidden_here : (k + 1) * hidden_here] = part
        pre_copies.append(
            [
                send(pre_out.at[h, lax.rem(x + r, nx)], pre_in.at[h, r - 1], x_dev(r))
                for r in range(1, nx)
            ]
        )

    def rows_over_x(h):
        for q in range(np_):
            if q:
                row_copies[h][q].wait_recv()
            from_left[h].append(send(rows_in.at[h, q], rows_x.at[h, 0, q], x_dev(1)))
            from_right[h].append(send(rows_in.at[h, q], rows_x.at[h, 1, q], x_dev(nx - 1)))

    def pass_on(h):
        for q in range(half):
            from_left[h][q].wait_recv()
            from_far[h].append(send(rows_x.at[h, 0, q], rows_x.at[h, 2, q], x_dev(1)))
            k = half + q
            from_right[h][k].wait_recv()
            from_far[h].append(send(rows_x.at[h, 1, k], rows_x.at[h, 2, k], x_dev(nx - 1)))

    w_gate, w_up, w_down = s.expert_gate, s.expert_up, s.expert_down

    def of_share(taken, share):
        taken = taken.reshape(rows, quarter)
        return dot(taken, w_gate[share]), dot(taken, w_up[share])

    right, left, far = lax.rem(x + 1, nx), lax.rem(x + nx - 1, nx), lax.rem(x + 2, nx)

    def expert_hidden(h):
        gate_value, up_value = of_share(rows_in[h], x)
        arrive(from_left[h][half:])
        more = of_share(rows_x[h, 0], left)
        gate_value, up_value = gate_value + more[0], up_value + more[1]
        arrive(from_right[h][:half])
        more = of_share(rows_x[h, 1], right)
        gate_value, up_value = gate_value + more[0], up_value + more[1]
        arrive(from_far[h])
        more = of_share(rows_x[h, 2], far)
        gate_value, up_value = gate_value + more[0], up_value + more[1]
        return (jax.nn.silu(gate_value) * up_value).astype(jnp.bfloat16)

    sum_out, sum_in = s.sum_out, s.sum_in
    to_right, to_left = x_dev(1), x_dev(nx - 1)
    cut = rows // 2

    def put_out(h, k, values, device):
        sum_out[h, k] = values.astype(jnp.bfloat16)
        return send(sum_out.at[h, k], sum_in.at[h, k], device)

    def sums_start(h, hidden):
        low, high = hidden[:cut], hidden[cut:]
        return [
            put_out(h, 0, dot(low, w_down[far]), to_right),
            put_out(h, 1, dot(high, w_down[far]), to_left),
            put_out(h, 2, dot(high, w_down[right]), to_right),
            put_out(h, 3, dot(low, w_down[left]), to_left),
        ]

    def sums_pass_on(h, hidden, sums):
        low, high = hidden[:cut], hidden[cut:]
        value = dot(low, w_down[right])
        sums[0].wait_recv()
        sums.append(put_out(h, 4, value + sum_in[h, 0].astype(jnp.float32), to_right))
        value = dot(high, w_down[left])
        sums[1].wait_recv()
        sums.append(put_out(h, 5, value + sum_in[h, 1].astype(jnp.float32), to_left))

    back_out, back_in = s.back_out, s.back_in

    def sums_end(h, hidden, sums):
        done = dot(hidden, w_down[x])
        back = [None]
        for k, (a, b) in enumerate(((3, 4), (2, 5))):
            sums[a].wait_recv()
            sums[b].wait_recv()
            total = done[k * cut : (k + 1) * cut]
            total += sum_in[h, a].astype(jnp.float32) + sum_in[h, b].astype(jnp.float32)
            back_out[h, k * half : (k + 1) * half] = total.astype(jnp.bfloat16).reshape(
                half, chunk, quarter
            )
            if k == 0:
                back_in[h, 0] = back_out[h, 0]
            back += [
                send(back_out.at[h, q], back_in.at[h, q], p_dev(np_ - q))
                for q in range(max(1, k * half), (k + 1) * half)
            ]
        return back[1:]

    def dense_hidden(h):
        arrive(pre_copies[h])
        pre = pre_out[h, x].astype(jnp.float32)
        for r in range(1, nx):
            pre += pre_in[h, r - 1].astype(jnp.float32)
        value = jax.nn.silu(pre[:, :hidden_here]) * pre[:, hidden_here:]
        hidden_x[h, x] = value.astype(jnp.bfloat16)
        return [send(hidden_x.at[h, x], hidden_x.at[h, x], x_dev(r)) for r in range(1, nx)]

    feeds = rows_to_experts(0)
    arrive(dense_copies)
    dense_sums(0, feeds)
    feeds = rows_to_experts(1)
    dense_sums(1, feeds)
    rows_over_x(0)
    pass_on(0)
    rows_over_x(1)
    hidden_copies = [dense_hidden(0)]
    ready.expert_gate()
    ready.expert_up()
    ready.expert_down()
    hidden0 = expert_hidden(0)
    sums0 = sums_start(0, hidden0)
    pass_on(1)
    sums_pass_on(0, hidden0, sums0)
    hidden_copies.append(dense_hidden(1))
    hidden1 = expert_hidden(1)
    sums1 = sums_start(1, hidden1)
    backs = [sums_end(0, hidden0, sums0)]
    sums_pass_on(1, hidden1, sums1)

    arrive(pick_copies)
    j_col = iota((half_toks, rows), 1)
    same_block = block_of(j_col) == iota((half_toks, rows), 0) >> shift_of(toks)
    take, dense_part = [], []
    ready.dense_down()
    down = s.dense_down[...].reshape(hidden_here, quarter)
    for h in range(2):
        table = pick_z[h * hz : (h + 1) * hz].reshape(half_toks, LANES)
        table_hi = table.astype(jnp.bfloat16)
        table_lo = (table - table_hi.astype(jnp.float32)).astype(jnp.bfloat16)
        taken = (dot(codes[h], choose) == slot_of(j_col)) & same_block
        take.append(
            [
                jnp.where(taken, dot(k, choose), 0.0).astype(jnp.bfloat16)
                for k in (table_hi, table_lo)
            ]
        )
        arrive(hidden_copies[h])
        value = hidden_x[h].astype(jnp.float32).reshape(nx, hz, own, hidden_here)
        value = value.swapaxes(0, 1).reshape(half_toks, hidden_here).astype(jnp.bfloat16)
        dense_part.append(dot(value, down) * table[:, experts : experts + 1])

    last_out, last_in = s.last_out, s.last_in
    last, parts = [], []

    def give_back(h):
        arrive(backs[h])
        results = back_in[h].reshape(rows, quarter)
        part = dot(take[h][0], results) + dot(take[h][1], results) + dense_part[h]
        last_out[h * hz : (h + 1) * hz] = part.astype(jnp.bfloat16).reshape(hz, toks, quarter)
        last.extend(
            send(last_out.at[k], last_in.at[k], z_dev(nz - order[k]))
            for k in others[h * hz : (h + 1) * hz]
        )
        return part

    give_back(0)
    backs.append(sums_end(1, hidden1, sums1))
    combined = give_back(1)[(here - hz) * toks : (here - hz + 1) * toks]
    gain = in_row(ready.out_gain())
    arrive(stream_copies)
    stream_part = stream_in[...].astype(jnp.float32).reshape(toks, quarter)
    for k in others:
        last[k].wait_recv()
        combined += last_in[k].astype(jnp.float32)

    square_x = s.square_x
    square = jnp.sum(combined * combined, axis=1, keepdims=True)
    on_lane = iota((toks, LANES), 0) == iota((toks, LANES), 1)
    as_row = jnp.sum(jnp.where(on_lane, square, 0.0), axis=0, keepdims=True)
    square_x[0] = jnp.broadcast_to(as_row, square_x.shape[1:])
    square_copies = [send(square_x.at[0], square_x.at[r], x_dev(r)) for r in range(1, nx)]
    combined = combined * gain
    arrive(square_copies)
    all_rows = square_x[0]
    for r in range(1, nx):
        all_rows += square_x[r]
    total_square = jnp.sum(jnp.where(on_lane, all_rows[0:1], 0.0), axis=1, keepdims=True)
    scale = lax.rsqrt(total_square / width + norm_eps)
    layer_out[...] = (stream_part + combined * scale).astype(jnp.bfloat16)

    for copy in started:
        copy.wait_send()
    for copy in small_out:
        copy.wait()


def copies_of(nz, np_, nx):
    x_copies = 6 * (nx - 1) + 4 * (nx - 1) + 4 * np_ + 2 * np_ + 12
    return x_copies + 4 * (nz - 1) + 7 * (np_ - 1)


def run_layer(sizes, p):
    nz, ny, nc, nx, cap = sizes
    np_ = ny * nc
    toks, width = p.resid.shape
    own, quarter = toks // nx, width // nx
    hz = nz // 2
    bf16, f32 = jnp.bfloat16, jnp.float32
    share = p.expert_gate.shape[2]
    hid = p.dense_gate.shape[0]
    channels = p.conv_state.shape[3]
    state_dim = p.scan_state.shape[3]

    def tall(a):
        return a.reshape(-1, LANES)

    g = SimpleNamespace(**vars(p))
    g.mix_gain, g.post_gain, g.ffn_gain = tall(p.mix_gain), tall(p.post_gain), tall(p.ffn_gain)
    g.dense_switch, g.inner_gain = tall(p.dense_switch), tall(p.inner_gain)
    g.out_gain = tall(p.out_gain)
    g.proj_step, g.expert_router = p.proj_step.T, p.expert_router.T
    g.group_router, g.route_experts = p.group_router.T, p.route_experts.T
    g.resid = p.resid.reshape(nx, own, width)
    g.conv_state = p.conv_state.transpose(1, 2, 0, 3)
    g.scan_state = p.scan_state.reshape(toks, channels, state_dim)
    g.step_bias, g.decay_rate = p.step_bias.reshape(1, -1), p.decay_rate.reshape(1, -1)
    g.expert_gate = p.expert_gate.reshape(nx, quarter, share)
    g.expert_up = p.expert_up.reshape(nx, quarter, share)
    g.expert_down = p.expert_down.reshape(share, width)
    names = tuple(vars(g))
    operands = list(vars(g).values())
    s = SimpleNamespace(**{k: pltpu.VMEM(v.shape, v.dtype) for k, v in vars(g).items()})
    s.dense_gate = s.dense_up = s.dense_down = pltpu.VMEM((np_, hid, quarter), bf16)
    s.expert_down = pltpu.VMEM((nx, share, quarter), bf16)
    s.proj_x = s.proj_b = s.proj_c = s.proj_z = pltpu.VMEM((8, LANES), f32)
    s.proj = pltpu.VMEM((width, 4 * channels), bf16)
    s.fresh = pltpu.VMEM((3, toks, channels), bf16)
    state_rows = (p.scan_state.shape[1] + 1, toks, channels)
    s.rows_ref = pltpu.VMEM(state_rows, f32)
    s.cols_ref = pltpu.VMEM((channels, channels), f32)
    s.c_ref = s.old_read = pltpu.VMEM((toks, channels), f32)
    s.mixed_f = pltpu.VMEM((nx, own, width), f32)
    s.mixed_b = pltpu.VMEM((nx, own, width), bf16)
    s.mixed_in = pltpu.VMEM((nx - 1, own, width), bf16)
    s.feed_out = s.feed_in = pltpu.VMEM((nx, own, quarter), bf16)
    s.stream_out = s.stream_in = pltpu.VMEM((nx, own, quarter), bf16)
    s.pick_in = pltpu.VMEM((nx, own, LANES), f32)
    s.pick_z = pltpu.VMEM((nz, toks, LANES), f32)
    s.code_z = pltpu.VMEM((nz, toks, LANES), bf16)
    s.feed_z = pltpu.VMEM((nz, toks, quarter), bf16)
    s.rows_out = s.rows_in = pltpu.VMEM((2, np_, hz * cap, quarter), bf16)
    s.back_out = s.back_in = pltpu.VMEM((2, np_, hz * cap, quarter), bf16)
    s.rows_x = pltpu.VMEM((2, 3, np_, hz * cap, quarter), bf16)
    s.pre_out = pltpu.VMEM((2, nx, hz * own, 2 * np_ * hid), bf16)
    s.pre_in = pltpu.VMEM((2, nx - 1, hz * own, 2 * np_ * hid), bf16)
    s.hidden_x = pltpu.VMEM((2, nx, hz * own, np_ * hid), bf16)
    s.sum_out = s.sum_in = pltpu.VMEM((2, 6, np_ * hz * cap // 2, quarter), bf16)
    s.last_out = pltpu.VMEM((nz, toks, quarter), bf16)
    s.last_in = pltpu.VMEM((nz, toks, quarter), bf16)
    s.square_x = pltpu.VMEM((nx, 8, LANES), f32)
    plan = names, tuple(vars(s))
    copies = copies_of(nz, np_, nx)
    shapes = [
        pltpu.SemaphoreType.DMA((copies,)),
        pltpu.SemaphoreType.DMA((copies,)),
        pltpu.SemaphoreType.DMA((len(names) + nx + 2,)),
        *vars(s).values(),
    ]
    anyw = pl.BlockSpec(memory_space=pl.ANY)
    return pl.pallas_call(
        functools.partial(layer, sizes, plan),
        out_shape=(
            jax.ShapeDtypeStruct((toks, quarter), bf16),
            jax.ShapeDtypeStruct(state_rows, f32),
            jax.ShapeDtypeStruct((channels, channels), f32),
            jax.ShapeDtypeStruct((3, toks, channels), bf16),
        ),
        in_specs=[anyw] * len(operands),
        out_specs=(pl.BlockSpec(memory_space=pltpu.VMEM), anyw, anyw, anyw),
        scratch_shapes=shapes,
        compiler_params=pltpu.CompilerParams(
            collective_id=0, has_side_effects=True, vmem_limit_bytes=56 * 1024 * 1024
        ),
        name="layer",
    )(*operands)


def finish_step(
    rows_in,
    cols_in,
    fresh_in,
    conv,
    result,
    state,
    new_state,
    new_conv,
    layer_out,
    rows,
    cols,
    fresh,
    conv_v,
    result_v,
    state_v,
    sem,
):
    used = [0]

    def move(src, dst):
        copy = pltpu.make_async_copy(src, dst, sem.at[used[0]])
        used[0] += 1
        copy.start()
        return copy

    toks = state.shape[0]
    heads = rows.shape[0] - 1
    block = 8
    pieces = [pl.ds(i, block) for i in range(0, toks, block)]
    small = [move(rows_in, rows), move(cols_in, cols)]
    states = [move(state.at[at], state_v.at[at]) for at in pieces]
    others = [move(result, result_v), move(conv, conv_v), move(fresh_in, fresh)]
    for copy in small:
        copy.wait()
    head_dim = cols.shape[0] // heads
    out = []
    for i, at in enumerate(pieces):
        states[i].wait()
        for t in range(i * block, (i + 1) * block):
            new = slice(t, t + 1)
            for h in range(heads):
                part = slice(h * head_dim, (h + 1) * head_dim)
                added = cols[part, new] * rows[heads, new]
                state_v[t, part] = rows[h, new] * state_v[t, part] + added
        out.append(move(state_v.at[at], new_state.at[at]))
        if i == 0:
            for copy in others:
                copy.wait()
            out.append(move(result_v, layer_out))
            for k in range(3):
                out.append(move(conv_v.at[k, pl.ds(1, 2)], new_conv.at[k, pl.ds(0, 2)]))
                out.append(move(fresh.at[k], new_conv.at[k, 2]))
    for copy in out:
        copy.wait()


def finish(result, rows, cols, fresh, p):
    toks, heads, head_dim, state_dim = p.scan_state.shape
    channels = heads * head_dim
    conv = p.conv_state.transpose(1, 2, 0, 3)
    state = p.scan_state.reshape(toks, channels, state_dim)
    anyw = pl.BlockSpec(memory_space=pl.ANY)
    operands = (rows, cols, fresh, conv, result, state)
    new_state, new_conv, layer_out = pl.pallas_call(
        finish_step,
        out_shape=tuple(jax.ShapeDtypeStruct(a.shape, a.dtype) for a in (state, conv, result)),
        in_specs=[anyw] * 6,
        out_specs=(anyw,) * 3,
        scratch_shapes=[pltpu.VMEM(a.shape, a.dtype) for a in operands]
        + [pltpu.SemaphoreType.DMA((5 + 2 * (toks // 8) + 7,))],
        name="finish",
    )(*operands)
    return (
        layer_out,
        new_state.reshape(p.scan_state.shape),
        new_conv.transpose(2, 0, 1, 3),
    )


def on_device(
    resid,
    mix_gain,
    proj_x,
    proj_z,
    proj_b,
    proj_c,
    proj_step,
    step_bias,
    decay_rate,
    conv_taps,
    conv_state,
    scan_state,
    inner_gain,
    proj_out,
    post_gain,
    ffn_gain,
    group_router,
    expert_router,
    route_experts,
    expert_gate,
    expert_up,
    expert_down,
    dense_switch,
    dense_gate,
    dense_up,
    dense_down,
    out_gain,
):
    params = SimpleNamespace(**locals())
    sizes = tuple(lax.axis_size(a) for a in EP) + (lax.axis_size("tp"), CAPACITY)
    return finish(*run_layer(sizes, params), params)


TORUS = (8, 4, 2)


def solution(mesh):
    torus = Mesh(mesh.devices.reshape(*TORUS, mesh.shape["tp"]), EP + ("tp",))
    in_specs = (
        P(EP, None),
        P(),
        P(None, "tp"),
        P(None, "tp"),
        P(None, "tp"),
        P(None, "tp"),
        P(),
        P("tp"),
        P("tp"),
        P(None, None, "tp"),
        P(EP, None, None, "tp"),
        P(EP, "tp", None, None),
        P("tp"),
        P("tp", None),
        P(),
        P(),
        P(),
        P(),
        P(EP, None),
        P(EP, None, "tp"),
        P(EP, None, "tp"),
        P(EP, "tp", None),
        P(),
        P(EP, "tp"),
        P(EP, "tp"),
        P(EP, "tp"),
        P("tp"),
    )
    out_specs = (P(EP, "tp"), P(EP, "tp", None, None), P(EP, None, None, "tp"))
    return jax.shard_map(
        on_device, mesh=torus, in_specs=in_specs, out_specs=out_specs, check_vma=False
    )
```

```python
import functools
from types import SimpleNamespace

import jax
import jax.numpy as jnp
from jax import lax
from jax.experimental import pallas as pl
from jax.experimental.pallas import tpu as pltpu
from jax.sharding import Mesh
from jax.sharding import PartitionSpec as P

EP = ("ep_0", "ep_1", "ep_2")
MESH = pl.DeviceIdType.MESH
norm_eps = 1e-06
CAPACITY = 4
LANES = 128


def dot(a, b):
    return jnp.dot(a, b, preferred_element_type=jnp.float32)


def dot_nt(a, b):
    return lax.dot_general(a, b, (((1,), (1,)), ((), ())), preferred_element_type=jnp.float32)


def in_row(gain_ref):
    gain = gain_ref[...].astype(jnp.float32)
    return jnp.concatenate([gain[i : i + 1] for i in range(gain.shape[0])], axis=1)


def iota(shape, dim):
    return lax.broadcasted_iota(jnp.int32, shape, dim)


def shift_of(count):
    return count.bit_length() - 1


def root_mean(values):
    return values * lax.rsqrt(jnp.mean(values * values, axis=-1, keepdims=True) + norm_eps)


def far_first(nz):
    return sorted(range(nz), key=lambda r: (-min(r, nz - r), r))


def layer(sizes, plan, *refs):
    nz, ny, nc, nx, cap = sizes
    np_ = ny * nc
    names, scratch = plan
    given = SimpleNamespace(**dict(zip(names, refs)))
    layer_out, state_rows, state_cols, fresh_out = refs[len(names) :][:4]
    send_sem, recv_sem, local_sem = refs[len(names) + 4 :][:3]
    s = SimpleNamespace(**dict(zip(scratch, refs[len(names) + 7 :])))
    z, y, c, x = (lax.axis_index(a) for a in ("ep_0", "ep_1", "ep_2", "tp"))
    place = y * nc + c
    own, width = given.resid.shape[1:]
    toks = own * nx
    quarter = width // nx
    hz = nz // 2
    half_toks = hz * toks
    chunk = hz * cap
    rows = np_ * chunk
    half = np_ // 2
    order = far_first(nz)
    here = order.index(0)
    others = [k for k in range(nz) if k != here]

    def z_dev(r):
        return {"ep_0": lax.rem(z + r, nz)}

    def p_dev(q):
        to = lax.rem(place + q, np_)
        return {"ep_1": to // nc, "ep_2": lax.rem(to, nc)}

    def x_dev(r):
        return {"tp": lax.rem(x + r, nx)}

    used = SimpleNamespace(send=0, recv=0)
    at_end = []

    def take_of(whole, sem):
        return lambda: pltpu.make_async_copy(whole, whole, sem).wait()

    class Group:
        def __init__(self, whole):
            self.out_sem, self.in_sem = send_sem.at[used.send], recv_sem.at[used.recv]
            used.send += 1
            used.recv += 1
            self.arrived = take_of(whole, self.in_sem)
            at_end.append(take_of(whole, self.out_sem))

        def start(self, src, dst, device, in_sem=None):
            pltpu.make_async_remote_copy(
                src_ref=src,
                dst_ref=dst,
                send_sem=self.out_sem,
                recv_sem=self.in_sem if in_sem is None else in_sem,
                device_id=device,
                device_id_type=MESH,
            ).start()

    def send(copies, whole, apart=False):
        if not copies:
            return []
        group = Group(whole)
        waits = []
        for k, (src, dst, device) in enumerate(copies):
            in_sem = group.in_sem
            if apart and k:
                in_sem = recv_sem.at[used.recv]
                used.recv += 1
            group.start(src, dst, device, in_sem)
            waits.append(take_of(dst, in_sem))
        return waits if apart else [group.arrived]

    local_used = [0]

    def fetch(src, dst, sem=None):
        if sem is None:
            sem = local_sem.at[local_used[0]]
            local_used[0] += 1
        copy = pltpu.make_async_copy(src, dst, sem)
        copy.start()
        return copy

    def arrive(waits):
        for wait in waits:
            wait()

    barrier = pltpu.get_barrier_semaphore()
    peers = (
        [x_dev(r) for r in range(1, nx)]
        + [p_dev(q) for q in range(1, np_)]
        + [z_dev(r) for r in range(1, nz)]
    )
    for device in peers:
        pl.semaphore_signal(barrier, inc=1, device_id=device, device_id_type=MESH)

    def bring(*pairs):
        coming = [fetch(src, dst) for src, dst in pairs]

        def get():
            while coming:
                coming.pop().wait()
            return pairs[0][1]

        return get

    g, ready = given, SimpleNamespace()
    ready.route_experts = bring((g.route_experts, s.route_experts))
    ready.resid = bring((g.resid, s.resid))
    ready.mix_gain = bring((g.mix_gain, s.mix_gain))
    wide = g.proj_x.shape[1]
    proj_sem = local_sem.at[local_used[0]]
    local_used[0] += 1
    for k, one in enumerate((g.proj_x, g.proj_b, g.proj_c, g.proj_z)):
        fetch(one, s.proj.at[:, pl.ds(k * wide, wide)], proj_sem)
    ready.proj_step = bring((g.proj_step, s.proj_step))
    ready.conv_taps = bring((g.conv_taps, s.conv_taps))
    ready.conv_state = bring((g.conv_state, s.conv_state))
    ready.step_bias = bring((g.step_bias, s.step_bias))
    ready.decay_rate = bring((g.decay_rate, s.decay_rate))
    ready.scan_state = bring((g.scan_state, s.scan_state))
    ready.inner_gain = bring((g.inner_gain, s.inner_gain))
    ready.proj_out = bring((g.proj_out, s.proj_out))
    ready.post_gain = bring((g.post_gain, s.post_gain))
    ready.ffn_gain = bring((g.ffn_gain, s.ffn_gain))
    ready.expert_router = bring((g.expert_router, s.expert_router))
    ready.group_router = bring((g.group_router, s.group_router))
    ready.dense_switch = bring((g.dense_switch, s.dense_switch))
    ready.out_gain = bring((g.out_gain, s.out_gain))
    ready.dense_gate = bring((g.dense_gate, s.dense_gate.at[0]))
    ready.dense_up = bring((g.dense_up, s.dense_up.at[0]))
    ready.dense_down = bring((g.dense_down, s.dense_down.at[0]))
    ready.expert_gate = bring((g.expert_gate, s.expert_gate))
    ready.expert_up = bring((g.expert_up, s.expert_up))
    down_sem = local_sem.at[local_used[0]]
    local_used[0] += 1
    for j in range(nx):
        fetch(g.expert_down.at[:, pl.ds(j * quarter, quarter)], s.expert_down.at[j], down_sem)

    route_t = ready.route_experts()[...]
    picks = route_t.shape[0]
    expert_ids = iota((LANES, toks), 0)
    named = jnp.zeros((LANES, toks), jnp.float32)
    for k in range(picks):
        named += jnp.where(expert_ids == route_t[k : k + 1, :], 1.0, 0.0)
    named_b = named.astype(jnp.bfloat16)
    before = jnp.where(iota((toks, toks), 0) < iota((toks, toks), 1), 1.0, 0.0).astype(jnp.bfloat16)
    code_t = (named * (dot(named_b, before) + 1.0)).astype(jnp.bfloat16)
    eye = jnp.where(iota((toks, toks), 0) == iota((toks, toks), 1), 1.0, 0.0).astype(jnp.bfloat16)
    code_z = s.code_z
    code_z[here] = dot_nt(eye, code_t).astype(jnp.bfloat16)

    resid = ready.resid()
    gain = in_row(ready.mix_gain())
    normed = root_mean(resid[...].astype(jnp.float32).reshape(toks, width)) * gain
    normed = normed.astype(jnp.bfloat16)
    take_of(s.proj, proj_sem)()
    projected = dot(normed, s.proj[...])
    step_all = dot_nt(normed, ready.proj_step()[...])
    taps = ready.conv_taps()[...].astype(jnp.float32)
    old_conv = ready.conv_state()
    channels = taps.shape[2]
    acts = []
    fresh_ref = s.fresh
    for k in range(3):
        fresh = projected[:, k * channels : (k + 1) * channels].astype(jnp.bfloat16)
        fresh_ref[k] = fresh
        mixed_in = fresh.astype(jnp.float32) * taps[k, 3:4]
        for i in range(3):
            mixed_in += old_conv[k, i].astype(jnp.float32) * taps[k, i : i + 1]
        acts.append(jax.nn.silu(mixed_in))
    xs, bs, cs = acts
    gate_z = projected[:, 3 * channels :]
    bias, rate = ready.step_bias()[...], ready.decay_rate()[...]
    heads_here = bias.shape[1]
    head_dim = channels // heads_here
    head_of = iota((toks, channels), 1) >> shift_of(head_dim)
    head_col = iota(step_all.shape, 1)
    step = jnp.zeros((toks, channels), jnp.float32)
    keep = jnp.zeros((toks, channels), jnp.float32)
    rows_ref = s.rows_ref
    for h in range(heads_here):
        raw = jnp.sum(
            jnp.where(head_col == x * heads_here + h, step_all, 0.0), axis=1, keepdims=True
        )
        one = jax.nn.softplus(raw + bias[:, h : h + 1])
        step = jnp.where(head_of == h, one, step)
        kept = jnp.exp(-rate[:, h : h + 1] * one)
        keep = jnp.where(head_of == h, kept, keep)
        rows_ref[h] = jnp.broadcast_to(kept, (toks, channels))
    driven = step * xs
    rows_ref[heads_here] = bs
    s.cols_ref[...] = jnp.concatenate([driven] * (channels // toks), axis=0).T
    small_out = [
        fetch(rows_ref, state_rows),
        fetch(s.cols_ref, state_cols),
        fetch(fresh_ref, fresh_out),
    ]
    c_ref, old_read = s.c_ref, s.old_read
    c_ref[...] = cs
    diag = iota((channels, channels), 0) == iota((channels, channels), 1)
    old_state = ready.scan_state()

    @pl.loop(0, toks // 8)
    def _(i):
        at = pl.multiple_of(i * 8, 8)
        c8 = c_ref[pl.ds(at, 8), :]
        out = []
        for t in range(8):
            sums = jnp.sum(old_state[at + t] * c8[t : t + 1], axis=1, keepdims=True)
            out.append(jnp.sum(jnp.where(diag, sums, 0.0), axis=0, keepdims=True))
        old_read[pl.ds(at, 8), :] = jnp.concatenate(out, axis=0)

    read = keep * old_read[...] + driven * jnp.sum(bs * cs, axis=1, keepdims=True)
    gated = (read * jax.nn.silu(gate_z) * in_row(ready.inner_gain())).astype(jnp.bfloat16)

    mixed_f, mixed_b, mixed_in = s.mixed_f, s.mixed_b, s.mixed_in
    share = dot(gated, ready.proj_out()[...]).reshape(nx, own, width)
    mixed_f[...] = share
    mixed_b[...] = share.astype(jnp.bfloat16)

    pl.semaphore_wait(barrier, len(peers))

    copies = send(
        [(mixed_b.at[lax.rem(x + r, nx)], mixed_in.at[r - 1], x_dev(r)) for r in range(1, nx)],
        mixed_in,
    )
    code_copies = send(
        [(code_z.at[here], code_z.at[k], z_dev(order[k])) for k in others],
        code_z.at[pl.ds(0, nz - 1)],
    )
    dense_copies = []
    for one, all_here in (
        (g.dense_gate, s.dense_gate),
        (g.dense_up, s.dense_up),
        (g.dense_down, s.dense_down),
    ):
        dense_copies += send(
            [(one, all_here.at[q], p_dev(q)) for q in range(1, np_)],
            all_here.at[pl.ds(1, np_ - 1)],
        )

    post_gain, ffn_gain = in_row(ready.post_gain()), in_row(ready.ffn_gain())
    resid_own = resid[x].astype(jnp.float32)
    arrive(copies)
    mixed = mixed_f[x]
    for r in range(1, nx):
        mixed += mixed_in[r - 1].astype(jnp.float32)
    stream = (resid_own + root_mean(mixed) * post_gain).astype(jnp.bfloat16)
    feed = (root_mean(stream.astype(jnp.float32)) * ffn_gain).astype(jnp.bfloat16)
    feed_out, feed_in = s.feed_out, s.feed_in
    stream_out, stream_in = s.stream_out, s.stream_in
    for j in range(nx):
        feed_out[j] = feed[:, j * quarter : (j + 1) * quarter]
    far = lax.rem(x + 2, nx)
    far_in = s.far_in
    feed_in[x] = feed_out[x]
    far_in[x] = feed_out[far]
    feed_copies = send(
        [(feed_out.at[lax.rem(x + r, nx)], feed_in.at[x], x_dev(r)) for r in range(1, nx)],
        feed_in.at[pl.ds(0, nx - 1)],
    )
    far_copies = send(
        [(feed_out.at[lax.rem(x + r + 2, nx)], far_in.at[x], x_dev(r)) for r in range(1, nx)],
        far_in.at[pl.ds(0, nx - 1)],
    )
    for j in range(nx):
        stream_out[j] = stream[:, j * quarter : (j + 1) * quarter]

    feed_f = feed.astype(jnp.float32)
    expert_rows, group_rows = ready.expert_router(), ready.group_router()
    experts = expert_rows.shape[0]
    groups = group_rows.shape[0]
    group_size = experts // groups
    token_pick = jnp.where(iota((own, toks), 1) == iota((own, toks), 0) + x * own, 1.0, 0.0)
    own_route = dot_nt(token_pick.astype(jnp.bfloat16), route_t.astype(jnp.bfloat16))
    logits = dot_nt(feed, expert_rows[...])
    lanes = iota((own, experts), 1).astype(jnp.float32)
    weights = []
    for k in range(picks):
        chosen = jnp.sum(
            jnp.where(lanes == own_route[:, k : k + 1], logits, 0.0), axis=1, keepdims=True
        )
        weights.append(jnp.exp(chosen))
    total = functools.reduce(jnp.add, weights)
    group_f = group_rows[...].astype(jnp.float32)
    group_exp = [
        jnp.exp(jnp.sum(feed_f * group_f[g : g + 1], axis=1, keepdims=True)) for g in range(groups)
    ]
    group_total = functools.reduce(jnp.add, group_exp)
    first = own_route[:, 0:1]
    group_weight = jnp.zeros((own, 1), jnp.float32)
    for g in range(groups):
        in_group = (first >= g * group_size) & (first < (g + 1) * group_size)
        group_weight += jnp.where(in_group, group_exp[g] / group_total, 0.0)
    switch_row = in_row(ready.dense_switch())
    switch = jax.nn.sigmoid(jnp.sum(feed_f * switch_row, axis=1, keepdims=True))
    all_lanes = iota((own, LANES), 1).astype(jnp.float32)
    pick_table = jnp.where(all_lanes < experts, 0.0, switch)
    for k in range(picks):
        pick_table += jnp.where(
            all_lanes == own_route[:, k : k + 1], weights[k] / total * group_weight, 0.0
        )
    pick_in, pick_z = s.pick_in, s.pick_z
    pick_in[x] = pick_table

    arrive(feed_copies)
    feed_z, far_z = s.feed_z, s.far_z
    feed_z[here] = feed_in[...].astype(jnp.float32).reshape(toks, quarter).astype(jnp.bfloat16)

    def to_z(ref, ks):
        return send(
            [(ref.at[here], ref.at[k], z_dev(order[k])) for k in ks], ref.at[pl.ds(0, len(ks))]
        )

    feed_copies = [to_z(feed_z, others[:hz]), to_z(feed_z, others[hz:])]
    arrive(far_copies)
    far_z[here] = far_in[...].astype(jnp.float32).reshape(toks, quarter).astype(jnp.bfloat16)
    far_copies = to_z(far_z, others)
    pick_copies = send(
        [(pick_in.at[x], pick_in.at[x], x_dev(r)) for r in range(1, nx)],
        pick_in.at[pl.ds(0, nx - 1)],
    )
    stream_in[x] = stream_out[x]
    stream_copies = send(
        [(stream_out.at[lax.rem(x + r, nx)], stream_in.at[x], x_dev(r)) for r in range(1, nx)],
        stream_in.at[pl.ds(0, nx - 1)],
    )

    def expert_of(j):
        return z * np_ + ((place + (j >> shift_of(chunk))) & (np_ - 1))

    def block_of(j):
        return (j & (chunk - 1)) >> shift_of(cap)

    def slot_of(j):
        return ((j & (cap - 1)) + 1).astype(jnp.float32)

    arrive(code_copies)
    codes = [
        code_z[h * hz : (h + 1) * hz].reshape(half_toks, LANES) for h in range(2)
    ]
    choose_t = jnp.where(
        iota((rows, LANES), 1) == expert_of(iota((rows, LANES), 0)), 1.0, 0.0
    ).astype(jnp.bfloat16)
    choose = jnp.where(
        iota((LANES, rows), 0) == expert_of(iota((LANES, rows), 1)), 1.0, 0.0
    ).astype(jnp.bfloat16)
    j_row = iota((rows, half_toks), 0)
    same_block = block_of(j_row) == iota((rows, half_toks), 1) >> shift_of(toks)
    put = [
        jnp.where((dot_nt(choose_t, k) == slot_of(j_row)) & same_block, 1.0, 0.0).astype(
            jnp.bfloat16
        )
        for k in codes
    ]

    arrive(pick_copies)
    pick_z[here] = pick_in[...].reshape(toks, LANES)
    pick_copies = to_z(pick_z, others)

    rows_out, rows_in, rows_x = s.rows_out, s.rows_in, s.rows_x
    far_out = s.far_out
    pre_out, pre_in, hidden_x = s.pre_out, s.pre_in, s.hidden_x
    hidden_here = s.dense_gate.shape[0] * s.dense_gate.shape[1]
    row_copies, pre_copies = [], []
    to_right, to_left = x_dev(1), x_dev(nx - 1)
    from_left, from_right, from_far = [], [], []

    def rows_to_experts(h):
        arrive(feed_copies[h])
        feeds = feed_z[h * hz : (h + 1) * hz].reshape(half_toks, quarter)
        rows_out[h] = dot(put[h], feeds).astype(jnp.bfloat16).reshape(np_, chunk, quarter)
        rows_in[h, 0] = rows_out[h, 0]
        row_copies.append(
            send(
                [(rows_out.at[h, q], rows_in.at[h, q], p_dev(q)) for q in range(1, np_)],
                rows_in.at[h, pl.ds(1, np_ - 1)],
                apart=True,
            )
        )
        return feeds

    def far_to_experts(h):
        feeds = far_z[h * hz : (h + 1) * hz].reshape(half_toks, quarter)
        value = dot(put[h], feeds).astype(jnp.bfloat16).reshape(np_, chunk, quarter)
        far_out[h] = value
        rows_x[h, 2, 0] = far_out[h, 0]
        from_far.append(
            send(
                [(far_out.at[h, q], rows_x.at[h, 2, q], p_dev(q)) for q in range(1, np_)],
                rows_x.at[h, 2, pl.ds(1, np_ - 1)],
            )
        )

    def dense_sums(h, feeds):
        ready.dense_gate()
        ready.dense_up()
        for k, weight in enumerate((s.dense_gate, s.dense_up)):
            part = dot_nt(feeds, weight[...].reshape(hidden_here, quarter))
            part = part.reshape(hz, nx, own, hidden_here).swapaxes(0, 1)
            part = part.reshape(nx, hz * own, hidden_here).astype(jnp.bfloat16)
            pre_out[h, :, :, k * hidden_here : (k + 1) * hidden_here] = part
        pre_copies.append(
            send(
                [
                    (pre_out.at[h, lax.rem(x + r, nx)], pre_in.at[h, r - 1], x_dev(r))
                    for r in range(1, nx)
                ],
                pre_in.at[h],
            )
        )

    def rows_over_x(h):
        right_group = Group(rows_x.at[h, 0])
        left_group = Group(rows_x.at[h, 1])
        for q in range(np_):
            if q:
                row_copies[h][q - 1]()
            right_group.start(rows_in.at[h, q], rows_x.at[h, 0, q], to_right)
            left_group.start(rows_in.at[h, q], rows_x.at[h, 1, q], to_left)
        from_left.append([right_group.arrived])
        from_right.append([left_group.arrived])

    w_gate, w_up, w_down = s.expert_gate, s.expert_up, s.expert_down

    def of_share(taken, share):
        taken = taken.reshape(rows, quarter)
        return dot(taken, w_gate[share]), dot(taken, w_up[share])

    right, left = lax.rem(x + 1, nx), lax.rem(x + nx - 1, nx)

    def expert_hidden(h):
        gate_value, up_value = of_share(rows_in[h], x)
        arrive(from_left[h])
        more = of_share(rows_x[h, 0], left)
        gate_value, up_value = gate_value + more[0], up_value + more[1]
        arrive(from_right[h])
        more = of_share(rows_x[h, 1], right)
        gate_value, up_value = gate_value + more[0], up_value + more[1]
        arrive(from_far[h])
        more = of_share(rows_x[h, 2], far)
        gate_value, up_value = gate_value + more[0], up_value + more[1]
        return (jax.nn.silu(gate_value) * up_value).astype(jnp.bfloat16)

    sum_out, sum_in = s.sum_out, s.sum_in
    cut = rows // 2

    def put_out(h, k, values, device):
        sum_out[h, k] = values.astype(jnp.bfloat16)
        return send([(sum_out.at[h, k], sum_in.at[h, k], device)], sum_in.at[h, k])

    def sums_start(h, hidden):
        low, high = hidden[:cut], hidden[cut:]
        return [
            put_out(h, 0, dot(low, w_down[far]), to_right),
            put_out(h, 1, dot(high, w_down[far]), to_left),
            put_out(h, 2, dot(high, w_down[right]), to_right),
            put_out(h, 3, dot(low, w_down[left]), to_left),
        ]

    def sums_pass_on(h, hidden, sums):
        low, high = hidden[:cut], hidden[cut:]
        value = dot(low, w_down[right])
        arrive(sums[0])
        sums.append(put_out(h, 4, value + sum_in[h, 0].astype(jnp.float32), to_right))
        value = dot(high, w_down[left])
        arrive(sums[1])
        sums.append(put_out(h, 5, value + sum_in[h, 1].astype(jnp.float32), to_left))

    back_out, back_in = s.back_out, s.back_in

    def sums_end(h, hidden, sums):
        done = dot(hidden, w_down[x])
        for k, (a, b) in enumerate(((3, 4), (2, 5))):
            arrive(sums[a] + sums[b])
            total = done[k * cut : (k + 1) * cut]
            total += sum_in[h, a].astype(jnp.float32) + sum_in[h, b].astype(jnp.float32)
            back_out[h, k * half : (k + 1) * half] = total.astype(jnp.bfloat16).reshape(
                half, chunk, quarter
            )
        back_in[h, 0] = back_out[h, 0]
        return send(
            [(back_out.at[h, q], back_in.at[h, q], p_dev(np_ - q)) for q in range(1, np_)],
            back_in.at[h, pl.ds(1, np_ - 1)],
        )

    def dense_hidden(h):
        arrive(pre_copies[h])
        pre = pre_out[h, x].astype(jnp.float32)
        for r in range(1, nx):
            pre += pre_in[h, r - 1].astype(jnp.float32)
        value = jax.nn.silu(pre[:, :hidden_here]) * pre[:, hidden_here:]
        hidden_x[h, x] = value.astype(jnp.bfloat16)
        return send(
            [(hidden_x.at[h, x], hidden_x.at[h, x], x_dev(r)) for r in range(1, nx)],
            hidden_x.at[h, pl.ds(0, nx - 1)],
        )

    feeds = rows_to_experts(0)
    arrive(dense_copies)
    dense_sums(0, feeds)
    feeds = rows_to_experts(1)
    dense_sums(1, feeds)
    rows_over_x(0)
    arrive(far_copies)
    far_to_experts(0)
    far_to_experts(1)
    rows_over_x(1)
    hidden_copies = [dense_hidden(0)]
    ready.expert_gate()
    ready.expert_up()
    take_of(s.expert_down, down_sem)()
    hidden0 = expert_hidden(0)
    sums0 = sums_start(0, hidden0)
    hidden1 = expert_hidden(1)
    sums1 = sums_start(1, hidden1)
    sums_pass_on(0, hidden0, sums0)
    hidden_copies.append(dense_hidden(1))
    backs = [sums_end(0, hidden0, sums0)]
    sums_pass_on(1, hidden1, sums1)

    arrive(pick_copies)
    j_col = iota((half_toks, rows), 1)
    same_block = block_of(j_col) == iota((half_toks, rows), 0) >> shift_of(toks)
    take, dense_part = [], []
    ready.dense_down()
    down = s.dense_down[...].reshape(hidden_here, quarter)
    for h in range(2):
        table = pick_z[h * hz : (h + 1) * hz].reshape(half_toks, LANES)
        table_hi = table.astype(jnp.bfloat16)
        table_lo = (table - table_hi.astype(jnp.float32)).astype(jnp.bfloat16)
        taken = (dot(codes[h], choose) == slot_of(j_col)) & same_block
        take.append(
            [
                jnp.where(taken, dot(k, choose), 0.0).astype(jnp.bfloat16)
                for k in (table_hi, table_lo)
            ]
        )
        arrive(hidden_copies[h])
        value = hidden_x[h].astype(jnp.float32).reshape(nx, hz, own, hidden_here)
        value = value.swapaxes(0, 1).reshape(half_toks, hidden_here).astype(jnp.bfloat16)
        dense_part.append(dot(value, down) * table[:, experts : experts + 1])

    last_out, last_in = s.last_out, s.last_in
    last, parts = [], []

    def give_back(h):
        arrive(backs[h])
        results = back_in[h].reshape(rows, quarter)
        part = dot(take[h][0], results) + dot(take[h][1], results) + dense_part[h]
        last_out[h * hz : (h + 1) * hz] = part.astype(jnp.bfloat16).reshape(hz, toks, quarter)
        ks = others[h * hz : (h + 1) * hz]
        last.append(
            send(
                [(last_out.at[k], last_in.at[k], z_dev(nz - order[k])) for k in ks],
                last_in.at[pl.ds(0, len(ks))],
            )
        )
        return part

    give_back(0)
    backs.append(sums_end(1, hidden1, sums1))
    combined = give_back(1)[(here - hz) * toks : (here - hz + 1) * toks]
    gain = in_row(ready.out_gain())
    arrive(stream_copies)
    stream_part = stream_in[...].astype(jnp.float32).reshape(toks, quarter)
    for h in range(2):
        arrive(last[h])
        for k in others[h * hz : (h + 1) * hz]:
            combined += last_in[k].astype(jnp.float32)

    square_x = s.square_x
    square = jnp.sum(combined * combined, axis=1, keepdims=True)
    on_lane = iota((toks, LANES), 0) == iota((toks, LANES), 1)
    as_row = jnp.sum(jnp.where(on_lane, square, 0.0), axis=0, keepdims=True)
    square_x[0] = jnp.broadcast_to(as_row, square_x.shape[1:])
    square_copies = send(
        [(square_x.at[0], square_x.at[r], x_dev(r)) for r in range(1, nx)],
        square_x.at[pl.ds(1, nx - 1)],
    )
    combined = combined * gain
    arrive(square_copies)
    all_rows = square_x[0]
    for r in range(1, nx):
        all_rows += square_x[r]
    total_square = jnp.sum(jnp.where(on_lane, all_rows[0:1], 0.0), axis=1, keepdims=True)
    scale = lax.rsqrt(total_square / width + norm_eps)
    layer_out[...] = (stream_part + combined * scale).astype(jnp.bfloat16)

    arrive(at_end)
    for copy in small_out:
        copy.wait()


def run_layer(sizes, p):
    nz, ny, nc, nx, cap = sizes
    np_ = ny * nc
    toks, width = p.resid.shape
    own, quarter = toks // nx, width // nx
    hz = nz // 2
    bf16, f32 = jnp.bfloat16, jnp.float32
    share = p.expert_gate.shape[2]
    hid = p.dense_gate.shape[0]
    channels = p.conv_state.shape[3]
    state_dim = p.scan_state.shape[3]

    def tall(a):
        return a.reshape(-1, LANES)

    g = SimpleNamespace(**vars(p))
    g.mix_gain, g.post_gain, g.ffn_gain = tall(p.mix_gain), tall(p.post_gain), tall(p.ffn_gain)
    g.dense_switch, g.inner_gain = tall(p.dense_switch), tall(p.inner_gain)
    g.out_gain = tall(p.out_gain)
    g.proj_step, g.expert_router = p.proj_step.T, p.expert_router.T
    g.group_router, g.route_experts = p.group_router.T, p.route_experts.T
    g.resid = p.resid.reshape(nx, own, width)
    g.conv_state = p.conv_state.transpose(1, 2, 0, 3)
    g.scan_state = p.scan_state.reshape(toks, channels, state_dim)
    g.step_bias, g.decay_rate = p.step_bias.reshape(1, -1), p.decay_rate.reshape(1, -1)
    g.expert_gate = p.expert_gate.reshape(nx, quarter, share)
    g.expert_up = p.expert_up.reshape(nx, quarter, share)
    g.expert_down = p.expert_down.reshape(share, width)
    names = tuple(vars(g))
    operands = list(vars(g).values())
    s = SimpleNamespace(**{k: pltpu.VMEM(v.shape, v.dtype) for k, v in vars(g).items()})
    s.dense_gate = s.dense_up = s.dense_down = pltpu.VMEM((np_, hid, quarter), bf16)
    s.expert_down = pltpu.VMEM((nx, share, quarter), bf16)
    s.proj_x = s.proj_b = s.proj_c = s.proj_z = pltpu.VMEM((8, LANES), f32)
    s.proj = pltpu.VMEM((width, 4 * channels), bf16)
    s.fresh = pltpu.VMEM((3, toks, channels), bf16)
    state_rows = (p.scan_state.shape[1] + 1, toks, channels)
    s.rows_ref = pltpu.VMEM(state_rows, f32)
    s.cols_ref = pltpu.VMEM((channels, channels), f32)
    s.c_ref = s.old_read = pltpu.VMEM((toks, channels), f32)
    s.mixed_f = pltpu.VMEM((nx, own, width), f32)
    s.mixed_b = pltpu.VMEM((nx, own, width), bf16)
    s.mixed_in = pltpu.VMEM((nx - 1, own, width), bf16)
    s.feed_out = s.feed_in = s.far_in = pltpu.VMEM((nx, own, quarter), bf16)
    s.stream_out = s.stream_in = pltpu.VMEM((nx, own, quarter), bf16)
    s.pick_in = pltpu.VMEM((nx, own, LANES), f32)
    s.pick_z = pltpu.VMEM((nz, toks, LANES), f32)
    s.code_z = pltpu.VMEM((nz, toks, LANES), bf16)
    s.feed_z = s.far_z = pltpu.VMEM((nz, toks, quarter), bf16)
    s.rows_out = s.rows_in = s.far_out = pltpu.VMEM((2, np_, hz * cap, quarter), bf16)
    s.back_out = s.back_in = pltpu.VMEM((2, np_, hz * cap, quarter), bf16)
    s.rows_x = pltpu.VMEM((2, 3, np_, hz * cap, quarter), bf16)
    s.pre_out = pltpu.VMEM((2, nx, hz * own, 2 * np_ * hid), bf16)
    s.pre_in = pltpu.VMEM((2, nx - 1, hz * own, 2 * np_ * hid), bf16)
    s.hidden_x = pltpu.VMEM((2, nx, hz * own, np_ * hid), bf16)
    s.sum_out = s.sum_in = pltpu.VMEM((2, 6, np_ * hz * cap // 2, quarter), bf16)
    s.last_out = pltpu.VMEM((nz, toks, quarter), bf16)
    s.last_in = pltpu.VMEM((nz, toks, quarter), bf16)
    s.square_x = pltpu.VMEM((nx, 8, LANES), f32)
    plan = names, tuple(vars(s))
    groups = 44
    shapes = [
        pltpu.SemaphoreType.DMA((groups,)),
        pltpu.SemaphoreType.DMA((groups + 2 * (np_ - 2),)),
        pltpu.SemaphoreType.DMA((len(names),)),
        *vars(s).values(),
    ]
    anyw = pl.BlockSpec(memory_space=pl.ANY)
    return pl.pallas_call(
        functools.partial(layer, sizes, plan),
        out_shape=(
            jax.ShapeDtypeStruct((toks, quarter), bf16),
            jax.ShapeDtypeStruct(state_rows, f32),
            jax.ShapeDtypeStruct((channels, channels), f32),
            jax.ShapeDtypeStruct((3, toks, channels), bf16),
        ),
        in_specs=[anyw] * len(operands),
        out_specs=(pl.BlockSpec(memory_space=pltpu.VMEM), anyw, anyw, anyw),
        scratch_shapes=shapes,
        compiler_params=pltpu.CompilerParams(
            collective_id=0, has_side_effects=True, vmem_limit_bytes=56 * 1024 * 1024
        ),
        name="layer",
    )(*operands)


def finish_step(
    rows_in,
    cols_in,
    fresh_in,
    conv,
    result,
    state,
    new_state,
    new_conv,
    layer_out,
    rows,
    cols,
    fresh,
    conv_v,
    result_v,
    state_v,
    sem,
):
    used = [0]

    def move(src, dst):
        copy = pltpu.make_async_copy(src, dst, sem.at[used[0]])
        used[0] += 1
        copy.start()
        return copy

    toks = state.shape[0]
    heads = rows.shape[0] - 1
    block = 8
    pieces = [pl.ds(i, block) for i in range(0, toks, block)]
    small = [move(rows_in, rows), move(cols_in, cols)]
    states = [move(state.at[at], state_v.at[at]) for at in pieces]
    others = [move(result, result_v), move(conv, conv_v), move(fresh_in, fresh)]
    for copy in small:
        copy.wait()
    head_dim = cols.shape[0] // heads
    out = []
    for i, at in enumerate(pieces):
        states[i].wait()
        for t in range(i * block, (i + 1) * block):
            new = slice(t, t + 1)
            for h in range(heads):
                part = slice(h * head_dim, (h + 1) * head_dim)
                added = cols[part, new] * rows[heads, new]
                state_v[t, part] = rows[h, new] * state_v[t, part] + added
        out.append(move(state_v.at[at], new_state.at[at]))
        if i == 0:
            for copy in others:
                copy.wait()
            out.append(move(result_v, layer_out))
            for k in range(3):
                out.append(move(conv_v.at[k, pl.ds(1, 2)], new_conv.at[k, pl.ds(0, 2)]))
                out.append(move(fresh.at[k], new_conv.at[k, 2]))
    for copy in out:
        copy.wait()


def finish(result, rows, cols, fresh, p):
    toks, heads, head_dim, state_dim = p.scan_state.shape
    channels = heads * head_dim
    conv = p.conv_state.transpose(1, 2, 0, 3)
    state = p.scan_state.reshape(toks, channels, state_dim)
    anyw = pl.BlockSpec(memory_space=pl.ANY)
    operands = (rows, cols, fresh, conv, result, state)
    new_state, new_conv, layer_out = pl.pallas_call(
        finish_step,
        out_shape=tuple(jax.ShapeDtypeStruct(a.shape, a.dtype) for a in (state, conv, result)),
        in_specs=[anyw] * 6,
        out_specs=(anyw,) * 3,
        scratch_shapes=[pltpu.VMEM(a.shape, a.dtype) for a in operands]
        + [pltpu.SemaphoreType.DMA((5 + 2 * (toks // 8) + 7,))],
        name="finish",
    )(*operands)
    return (
        layer_out,
        new_state.reshape(p.scan_state.shape),
        new_conv.transpose(2, 0, 1, 3),
    )


def on_device(
    resid,
    mix_gain,
    proj_x,
    proj_z,
    proj_b,
    proj_c,
    proj_step,
    step_bias,
    decay_rate,
    conv_taps,
    conv_state,
    scan_state,
    inner_gain,
    proj_out,
    post_gain,
    ffn_gain,
    group_router,
    expert_router,
    route_experts,
    expert_gate,
    expert_up,
    expert_down,
    dense_switch,
    dense_gate,
    dense_up,
    dense_down,
    out_gain,
):
    params = SimpleNamespace(**locals())
    sizes = tuple(lax.axis_size(a) for a in EP) + (lax.axis_size("tp"), CAPACITY)
    return finish(*run_layer(sizes, params), params)


TORUS = (8, 4, 2)


def solution(mesh):
    torus = Mesh(mesh.devices.reshape(*TORUS, mesh.shape["tp"]), EP + ("tp",))
    in_specs = (
        P(EP, None),
        P(),
        P(None, "tp"),
        P(None, "tp"),
        P(None, "tp"),
        P(None, "tp"),
        P(),
        P("tp"),
        P("tp"),
        P(None, None, "tp"),
        P(EP, None, None, "tp"),
        P(EP, "tp", None, None),
        P("tp"),
        P("tp", None),
        P(),
        P(),
        P(),
        P(),
        P(EP, None),
        P(EP, None, "tp"),
        P(EP, None, "tp"),
        P(EP, "tp", None),
        P(),
        P(EP, "tp"),
        P(EP, "tp"),
        P(EP, "tp"),
        P("tp"),
    )
    out_specs = (P(EP, "tp"), P(EP, "tp", None, None), P(EP, None, None, "tp"))
    return jax.shard_map(
        on_device, mesh=torus, in_specs=in_specs, out_specs=out_specs, check_vma=False
    )
```

```python
import functools
from types import SimpleNamespace

import jax
import jax.numpy as jnp
from jax import lax
from jax.experimental import pallas as pl
from jax.experimental.pallas import tpu as pltpu
from jax.sharding import Mesh
from jax.sharding import PartitionSpec as P

EP = ("ep_0", "ep_1", "ep_2")
MESH = pl.DeviceIdType.MESH
norm_eps = 1e-06
CAPACITY = 4
LANES = 128


def dot(a, b):
    return jnp.dot(a, b, preferred_element_type=jnp.float32)


def dot_nt(a, b):
    return lax.dot_general(a, b, (((1,), (1,)), ((), ())), preferred_element_type=jnp.float32)


def in_row(gain_ref):
    gain = gain_ref[...].astype(jnp.float32)
    return jnp.concatenate([gain[i : i + 1] for i in range(gain.shape[0])], axis=1)


def iota(shape, dim):
    return lax.broadcasted_iota(jnp.int32, shape, dim)


def shift_of(count):
    return count.bit_length() - 1


def root_mean(values):
    return values * lax.rsqrt(jnp.mean(values * values, axis=-1, keepdims=True) + norm_eps)


def far_first(nz):
    return sorted(range(nz), key=lambda r: (-min(r, nz - r), r))


def layer(sizes, plan, *refs):
    nz, ny, nc, nx, cap = sizes
    np_ = ny * nc
    names, scratch = plan
    given = SimpleNamespace(**dict(zip(names, refs)))
    layer_out, state_rows, state_cols, fresh_out = refs[len(names) :][:4]
    send_sem, recv_sem, local_sem = refs[len(names) + 4 :][:3]
    s = SimpleNamespace(**dict(zip(scratch, refs[len(names) + 7 :])))
    z, y, c, x = (lax.axis_index(a) for a in ("ep_0", "ep_1", "ep_2", "tp"))
    place = y * nc + c
    own, width = given.resid.shape[1:]
    toks = own * nx
    quarter = width // nx
    hz = nz // 2
    half_toks = hz * toks
    chunk = hz * cap
    rows = np_ * chunk
    half = np_ // 2
    order = far_first(nz)
    here = order.index(0)
    others = [k for k in range(nz) if k != here]

    def z_dev(r):
        return {"ep_0": lax.rem(z + r, nz)}

    def p_dev(q):
        to = lax.rem(place + q, np_)
        return {"ep_1": to // nc, "ep_2": lax.rem(to, nc)}

    def x_dev(r):
        return {"tp": lax.rem(x + r, nx)}

    used = SimpleNamespace(send=0, recv=0)
    at_end = []

    def take_of(whole, sem):
        return lambda: pltpu.make_async_copy(whole, whole, sem).wait()

    class Group:
        def __init__(self, whole):
            self.out_sem, self.in_sem = send_sem.at[used.send], recv_sem.at[used.recv]
            used.send += 1
            used.recv += 1
            self.arrived = take_of(whole, self.in_sem)
            at_end.append(take_of(whole, self.out_sem))

        def start(self, src, dst, device, in_sem=None):
            pltpu.make_async_remote_copy(
                src_ref=src,
                dst_ref=dst,
                send_sem=self.out_sem,
                recv_sem=self.in_sem if in_sem is None else in_sem,
                device_id=device,
                device_id_type=MESH,
            ).start()

    def send(copies, whole, apart=False):
        if not copies:
            return []
        group = Group(whole)
        waits = []
        for k, (src, dst, device) in enumerate(copies):
            in_sem = group.in_sem
            if apart and k:
                in_sem = recv_sem.at[used.recv]
                used.recv += 1
            group.start(src, dst, device, in_sem)
            waits.append(take_of(dst, in_sem))
        return waits if apart else [group.arrived]

    local_used = [0]

    def fetch(src, dst, sem=None):
        if sem is None:
            sem = local_sem.at[local_used[0]]
            local_used[0] += 1
        copy = pltpu.make_async_copy(src, dst, sem)
        copy.start()
        return copy

    def arrive(waits):
        for wait in waits:
            wait()

    barrier = pltpu.get_barrier_semaphore()
    peers = (
        [x_dev(r) for r in range(1, nx)]
        + [p_dev(q) for q in range(1, np_)]
        + [z_dev(r) for r in range(1, nz)]
    )
    for device in peers:
        pl.semaphore_signal(barrier, inc=1, device_id=device, device_id_type=MESH)

    def bring(*pairs):
        coming = [fetch(src, dst) for src, dst in pairs]

        def get():
            while coming:
                coming.pop().wait()
            return pairs[0][1]

        return get

    g, ready = given, SimpleNamespace()
    ready.route_experts = bring((g.route_experts, s.route_experts))
    ready.resid = bring((g.resid, s.resid))
    ready.mix_gain = bring((g.mix_gain, s.mix_gain))
    wide = g.proj_x.shape[1]
    proj_sem = local_sem.at[local_used[0]]
    local_used[0] += 1
    for k, one in enumerate((g.proj_x, g.proj_b, g.proj_c, g.proj_z)):
        fetch(one, s.proj.at[:, pl.ds(k * wide, wide)], proj_sem)
    ready.proj_step = bring((g.proj_step, s.proj_step))
    ready.conv_taps = bring((g.conv_taps, s.conv_taps))
    ready.conv_state = bring((g.conv_state, s.conv_state))
    ready.step_bias = bring((g.step_bias, s.step_bias))
    ready.decay_rate = bring((g.decay_rate, s.decay_rate))
    ready.scan_state = bring((g.scan_state, s.scan_state))
    ready.inner_gain = bring((g.inner_gain, s.inner_gain))
    ready.proj_out = bring((g.proj_out, s.proj_out))
    ready.post_gain = bring((g.post_gain, s.post_gain))
    ready.ffn_gain = bring((g.ffn_gain, s.ffn_gain))
    ready.expert_router = bring((g.expert_router, s.expert_router))
    ready.group_router = bring((g.group_router, s.group_router))
    ready.dense_switch = bring((g.dense_switch, s.dense_switch))
    ready.out_gain = bring((g.out_gain, s.out_gain))
    ready.dense_gate = bring((g.dense_gate, s.dense_gate.at[0]))
    ready.dense_up = bring((g.dense_up, s.dense_up.at[0]))
    ready.dense_down = bring((g.dense_down, s.dense_down.at[0]))
    ready.expert_gate = bring((g.expert_gate, s.expert_gate))
    ready.expert_up = bring((g.expert_up, s.expert_up))
    down_sem = local_sem.at[local_used[0]]
    local_used[0] += 1
    for j in range(nx):
        fetch(g.expert_down.at[:, pl.ds(j * quarter, quarter)], s.expert_down.at[j], down_sem)

    route_t = ready.route_experts()[...]
    picks = route_t.shape[0]
    expert_ids = iota((LANES, toks), 0)
    named = jnp.zeros((LANES, toks), jnp.float32)
    for k in range(picks):
        named += jnp.where(expert_ids == route_t[k : k + 1, :], 1.0, 0.0)
    named_b = named.astype(jnp.bfloat16)
    before = jnp.where(iota((toks, toks), 0) < iota((toks, toks), 1), 1.0, 0.0).astype(jnp.bfloat16)
    code_t = (named * (dot(named_b, before) + 1.0)).astype(jnp.bfloat16)
    eye = jnp.where(iota((toks, toks), 0) == iota((toks, toks), 1), 1.0, 0.0).astype(jnp.bfloat16)
    code_z = s.code_z
    code_z[here] = dot_nt(eye, code_t).astype(jnp.bfloat16)

    resid = ready.resid()
    gain = in_row(ready.mix_gain())
    normed = root_mean(resid[...].astype(jnp.float32).reshape(toks, width)) * gain
    normed = normed.astype(jnp.bfloat16)
    take_of(s.proj, proj_sem)()
    projected = dot(normed, s.proj[...])
    step_all = dot_nt(normed, ready.proj_step()[...])
    taps = ready.conv_taps()[...].astype(jnp.float32)
    old_conv = ready.conv_state()
    channels = taps.shape[2]
    acts = []
    fresh_ref = s.fresh
    for k in range(3):
        fresh = projected[:, k * channels : (k + 1) * channels].astype(jnp.bfloat16)
        fresh_ref[k] = fresh
        mixed_in = fresh.astype(jnp.float32) * taps[k, 3:4]
        for i in range(3):
            mixed_in += old_conv[k, i].astype(jnp.float32) * taps[k, i : i + 1]
        acts.append(jax.nn.silu(mixed_in))
    xs, bs, cs = acts
    gate_z = projected[:, 3 * channels :]
    bias, rate = ready.step_bias()[...], ready.decay_rate()[...]
    heads_here = bias.shape[1]
    head_dim = channels // heads_here
    head_of = iota((toks, channels), 1) >> shift_of(head_dim)
    head_col = iota(step_all.shape, 1)
    step = jnp.zeros((toks, channels), jnp.float32)
    keep = jnp.zeros((toks, channels), jnp.float32)
    rows_ref = s.rows_ref
    for h in range(heads_here):
        raw = jnp.sum(
            jnp.where(head_col == x * heads_here + h, step_all, 0.0), axis=1, keepdims=True
        )
        one = jax.nn.softplus(raw + bias[:, h : h + 1])
        step = jnp.where(head_of == h, one, step)
        kept = jnp.exp(-rate[:, h : h + 1] * one)
        keep = jnp.where(head_of == h, kept, keep)
        rows_ref[h] = jnp.broadcast_to(kept, (toks, channels))
    driven = step * xs
    rows_ref[heads_here] = bs
    s.cols_ref[...] = jnp.concatenate([driven] * (channels // toks), axis=0).T
    small_out = [
        fetch(rows_ref, state_rows),
        fetch(s.cols_ref, state_cols),
        fetch(fresh_ref, fresh_out),
    ]
    c_ref, old_read = s.c_ref, s.old_read
    c_ref[...] = cs
    diag = iota((channels, channels), 0) == iota((channels, channels), 1)
    old_state = ready.scan_state()

    @pl.loop(0, toks // 8)
    def _(i):
        at = pl.multiple_of(i * 8, 8)
        c8 = c_ref[pl.ds(at, 8), :]
        out = []
        for t in range(8):
            sums = jnp.sum(old_state[at + t] * c8[t : t + 1], axis=1, keepdims=True)
            out.append(jnp.sum(jnp.where(diag, sums, 0.0), axis=0, keepdims=True))
        old_read[pl.ds(at, 8), :] = jnp.concatenate(out, axis=0)

    read = keep * old_read[...] + driven * jnp.sum(bs * cs, axis=1, keepdims=True)
    gated = (read * jax.nn.silu(gate_z) * in_row(ready.inner_gain())).astype(jnp.bfloat16)

    mixed_f, mixed_b, mixed_in = s.mixed_f, s.mixed_b, s.mixed_in
    share = dot(gated, ready.proj_out()[...]).reshape(nx, own, width)
    mixed_f[...] = share
    mixed_b[...] = share.astype(jnp.bfloat16)

    pl.semaphore_wait(barrier, len(peers))

    copies = send(
        [(mixed_b.at[lax.rem(x + r, nx)], mixed_in.at[r - 1], x_dev(r)) for r in range(1, nx)],
        mixed_in,
    )
    code_copies = send(
        [(code_z.at[here], code_z.at[k], z_dev(order[k])) for k in others],
        code_z.at[pl.ds(0, nz - 1)],
    )
    dense_copies = []
    for one, all_here in (
        (g.dense_gate, s.dense_gate),
        (g.dense_up, s.dense_up),
        (g.dense_down, s.dense_down),
    ):
        dense_copies += send(
            [(one, all_here.at[q], p_dev(q)) for q in range(1, np_)],
            all_here.at[pl.ds(1, np_ - 1)],
        )

    post_gain, ffn_gain = in_row(ready.post_gain()), in_row(ready.ffn_gain())
    resid_own = resid[x].astype(jnp.float32)
    arrive(copies)
    mixed = mixed_f[x]
    for r in range(1, nx):
        mixed += mixed_in[r - 1].astype(jnp.float32)
    stream = (resid_own + root_mean(mixed) * post_gain).astype(jnp.bfloat16)
    feed = (root_mean(stream.astype(jnp.float32)) * ffn_gain).astype(jnp.bfloat16)
    feed_out, feed_in = s.feed_out, s.feed_in
    stream_out, stream_in = s.stream_out, s.stream_in
    for j in range(nx):
        feed_out[j] = feed[:, j * quarter : (j + 1) * quarter]
    far = lax.rem(x + 2, nx)
    far_in = s.far_in
    feed_in[x] = feed_out[x]
    far_in[x] = feed_out[far]
    feed_copies = send(
        [(feed_out.at[lax.rem(x + r, nx)], feed_in.at[x], x_dev(r)) for r in range(1, nx)],
        feed_in.at[pl.ds(0, nx - 1)],
    )
    far_copies = send(
        [(feed_out.at[lax.rem(x + r + 2, nx)], far_in.at[x], x_dev(r)) for r in range(1, nx)],
        far_in.at[pl.ds(0, nx - 1)],
    )
    for j in range(nx):
        stream_out[j] = stream[:, j * quarter : (j + 1) * quarter]

    feed_f = feed.astype(jnp.float32)
    expert_rows, group_rows = ready.expert_router(), ready.group_router()
    experts = expert_rows.shape[0]
    groups = group_rows.shape[0]
    group_size = experts // groups
    token_pick = jnp.where(iota((own, toks), 1) == iota((own, toks), 0) + x * own, 1.0, 0.0)
    own_route = dot_nt(token_pick.astype(jnp.bfloat16), route_t.astype(jnp.bfloat16))
    logits = dot_nt(feed, expert_rows[...])
    lanes = iota((own, experts), 1).astype(jnp.float32)
    weights = []
    for k in range(picks):
        chosen = jnp.sum(
            jnp.where(lanes == own_route[:, k : k + 1], logits, 0.0), axis=1, keepdims=True
        )
        weights.append(jnp.exp(chosen))
    total = functools.reduce(jnp.add, weights)
    group_f = group_rows[...].astype(jnp.float32)
    group_exp = [
        jnp.exp(jnp.sum(feed_f * group_f[g : g + 1], axis=1, keepdims=True)) for g in range(groups)
    ]
    group_total = functools.reduce(jnp.add, group_exp)
    first = own_route[:, 0:1]
    group_weight = jnp.zeros((own, 1), jnp.float32)
    for g in range(groups):
        in_group = (first >= g * group_size) & (first < (g + 1) * group_size)
        group_weight += jnp.where(in_group, group_exp[g] / group_total, 0.0)
    switch_row = in_row(ready.dense_switch())
    switch = jax.nn.sigmoid(jnp.sum(feed_f * switch_row, axis=1, keepdims=True))
    all_lanes = iota((own, LANES), 1).astype(jnp.float32)
    pick_table = jnp.where(all_lanes < experts, 0.0, switch)
    for k in range(picks):
        pick_table += jnp.where(
            all_lanes == own_route[:, k : k + 1], weights[k] / total * group_weight, 0.0
        )
    pick_in, pick_z = s.pick_in, s.pick_z
    pick_in[x] = pick_table

    arrive(feed_copies)
    feed_z, far_z = s.feed_z, s.far_z
    feed_z[here] = feed_in[...].astype(jnp.float32).reshape(toks, quarter).astype(jnp.bfloat16)

    def to_z(ref, ks):
        return send(
            [(ref.at[here], ref.at[k], z_dev(order[k])) for k in ks], ref.at[pl.ds(0, len(ks))]
        )

    feed_copies = [to_z(feed_z, others[:hz]), to_z(feed_z, others[hz:])]
    arrive(far_copies)
    far_z[here] = far_in[...].astype(jnp.float32).reshape(toks, quarter).astype(jnp.bfloat16)
    far_copies = to_z(far_z, others)
    pick_copies = send(
        [(pick_in.at[x], pick_in.at[x], x_dev(r)) for r in range(1, nx)],
        pick_in.at[pl.ds(0, nx - 1)],
    )
    stream_in[x] = stream_out[x]
    stream_copies = send(
        [(stream_out.at[lax.rem(x + r, nx)], stream_in.at[x], x_dev(r)) for r in range(1, nx)],
        stream_in.at[pl.ds(0, nx - 1)],
    )

    def expert_of(j):
        return z * np_ + ((place + (j >> shift_of(chunk))) & (np_ - 1))

    def block_of(j):
        return (j & (chunk - 1)) >> shift_of(cap)

    def slot_of(j):
        return ((j & (cap - 1)) + 1).astype(jnp.float32)

    arrive(code_copies)
    codes = [
        code_z[h * hz : (h + 1) * hz].reshape(half_toks, LANES) for h in range(2)
    ]
    choose_t = jnp.where(
        iota((rows, LANES), 1) == expert_of(iota((rows, LANES), 0)), 1.0, 0.0
    ).astype(jnp.bfloat16)
    choose = jnp.where(
        iota((LANES, rows), 0) == expert_of(iota((LANES, rows), 1)), 1.0, 0.0
    ).astype(jnp.bfloat16)
    j_row = iota((rows, half_toks), 0)
    same_block = block_of(j_row) == iota((rows, half_toks), 1) >> shift_of(toks)
    put = [
        jnp.where((dot_nt(choose_t, k) == slot_of(j_row)) & same_block, 1.0, 0.0).astype(
            jnp.bfloat16
        )
        for k in codes
    ]

    arrive(pick_copies)
    pick_z[here] = pick_in[...].reshape(toks, LANES)
    pick_copies = to_z(pick_z, others)

    rows_out, rows_in, rows_x = s.rows_out, s.rows_in, s.rows_x
    far_out = s.far_out
    pre_out, pre_in, hidden_x = s.pre_out, s.pre_in, s.hidden_x
    hidden_here = s.dense_gate.shape[0] * s.dense_gate.shape[1]
    row_copies, pre_copies = [], []
    to_right, to_left = x_dev(1), x_dev(nx - 1)
    from_left, from_right, from_far = [], [], []

    def rows_to_experts(h):
        arrive(feed_copies[h])
        feeds = feed_z[h * hz : (h + 1) * hz].reshape(half_toks, quarter)
        rows_out[h] = dot(put[h], feeds).astype(jnp.bfloat16).reshape(np_, chunk, quarter)
        rows_in[h, 0] = rows_out[h, 0]
        row_copies.append(
            send(
                [(rows_out.at[h, q], rows_in.at[h, q], p_dev(q)) for q in range(1, np_)],
                rows_in.at[h, pl.ds(1, np_ - 1)],
                apart=True,
            )
        )
        return feeds

    def far_to_experts(h):
        feeds = far_z[h * hz : (h + 1) * hz].reshape(half_toks, quarter)
        value = dot(put[h], feeds).astype(jnp.bfloat16).reshape(np_, chunk, quarter)
        far_out[h] = value
        rows_x[h, 2, 0] = far_out[h, 0]
        from_far.append(
            send(
                [(far_out.at[h, q], rows_x.at[h, 2, q], p_dev(q)) for q in range(1, np_)],
                rows_x.at[h, 2, pl.ds(1, np_ - 1)],
            )
        )

    def dense_sums(h, feeds):
        ready.dense_gate()
        ready.dense_up()
        for k, weight in enumerate((s.dense_gate, s.dense_up)):
            part = dot_nt(feeds, weight[...].reshape(hidden_here, quarter))
            part = part.reshape(hz, nx, own, hidden_here).swapaxes(0, 1)
            part = part.reshape(nx, hz * own, hidden_here).astype(jnp.bfloat16)
            pre_out[h, :, :, k * hidden_here : (k + 1) * hidden_here] = part
        pre_copies.append(
            send(
                [
                    (pre_out.at[h, lax.rem(x + r, nx)], pre_in.at[h, r - 1], x_dev(r))
                    for r in range(1, nx)
                ],
                pre_in.at[h],
            )
        )

    def rows_over_x(h):
        right_group = Group(rows_x.at[h, 0])
        left_group = Group(rows_x.at[h, 1])
        for q in range(np_):
            if q:
                row_copies[h][q - 1]()
            right_group.start(rows_in.at[h, q], rows_x.at[h, 0, q], to_right)
            left_group.start(rows_in.at[h, q], rows_x.at[h, 1, q], to_left)
        from_left.append([right_group.arrived])
        from_right.append([left_group.arrived])

    w_gate, w_up, w_down = s.expert_gate, s.expert_up, s.expert_down

    def of_share(taken, share):
        taken = taken.reshape(rows, quarter)
        return dot(taken, w_gate[share]), dot(taken, w_up[share])

    right, left = lax.rem(x + 1, nx), lax.rem(x + nx - 1, nx)

    def expert_hidden(h):
        gate_value, up_value = of_share(rows_in[h], x)
        arrive(from_left[h])
        more = of_share(rows_x[h, 0], left)
        gate_value, up_value = gate_value + more[0], up_value + more[1]
        arrive(from_right[h])
        more = of_share(rows_x[h, 1], right)
        gate_value, up_value = gate_value + more[0], up_value + more[1]
        arrive(from_far[h])
        more = of_share(rows_x[h, 2], far)
        gate_value, up_value = gate_value + more[0], up_value + more[1]
        return (jax.nn.silu(gate_value) * up_value).astype(jnp.bfloat16)

    sum_out, sum_in = s.sum_out, s.sum_in
    cut = rows // 2

    def put_out(h, k, values, device):
        sum_out[h, k] = values.astype(jnp.bfloat16)
        return send([(sum_out.at[h, k], sum_in.at[h, k], device)], sum_in.at[h, k])

    def sums_start(h, hidden):
        low, high = hidden[:cut], hidden[cut:]
        return [
            put_out(h, 0, dot(low, w_down[far]), to_right),
            put_out(h, 1, dot(high, w_down[far]), to_left),
            put_out(h, 2, dot(high, w_down[right]), to_right),
            put_out(h, 3, dot(low, w_down[left]), to_left),
        ]

    def sums_pass_on(h, hidden, sums):
        low, high = hidden[:cut], hidden[cut:]
        value = dot(low, w_down[right])
        arrive(sums[0])
        sums.append(put_out(h, 4, value + sum_in[h, 0].astype(jnp.float32), to_right))
        value = dot(high, w_down[left])
        arrive(sums[1])
        sums.append(put_out(h, 5, value + sum_in[h, 1].astype(jnp.float32), to_left))

    back_out, back_in = s.back_out, s.back_in

    def sums_end(h, hidden, sums):
        done = dot(hidden, w_down[x])
        for k, (a, b) in enumerate(((3, 4), (2, 5))):
            arrive(sums[a] + sums[b])
            total = done[k * cut : (k + 1) * cut]
            total += sum_in[h, a].astype(jnp.float32) + sum_in[h, b].astype(jnp.float32)
            back_out[h, k * half : (k + 1) * half] = total.astype(jnp.bfloat16).reshape(
                half, chunk, quarter
            )
        back_in[h, 0] = back_out[h, 0]
        return send(
            [(back_out.at[h, q], back_in.at[h, q], p_dev(np_ - q)) for q in range(1, np_)],
            back_in.at[h, pl.ds(1, np_ - 1)],
        )

    def dense_hidden(h):
        arrive(pre_copies[h])
        pre = pre_out[h, x].astype(jnp.float32)
        for r in range(1, nx):
            pre += pre_in[h, r - 1].astype(jnp.float32)
        value = jax.nn.silu(pre[:, :hidden_here]) * pre[:, hidden_here:]
        hidden_x[h, x] = value.astype(jnp.bfloat16)
        return send(
            [(hidden_x.at[h, x], hidden_x.at[h, x], x_dev(r)) for r in range(1, nx)],
            hidden_x.at[h, pl.ds(0, nx - 1)],
        )

    feeds = rows_to_experts(0)
    arrive(dense_copies)
    dense_sums(0, feeds)
    feeds = rows_to_experts(1)
    dense_sums(1, feeds)
    rows_over_x(0)
    arrive(far_copies)
    far_to_experts(0)
    far_to_experts(1)
    rows_over_x(1)
    ready.expert_gate()
    ready.expert_up()
    take_of(s.expert_down, down_sem)()
    hidden0 = expert_hidden(0)
    sums0 = sums_start(0, hidden0)
    hidden1 = expert_hidden(1)
    sums1 = sums_start(1, hidden1)
    sums_pass_on(0, hidden0, sums0)
    sums_pass_on(1, hidden1, sums1)
    hidden_copies = [dense_hidden(0), dense_hidden(1)]
    arrive(pick_copies)
    j_col = iota((half_toks, rows), 1)
    same_block = block_of(j_col) == iota((half_toks, rows), 0) >> shift_of(toks)
    take, tables = [], []
    for h in range(2):
        table = pick_z[h * hz : (h + 1) * hz].reshape(half_toks, LANES)
        table_hi = table.astype(jnp.bfloat16)
        table_lo = (table - table_hi.astype(jnp.float32)).astype(jnp.bfloat16)
        taken = (dot(codes[h], choose) == slot_of(j_col)) & same_block
        take.append(
            [
                jnp.where(taken, dot(k, choose), 0.0).astype(jnp.bfloat16)
                for k in (table_hi, table_lo)
            ]
        )
        tables.append(table[:, experts : experts + 1])

    backs = [sums_end(0, hidden0, sums0), sums_end(1, hidden1, sums1)]
    ready.dense_down()
    down = s.dense_down[...].reshape(hidden_here, quarter)
    dense_part = []
    for h in range(2):
        arrive(hidden_copies[h])
        value = hidden_x[h].astype(jnp.float32).reshape(nx, hz, own, hidden_here)
        value = value.swapaxes(0, 1).reshape(half_toks, hidden_here).astype(jnp.bfloat16)
        dense_part.append(dot(value, down) * tables[h])

    last_out, last_in = s.last_out, s.last_in
    last, parts = [], []

    def give_back(h):
        arrive(backs[h])
        results = back_in[h].reshape(rows, quarter)
        part = dot(take[h][0], results) + dot(take[h][1], results) + dense_part[h]
        last_out[h * hz : (h + 1) * hz] = part.astype(jnp.bfloat16).reshape(hz, toks, quarter)
        ks = others[h * hz : (h + 1) * hz]
        last.append(
            send(
                [(last_out.at[k], last_in.at[k], z_dev(nz - order[k])) for k in ks],
                last_in.at[pl.ds(0, len(ks))],
            )
        )
        return part

    give_back(0)
    combined = give_back(1)[(here - hz) * toks : (here - hz + 1) * toks]
    gain = in_row(ready.out_gain())
    arrive(stream_copies)
    stream_part = stream_in[...].astype(jnp.float32).reshape(toks, quarter)
    for h in range(2):
        arrive(last[h])
        for k in others[h * hz : (h + 1) * hz]:
            combined += last_in[k].astype(jnp.float32)

    square_x = s.square_x
    square = jnp.sum(combined * combined, axis=1, keepdims=True)
    on_lane = iota((toks, LANES), 0) == iota((toks, LANES), 1)
    as_row = jnp.sum(jnp.where(on_lane, square, 0.0), axis=0, keepdims=True)
    square_x[0] = jnp.broadcast_to(as_row, square_x.shape[1:])
    square_copies = send(
        [(square_x.at[0], square_x.at[r], x_dev(r)) for r in range(1, nx)],
        square_x.at[pl.ds(1, nx - 1)],
    )
    combined = combined * gain
    arrive(square_copies)
    all_rows = square_x[0]
    for r in range(1, nx):
        all_rows += square_x[r]
    total_square = jnp.sum(jnp.where(on_lane, all_rows[0:1], 0.0), axis=1, keepdims=True)
    scale = lax.rsqrt(total_square / width + norm_eps)
    layer_out[...] = (stream_part + combined * scale).astype(jnp.bfloat16)

    arrive(at_end)
    for copy in small_out:
        copy.wait()


def run_layer(sizes, p):
    nz, ny, nc, nx, cap = sizes
    np_ = ny * nc
    toks, width = p.resid.shape
    own, quarter = toks // nx, width // nx
    hz = nz // 2
    bf16, f32 = jnp.bfloat16, jnp.float32
    share = p.expert_gate.shape[2]
    hid = p.dense_gate.shape[0]
    channels = p.conv_state.shape[3]
    state_dim = p.scan_state.shape[3]

    def tall(a):
        return a.reshape(-1, LANES)

    g = SimpleNamespace(**vars(p))
    g.mix_gain, g.post_gain, g.ffn_gain = tall(p.mix_gain), tall(p.post_gain), tall(p.ffn_gain)
    g.dense_switch, g.inner_gain = tall(p.dense_switch), tall(p.inner_gain)
    g.out_gain = tall(p.out_gain)
    g.proj_step, g.expert_router = p.proj_step.T, p.expert_router.T
    g.group_router, g.route_experts = p.group_router.T, p.route_experts.T
    g.resid = p.resid.reshape(nx, own, width)
    g.conv_state = p.conv_state.transpose(1, 2, 0, 3)
    g.scan_state = p.scan_state.reshape(toks, channels, state_dim)
    g.step_bias, g.decay_rate = p.step_bias.reshape(1, -1), p.decay_rate.reshape(1, -1)
    g.expert_gate = p.expert_gate.reshape(nx, quarter, share)
    g.expert_up = p.expert_up.reshape(nx, quarter, share)
    g.expert_down = p.expert_down.reshape(share, width)
    names = tuple(vars(g))
    operands = list(vars(g).values())
    s = SimpleNamespace(**{k: pltpu.VMEM(v.shape, v.dtype) for k, v in vars(g).items()})
    s.dense_gate = s.dense_up = s.dense_down = pltpu.VMEM((np_, hid, quarter), bf16)
    s.expert_down = pltpu.VMEM((nx, share, quarter), bf16)
    s.proj_x = s.proj_b = s.proj_c = s.proj_z = pltpu.VMEM((8, LANES), f32)
    s.proj = pltpu.VMEM((width, 4 * channels), bf16)
    s.fresh = pltpu.VMEM((3, toks, channels), bf16)
    state_rows = (p.scan_state.shape[1] + 1, toks, channels)
    s.rows_ref = pltpu.VMEM(state_rows, f32)
    s.cols_ref = pltpu.VMEM((channels, channels), f32)
    s.c_ref = s.old_read = pltpu.VMEM((toks, channels), f32)
    s.mixed_f = pltpu.VMEM((nx, own, width), f32)
    s.mixed_b = pltpu.VMEM((nx, own, width), bf16)
    s.mixed_in = pltpu.VMEM((nx - 1, own, width), bf16)
    s.feed_out = s.feed_in = s.far_in = pltpu.VMEM((nx, own, quarter), bf16)
    s.stream_out = s.stream_in = pltpu.VMEM((nx, own, quarter), bf16)
    s.pick_in = pltpu.VMEM((nx, own, LANES), f32)
    s.pick_z = pltpu.VMEM((nz, toks, LANES), f32)
    s.code_z = pltpu.VMEM((nz, toks, LANES), bf16)
    s.feed_z = s.far_z = pltpu.VMEM((nz, toks, quarter), bf16)
    s.rows_out = s.rows_in = s.far_out = pltpu.VMEM((2, np_, hz * cap, quarter), bf16)
    s.back_out = s.back_in = pltpu.VMEM((2, np_, hz * cap, quarter), bf16)
    s.rows_x = pltpu.VMEM((2, 3, np_, hz * cap, quarter), bf16)
    s.pre_out = pltpu.VMEM((2, nx, hz * own, 2 * np_ * hid), bf16)
    s.pre_in = pltpu.VMEM((2, nx - 1, hz * own, 2 * np_ * hid), bf16)
    s.hidden_x = pltpu.VMEM((2, nx, hz * own, np_ * hid), bf16)
    s.sum_out = s.sum_in = pltpu.VMEM((2, 6, np_ * hz * cap // 2, quarter), bf16)
    s.last_out = pltpu.VMEM((nz, toks, quarter), bf16)
    s.last_in = pltpu.VMEM((nz, toks, quarter), bf16)
    s.square_x = pltpu.VMEM((nx, 8, LANES), f32)
    plan = names, tuple(vars(s))
    groups = 44
    shapes = [
        pltpu.SemaphoreType.DMA((groups,)),
        pltpu.SemaphoreType.DMA((groups + 2 * (np_ - 2),)),
        pltpu.SemaphoreType.DMA((len(names),)),
        *vars(s).values(),
    ]
    anyw = pl.BlockSpec(memory_space=pl.ANY)
    return pl.pallas_call(
        functools.partial(layer, sizes, plan),
        out_shape=(
            pltpu.VMEM((toks, quarter), bf16),
            pltpu.VMEM(state_rows, f32),
            pltpu.VMEM((channels, channels), f32),
            pltpu.VMEM((3, toks, channels), bf16),
        ),
        in_specs=[anyw] * len(operands),
        out_specs=(pl.BlockSpec(memory_space=pltpu.VMEM), anyw, anyw, anyw),
        scratch_shapes=shapes,
        compiler_params=pltpu.CompilerParams(
            collective_id=0, has_side_effects=True, vmem_limit_bytes=56 * 1024 * 1024
        ),
        name="layer",
    )(*operands)


def finish_step(
    rows, cols, fresh, conv, result, state, new_state, new_conv, layer_out, state_v, sem
):
    used = [0]

    def move(src, dst):
        copy = pltpu.make_async_copy(src, dst, sem.at[used[0]])
        used[0] += 1
        copy.start()
        return copy

    toks = state.shape[0]
    heads = rows.shape[0] - 1
    head_dim = cols.shape[0] // heads
    block = 4
    out = [
        move(result, layer_out),
        move(conv.at[:, pl.ds(1, 2)], new_conv.at[:, pl.ds(0, 2)]),
        move(fresh, new_conv.at[:, 2]),
    ]
    for i in range(0, toks, block):
        for t in range(i, i + block):
            new = slice(t, t + 1)
            for h in range(heads):
                part = slice(h * head_dim, (h + 1) * head_dim)
                added = cols[part, new] * rows[heads, new]
                state_v[t, part] = rows[h, new] * state[t, part] + added
        out.append(move(state_v.at[pl.ds(i, block)], new_state.at[pl.ds(i, block)]))
    for copy in out:
        copy.wait()


def finish(result, rows, cols, fresh, p):
    toks, heads, head_dim, state_dim = p.scan_state.shape
    channels = heads * head_dim
    conv = p.conv_state.transpose(1, 2, 0, 3)
    state = p.scan_state.reshape(toks, channels, state_dim)
    anyw = pl.BlockSpec(memory_space=pl.ANY)
    vmem = pl.BlockSpec(memory_space=pltpu.VMEM)
    new_state, new_conv, layer_out = pl.pallas_call(
        finish_step,
        out_shape=tuple(jax.ShapeDtypeStruct(a.shape, a.dtype) for a in (state, conv, result)),
        in_specs=[vmem] * 6,
        out_specs=(anyw,) * 3,
        scratch_shapes=[
            pltpu.VMEM(state.shape, state.dtype),
            pltpu.SemaphoreType.DMA((3 + toks // 4,)),
        ],
        compiler_params=pltpu.CompilerParams(vmem_limit_bytes=8 * 1024 * 1024),
        name="finish",
    )(rows, cols, fresh, conv, result, state)
    return (
        layer_out,
        new_state.reshape(p.scan_state.shape),
        new_conv.transpose(2, 0, 1, 3),
    )


def on_device(
    resid,
    mix_gain,
    proj_x,
    proj_z,
    proj_b,
    proj_c,
    proj_step,
    step_bias,
    decay_rate,
    conv_taps,
    conv_state,
    scan_state,
    inner_gain,
    proj_out,
    post_gain,
    ffn_gain,
    group_router,
    expert_router,
    route_experts,
    expert_gate,
    expert_up,
    expert_down,
    dense_switch,
    dense_gate,
    dense_up,
    dense_down,
    out_gain,
):
    params = SimpleNamespace(**locals())
    sizes = tuple(lax.axis_size(a) for a in EP) + (lax.axis_size("tp"), CAPACITY)
    return finish(*run_layer(sizes, params), params)


TORUS = (8, 4, 2)


def solution(mesh):
    torus = Mesh(mesh.devices.reshape(*TORUS, mesh.shape["tp"]), EP + ("tp",))
    in_specs = (
        P(EP, None),
        P(),
        P(None, "tp"),
        P(None, "tp"),
        P(None, "tp"),
        P(None, "tp"),
        P(),
        P("tp"),
        P("tp"),
        P(None, None, "tp"),
        P(EP, None, None, "tp"),
        P(EP, "tp", None, None),
        P("tp"),
        P("tp", None),
        P(),
        P(),
        P(),
        P(),
        P(EP, None),
        P(EP, None, "tp"),
        P(EP, None, "tp"),
        P(EP, "tp", None),
        P(),
        P(EP, "tp"),
        P(EP, "tp"),
        P(EP, "tp"),
        P("tp"),
    )
    out_specs = (P(EP, "tp"), P(EP, "tp", None, None), P(EP, None, None, "tp"))
    return jax.shard_map(
        on_device, mesh=torus, in_specs=in_specs, out_specs=out_specs, check_vma=False
    )
```

```python
import functools
from types import SimpleNamespace

import jax
import jax.numpy as jnp
from jax import lax
from jax.experimental import pallas as pl
from jax.experimental.pallas import tpu as pltpu
from jax.sharding import Mesh
from jax.sharding import PartitionSpec as P

EP = ("ep_0", "ep_1", "ep_2")
MESH = pl.DeviceIdType.MESH
norm_eps = 1e-06
CAPACITY = 4
LANES = 128


def dot(a, b):
    return jnp.dot(a, b, preferred_element_type=jnp.float32)


def dot_nt(a, b):
    return lax.dot_general(a, b, (((1,), (1,)), ((), ())), preferred_element_type=jnp.float32)


def in_row(gain_ref):
    gain = gain_ref[...].astype(jnp.float32)
    return jnp.concatenate([gain[i : i + 1] for i in range(gain.shape[0])], axis=1)


def iota(shape, dim):
    return lax.broadcasted_iota(jnp.int32, shape, dim)


def shift_of(count):
    return count.bit_length() - 1


def root_mean(values):
    return values * lax.rsqrt(jnp.mean(values * values, axis=-1, keepdims=True) + norm_eps)


def far_first(nz):
    return sorted(range(nz), key=lambda r: (-min(r, nz - r), r))


def layer(sizes, plan, *refs):
    nz, ny, nc, nx, cap = sizes
    np_ = ny * nc
    names, scratch = plan
    given = SimpleNamespace(**dict(zip(names, refs)))
    layer_out, state_rows, state_cols, fresh_out = refs[len(names) :][:4]
    send_sem, recv_sem, local_sem = refs[len(names) + 4 :][:3]
    s = SimpleNamespace(**dict(zip(scratch, refs[len(names) + 7 :])))
    z, y, c, x = (lax.axis_index(a) for a in ("ep_0", "ep_1", "ep_2", "tp"))
    place = y * nc + c
    own, width = given.resid.shape[1:]
    toks = own * nx
    quarter = width // nx
    hz = nz // 2
    half_toks = hz * toks
    chunk = hz * cap
    rows = np_ * chunk
    half = np_ // 2
    order = far_first(nz)
    here = order.index(0)
    others = [k for k in range(nz) if k != here]

    def z_dev(r):
        return {"ep_0": lax.rem(z + r, nz)}

    def p_dev(q):
        to = lax.rem(place + q, np_)
        return {"ep_1": to // nc, "ep_2": lax.rem(to, nc)}

    def x_dev(r):
        return {"tp": lax.rem(x + r, nx)}

    used = SimpleNamespace(send=0, recv=0)
    at_end = []

    def take_of(whole, sem):
        return lambda: pltpu.make_async_copy(whole, whole, sem).wait()

    class Group:
        def __init__(self, whole):
            self.out_sem, self.in_sem = send_sem.at[used.send], recv_sem.at[used.recv]
            used.send += 1
            used.recv += 1
            self.arrived = take_of(whole, self.in_sem)
            at_end.append(take_of(whole, self.out_sem))

        def start(self, src, dst, device, in_sem=None):
            pltpu.make_async_remote_copy(
                src_ref=src,
                dst_ref=dst,
                send_sem=self.out_sem,
                recv_sem=self.in_sem if in_sem is None else in_sem,
                device_id=device,
                device_id_type=MESH,
            ).start()

    def send(copies, whole, apart=False):
        if not copies:
            return []
        group = Group(whole)
        waits = []
        for k, (src, dst, device) in enumerate(copies):
            in_sem = group.in_sem
            if apart and k:
                in_sem = recv_sem.at[used.recv]
                used.recv += 1
            group.start(src, dst, device, in_sem)
            waits.append(take_of(dst, in_sem))
        return waits if apart else [group.arrived]

    local_used = [0]

    def fetch(src, dst, sem=None):
        if sem is None:
            sem = local_sem.at[local_used[0]]
            local_used[0] += 1
        copy = pltpu.make_async_copy(src, dst, sem)
        copy.start()
        return copy

    def arrive(waits):
        for wait in waits:
            wait()

    barrier = pltpu.get_barrier_semaphore()
    peers = (
        [x_dev(r) for r in range(1, nx)]
        + [p_dev(q) for q in range(1, np_)]
        + [z_dev(r) for r in range(1, nz)]
    )
    for device in peers:
        pl.semaphore_signal(barrier, inc=1, device_id=device, device_id_type=MESH)

    def bring(*pairs):
        coming = [fetch(src, dst) for src, dst in pairs]

        def get():
            while coming:
                coming.pop().wait()
            return pairs[0][1]

        return get

    g, ready = given, SimpleNamespace()
    ready.route_experts = bring((g.route_experts, s.route_experts))
    ready.resid = bring((g.resid, s.resid))
    ready.mix_gain = bring((g.mix_gain, s.mix_gain))
    wide = g.proj_x.shape[1]
    proj_sem = local_sem.at[local_used[0]]
    local_used[0] += 1
    for k, one in enumerate((g.proj_x, g.proj_b, g.proj_c, g.proj_z)):
        fetch(one, s.proj.at[:, pl.ds(k * wide, wide)], proj_sem)
    ready.proj_step = bring((g.proj_step, s.proj_step))
    ready.conv_taps = bring((g.conv_taps, s.conv_taps))
    ready.conv_state = bring((g.conv_state, s.conv_state))
    ready.step_bias = bring((g.step_bias, s.step_bias))
    ready.decay_rate = bring((g.decay_rate, s.decay_rate))
    ready.scan_state = bring((g.scan_state, s.scan_state))
    ready.inner_gain = bring((g.inner_gain, s.inner_gain))
    ready.proj_out = bring((g.proj_out, s.proj_out))
    ready.post_gain = bring((g.post_gain, s.post_gain))
    ready.ffn_gain = bring((g.ffn_gain, s.ffn_gain))
    ready.expert_router = bring((g.expert_router, s.expert_router))
    ready.group_router = bring((g.group_router, s.group_router))
    ready.dense_switch = bring((g.dense_switch, s.dense_switch))
    ready.out_gain = bring((g.out_gain, s.out_gain))
    ready.dense_gate = bring((g.dense_gate, s.dense_gate.at[0]))
    ready.dense_up = bring((g.dense_up, s.dense_up.at[0]))
    ready.dense_down = bring((g.dense_down, s.dense_down.at[0]))
    ready.expert_gate = bring((g.expert_gate, s.expert_gate))
    ready.expert_up = bring((g.expert_up, s.expert_up))
    down_sem = local_sem.at[local_used[0]]
    local_used[0] += 1
    for j in range(nx):
        fetch(g.expert_down.at[:, pl.ds(j * quarter, quarter)], s.expert_down.at[j], down_sem)

    route_t = ready.route_experts()[...]
    picks = route_t.shape[0]
    expert_ids = iota((LANES, toks), 0)
    named = jnp.zeros((LANES, toks), jnp.float32)
    for k in range(picks):
        named += jnp.where(expert_ids == route_t[k : k + 1, :], 1.0, 0.0)
    named_b = named.astype(jnp.bfloat16)
    before = jnp.where(iota((toks, toks), 0) < iota((toks, toks), 1), 1.0, 0.0).astype(jnp.bfloat16)
    code_t = (named * (dot(named_b, before) + 1.0)).astype(jnp.bfloat16)
    eye = jnp.where(iota((toks, toks), 0) == iota((toks, toks), 1), 1.0, 0.0).astype(jnp.bfloat16)
    code_z = s.code_z
    code_z[here] = dot_nt(eye, code_t).astype(jnp.bfloat16)

    resid = ready.resid()
    gain = in_row(ready.mix_gain())
    normed = root_mean(resid[...].astype(jnp.float32).reshape(toks, width)) * gain
    normed = normed.astype(jnp.bfloat16)
    take_of(s.proj, proj_sem)()
    projected = dot(normed, s.proj[...])
    step_all = dot_nt(normed, ready.proj_step()[...])
    taps = ready.conv_taps()[...].astype(jnp.float32)
    old_conv = ready.conv_state()
    channels = taps.shape[2]
    acts = []
    fresh_ref = s.fresh
    for k in range(3):
        fresh = projected[:, k * channels : (k + 1) * channels].astype(jnp.bfloat16)
        fresh_ref[k] = fresh
        mixed_in = fresh.astype(jnp.float32) * taps[k, 3:4]
        for i in range(3):
            mixed_in += old_conv[k, i].astype(jnp.float32) * taps[k, i : i + 1]
        acts.append(jax.nn.silu(mixed_in))
    xs, bs, cs = acts
    gate_z = projected[:, 3 * channels :]
    bias, rate = ready.step_bias()[...], ready.decay_rate()[...]
    heads_here = bias.shape[1]
    head_dim = channels // heads_here
    head_of = iota((toks, channels), 1) >> shift_of(head_dim)
    head_col = iota(step_all.shape, 1)
    step = jnp.zeros((toks, channels), jnp.float32)
    keep = jnp.zeros((toks, channels), jnp.float32)
    rows_ref = s.rows_ref
    for h in range(heads_here):
        raw = jnp.sum(
            jnp.where(head_col == x * heads_here + h, step_all, 0.0), axis=1, keepdims=True
        )
        one = jax.nn.softplus(raw + bias[:, h : h + 1])
        step = jnp.where(head_of == h, one, step)
        kept = jnp.exp(-rate[:, h : h + 1] * one)
        keep = jnp.where(head_of == h, kept, keep)
        rows_ref[h] = jnp.broadcast_to(kept, (toks, channels))
    driven = step * xs
    rows_ref[heads_here] = bs
    s.cols_ref[...] = jnp.concatenate([driven] * (channels // toks), axis=0).T
    small_out = [
        fetch(rows_ref, state_rows),
        fetch(s.cols_ref, state_cols),
        fetch(fresh_ref, fresh_out),
    ]
    c_ref, old_read = s.c_ref, s.old_read
    c_ref[...] = cs
    diag = iota((channels, channels), 0) == iota((channels, channels), 1)
    old_state = ready.scan_state()

    @pl.loop(0, toks // 8)
    def _(i):
        at = pl.multiple_of(i * 8, 8)
        c8 = c_ref[pl.ds(at, 8), :]
        out = []
        for t in range(8):
            sums = jnp.sum(old_state[at + t] * c8[t : t + 1], axis=1, keepdims=True)
            out.append(jnp.sum(jnp.where(diag, sums, 0.0), axis=0, keepdims=True))
        old_read[pl.ds(at, 8), :] = jnp.concatenate(out, axis=0)

    read = keep * old_read[...] + driven * jnp.sum(bs * cs, axis=1, keepdims=True)
    gated = (read * jax.nn.silu(gate_z) * in_row(ready.inner_gain())).astype(jnp.bfloat16)

    mixed_f, mixed_b, mixed_in = s.mixed_f, s.mixed_b, s.mixed_in
    share = dot(gated, ready.proj_out()[...]).reshape(nx, own, width)
    mixed_f[...] = share
    mixed_b[...] = share.astype(jnp.bfloat16)

    pl.semaphore_wait(barrier, len(peers))

    copies = send(
        [(mixed_b.at[lax.rem(x + r, nx)], mixed_in.at[r - 1], x_dev(r)) for r in range(1, nx)],
        mixed_in,
    )
    code_copies = send(
        [(code_z.at[here], code_z.at[k], z_dev(order[k])) for k in others],
        code_z.at[pl.ds(0, nz - 1)],
    )
    post_gain, ffn_gain = in_row(ready.post_gain()), in_row(ready.ffn_gain())
    resid_own = resid[x].astype(jnp.float32)
    arrive(copies)
    mixed = mixed_f[x]
    for r in range(1, nx):
        mixed += mixed_in[r - 1].astype(jnp.float32)
    stream = (resid_own + root_mean(mixed) * post_gain).astype(jnp.bfloat16)
    feed = (root_mean(stream.astype(jnp.float32)) * ffn_gain).astype(jnp.bfloat16)
    feed_out, feed_in = s.feed_out, s.feed_in
    stream_out, stream_in = s.stream_out, s.stream_in
    for j in range(nx):
        feed_out[j] = feed[:, j * quarter : (j + 1) * quarter]
    far = lax.rem(x + 2, nx)
    far_in = s.far_in
    feed_in[x] = feed_out[x]
    far_in[x] = feed_out[far]
    feed_copies = send(
        [(feed_out.at[lax.rem(x + r, nx)], feed_in.at[x], x_dev(r)) for r in range(1, nx)],
        feed_in.at[pl.ds(0, nx - 1)],
    )
    far_copies = send(
        [(feed_out.at[lax.rem(x + r + 2, nx)], far_in.at[x], x_dev(r)) for r in range(1, nx)],
        far_in.at[pl.ds(0, nx - 1)],
    )
    dense_copies = []
    for one, all_here in (
        (g.dense_gate, s.dense_gate),
        (g.dense_up, s.dense_up),
        (g.dense_down, s.dense_down),
    ):
        dense_copies += send(
            [(one, all_here.at[q], p_dev(q)) for q in range(1, np_)],
            all_here.at[pl.ds(1, np_ - 1)],
        )
    for j in range(nx):
        stream_out[j] = stream[:, j * quarter : (j + 1) * quarter]

    feed_f = feed.astype(jnp.float32)
    expert_rows, group_rows = ready.expert_router(), ready.group_router()
    experts = expert_rows.shape[0]
    groups = group_rows.shape[0]
    group_size = experts // groups
    token_pick = jnp.where(iota((own, toks), 1) == iota((own, toks), 0) + x * own, 1.0, 0.0)
    own_route = dot_nt(token_pick.astype(jnp.bfloat16), route_t.astype(jnp.bfloat16))
    logits = dot_nt(feed, expert_rows[...])
    lanes = iota((own, experts), 1).astype(jnp.float32)
    weights = []
    for k in range(picks):
        chosen = jnp.sum(
            jnp.where(lanes == own_route[:, k : k + 1], logits, 0.0), axis=1, keepdims=True
        )
        weights.append(jnp.exp(chosen))
    total = functools.reduce(jnp.add, weights)
    group_f = group_rows[...].astype(jnp.float32)
    group_exp = [
        jnp.exp(jnp.sum(feed_f * group_f[g : g + 1], axis=1, keepdims=True)) for g in range(groups)
    ]
    group_total = functools.reduce(jnp.add, group_exp)
    first = own_route[:, 0:1]
    group_weight = jnp.zeros((own, 1), jnp.float32)
    for g in range(groups):
        in_group = (first >= g * group_size) & (first < (g + 1) * group_size)
        group_weight += jnp.where(in_group, group_exp[g] / group_total, 0.0)
    switch_row = in_row(ready.dense_switch())
    switch = jax.nn.sigmoid(jnp.sum(feed_f * switch_row, axis=1, keepdims=True))
    all_lanes = iota((own, LANES), 1).astype(jnp.float32)
    pick_table = jnp.where(all_lanes < experts, 0.0, switch)
    for k in range(picks):
        pick_table += jnp.where(
            all_lanes == own_route[:, k : k + 1], weights[k] / total * group_weight, 0.0
        )
    pick_in, pick_z = s.pick_in, s.pick_z
    pick_in[x] = pick_table

    arrive(feed_copies)
    feed_z, far_z = s.feed_z, s.far_z
    feed_z[here] = feed_in[...].astype(jnp.float32).reshape(toks, quarter).astype(jnp.bfloat16)

    def to_z(ref, ks):
        return send(
            [(ref.at[here], ref.at[k], z_dev(order[k])) for k in ks], ref.at[pl.ds(0, len(ks))]
        )

    feed_copies = [to_z(feed_z, others[:hz]), to_z(feed_z, others[hz:])]
    arrive(far_copies)
    far_z[here] = far_in[...].astype(jnp.float32).reshape(toks, quarter).astype(jnp.bfloat16)
    far_copies = to_z(far_z, others)
    pick_copies = send(
        [(pick_in.at[x], pick_in.at[x], x_dev(r)) for r in range(1, nx)],
        pick_in.at[pl.ds(0, nx - 1)],
    )
    stream_in[x] = stream_out[x]
    stream_copies = send(
        [(stream_out.at[lax.rem(x + r, nx)], stream_in.at[x], x_dev(r)) for r in range(1, nx)],
        stream_in.at[pl.ds(0, nx - 1)],
    )

    def expert_of(j):
        return z * np_ + ((place + (j >> shift_of(chunk))) & (np_ - 1))

    def block_of(j):
        return (j & (chunk - 1)) >> shift_of(cap)

    def slot_of(j):
        return ((j & (cap - 1)) + 1).astype(jnp.float32)

    arrive(code_copies)
    codes = [
        code_z[h * hz : (h + 1) * hz].reshape(half_toks, LANES) for h in range(2)
    ]
    choose_t = jnp.where(
        iota((rows, LANES), 1) == expert_of(iota((rows, LANES), 0)), 1.0, 0.0
    ).astype(jnp.bfloat16)
    choose = jnp.where(
        iota((LANES, rows), 0) == expert_of(iota((LANES, rows), 1)), 1.0, 0.0
    ).astype(jnp.bfloat16)
    j_row = iota((rows, half_toks), 0)
    same_block = block_of(j_row) == iota((rows, half_toks), 1) >> shift_of(toks)
    put = [
        jnp.where((dot_nt(choose_t, k) == slot_of(j_row)) & same_block, 1.0, 0.0).astype(
            jnp.bfloat16
        )
        for k in codes
    ]

    arrive(pick_copies)
    pick_z[here] = pick_in[...].reshape(toks, LANES)
    pick_copies = to_z(pick_z, others)

    rows_out, rows_in, rows_x = s.rows_out, s.rows_in, s.rows_x
    far_out = s.far_out
    pre_out, pre_in, hidden_x = s.pre_out, s.pre_in, s.hidden_x
    hidden_here = s.dense_gate.shape[0] * s.dense_gate.shape[1]
    row_copies, pre_copies = [], []
    to_right, to_left = x_dev(1), x_dev(nx - 1)
    from_left, from_right, from_far = [], [], []

    def rows_to_experts(h):
        arrive(feed_copies[h])
        feeds = feed_z[h * hz : (h + 1) * hz].reshape(half_toks, quarter)
        rows_out[h] = dot(put[h], feeds).astype(jnp.bfloat16).reshape(np_, chunk, quarter)
        rows_in[h, 0] = rows_out[h, 0]
        row_copies.append(
            send(
                [(rows_out.at[h, q], rows_in.at[h, q], p_dev(q)) for q in range(1, np_)],
                rows_in.at[h, pl.ds(1, np_ - 1)],
                apart=True,
            )
        )
        return feeds

    def far_to_experts(h):
        feeds = far_z[h * hz : (h + 1) * hz].reshape(half_toks, quarter)
        value = dot(put[h], feeds).astype(jnp.bfloat16).reshape(np_, chunk, quarter)
        far_out[h] = value
        rows_x[h, 2, 0] = far_out[h, 0]
        from_far.append(
            send(
                [(far_out.at[h, q], rows_x.at[h, 2, q], p_dev(q)) for q in range(1, np_)],
                rows_x.at[h, 2, pl.ds(1, np_ - 1)],
            )
        )

    def dense_sums(h, feeds):
        ready.dense_gate()
        ready.dense_up()
        for k, weight in enumerate((s.dense_gate, s.dense_up)):
            part = dot_nt(feeds, weight[...].reshape(hidden_here, quarter))
            part = part.reshape(hz, nx, own, hidden_here).swapaxes(0, 1)
            part = part.reshape(nx, hz * own, hidden_here).astype(jnp.bfloat16)
            pre_out[h, :, :, k * hidden_here : (k + 1) * hidden_here] = part
        pre_copies.append(
            send(
                [
                    (pre_out.at[h, lax.rem(x + r, nx)], pre_in.at[h, r - 1], x_dev(r))
                    for r in range(1, nx)
                ],
                pre_in.at[h],
            )
        )

    def rows_over_x(h):
        right_group = Group(rows_x.at[h, 0])
        left_group = Group(rows_x.at[h, 1])
        for q in range(np_):
            if q:
                row_copies[h][q - 1]()
            right_group.start(rows_in.at[h, q], rows_x.at[h, 0, q], to_right)
            left_group.start(rows_in.at[h, q], rows_x.at[h, 1, q], to_left)
        from_left.append([right_group.arrived])
        from_right.append([left_group.arrived])

    w_gate, w_up, w_down = s.expert_gate, s.expert_up, s.expert_down

    def of_share(taken, share):
        taken = taken.reshape(rows, quarter)
        return dot(taken, w_gate[share]), dot(taken, w_up[share])

    right, left = lax.rem(x + 1, nx), lax.rem(x + nx - 1, nx)

    def expert_hidden(h):
        gate_value, up_value = of_share(rows_in[h], x)
        arrive(from_left[h])
        more = of_share(rows_x[h, 0], left)
        gate_value, up_value = gate_value + more[0], up_value + more[1]
        arrive(from_right[h])
        more = of_share(rows_x[h, 1], right)
        gate_value, up_value = gate_value + more[0], up_value + more[1]
        arrive(from_far[h])
        more = of_share(rows_x[h, 2], far)
        gate_value, up_value = gate_value + more[0], up_value + more[1]
        return (jax.nn.silu(gate_value) * up_value).astype(jnp.bfloat16)

    sum_out, sum_in = s.sum_out, s.sum_in
    cut = rows // 2

    def put_out(h, k, values, device):
        sum_out[h, k] = values.astype(jnp.bfloat16)
        return send([(sum_out.at[h, k], sum_in.at[h, k], device)], sum_in.at[h, k])

    def sums_start(h, hidden):
        low, high = hidden[:cut], hidden[cut:]
        return [
            put_out(h, 0, dot(low, w_down[far]), to_right),
            put_out(h, 1, dot(high, w_down[far]), to_left),
            put_out(h, 2, dot(high, w_down[right]), to_right),
            put_out(h, 3, dot(low, w_down[left]), to_left),
        ]

    def sums_pass_on(h, hidden, sums):
        low, high = hidden[:cut], hidden[cut:]
        value = dot(low, w_down[right])
        arrive(sums[0])
        sums.append(put_out(h, 4, value + sum_in[h, 0].astype(jnp.float32), to_right))
        value = dot(high, w_down[left])
        arrive(sums[1])
        sums.append(put_out(h, 5, value + sum_in[h, 1].astype(jnp.float32), to_left))

    back_out, back_in = s.back_out, s.back_in

    def sums_end(h, hidden, sums):
        done = dot(hidden, w_down[x])
        for k, (a, b) in enumerate(((3, 4), (2, 5))):
            arrive(sums[a] + sums[b])
            total = done[k * cut : (k + 1) * cut]
            total += sum_in[h, a].astype(jnp.float32) + sum_in[h, b].astype(jnp.float32)
            back_out[h, k * half : (k + 1) * half] = total.astype(jnp.bfloat16).reshape(
                half, chunk, quarter
            )
        back_in[h, 0] = back_out[h, 0]
        return send(
            [(back_out.at[h, q], back_in.at[h, q], p_dev(np_ - q)) for q in range(1, np_)],
            back_in.at[h, pl.ds(1, np_ - 1)],
        )

    def dense_hidden(h):
        arrive(pre_copies[h])
        pre = pre_out[h, x].astype(jnp.float32)
        for r in range(1, nx):
            pre += pre_in[h, r - 1].astype(jnp.float32)
        value = jax.nn.silu(pre[:, :hidden_here]) * pre[:, hidden_here:]
        hidden_x[h, x] = value.astype(jnp.bfloat16)
        return send(
            [(hidden_x.at[h, x], hidden_x.at[h, x], x_dev(r)) for r in range(1, nx)],
            hidden_x.at[h, pl.ds(0, nx - 1)],
        )

    feeds = rows_to_experts(0)
    arrive(dense_copies)
    dense_sums(0, feeds)
    feeds = rows_to_experts(1)
    dense_sums(1, feeds)
    rows_over_x(0)
    arrive(far_copies)
    far_to_experts(0)
    far_to_experts(1)
    rows_over_x(1)
    ready.expert_gate()
    ready.expert_up()
    take_of(s.expert_down, down_sem)()
    hidden0 = expert_hidden(0)
    sums0 = sums_start(0, hidden0)
    hidden1 = expert_hidden(1)
    sums1 = sums_start(1, hidden1)
    sums_pass_on(0, hidden0, sums0)
    sums_pass_on(1, hidden1, sums1)
    hidden_copies = [dense_hidden(0), dense_hidden(1)]
    arrive(pick_copies)
    j_col = iota((half_toks, rows), 1)
    same_block = block_of(j_col) == iota((half_toks, rows), 0) >> shift_of(toks)
    take, tables = [], []
    for h in range(2):
        table = pick_z[h * hz : (h + 1) * hz].reshape(half_toks, LANES)
        table_hi = table.astype(jnp.bfloat16)
        table_lo = (table - table_hi.astype(jnp.float32)).astype(jnp.bfloat16)
        taken = (dot(codes[h], choose) == slot_of(j_col)) & same_block
        take.append(
            [
                jnp.where(taken, dot(k, choose), 0.0).astype(jnp.bfloat16)
                for k in (table_hi, table_lo)
            ]
        )
        tables.append(table[:, experts : experts + 1])

    backs = [sums_end(0, hidden0, sums0), sums_end(1, hidden1, sums1)]
    ready.dense_down()
    down = s.dense_down[...].reshape(hidden_here, quarter)
    dense_part = []
    for h in range(2):
        arrive(hidden_copies[h])
        value = hidden_x[h].astype(jnp.float32).reshape(nx, hz, own, hidden_here)
        value = value.swapaxes(0, 1).reshape(half_toks, hidden_here).astype(jnp.bfloat16)
        dense_part.append(dot(value, down) * tables[h])

    last_out, last_in = s.last_out, s.last_in
    last, parts = [], []

    def give_back(h):
        arrive(backs[h])
        results = back_in[h].reshape(rows, quarter)
        part = dot(take[h][0], results) + dot(take[h][1], results) + dense_part[h]
        last_out[h * hz : (h + 1) * hz] = part.astype(jnp.bfloat16).reshape(hz, toks, quarter)
        ks = others[h * hz : (h + 1) * hz]
        last.append(
            send(
                [(last_out.at[k], last_in.at[k], z_dev(nz - order[k])) for k in ks],
                last_in.at[pl.ds(0, len(ks))],
            )
        )
        return part

    give_back(0)
    combined = give_back(1)[(here - hz) * toks : (here - hz + 1) * toks]
    gain = in_row(ready.out_gain())
    arrive(stream_copies)
    stream_part = stream_in[...].astype(jnp.float32).reshape(toks, quarter)
    for h in range(2):
        arrive(last[h])
        for k in others[h * hz : (h + 1) * hz]:
            combined += last_in[k].astype(jnp.float32)

    square_x = s.square_x
    square = jnp.sum(combined * combined, axis=1, keepdims=True)
    on_lane = iota((toks, LANES), 0) == iota((toks, LANES), 1)
    as_row = jnp.sum(jnp.where(on_lane, square, 0.0), axis=0, keepdims=True)
    square_x[0] = jnp.broadcast_to(as_row, square_x.shape[1:])
    square_copies = send(
        [(square_x.at[0], square_x.at[r], x_dev(r)) for r in range(1, nx)],
        square_x.at[pl.ds(1, nx - 1)],
    )
    combined = combined * gain
    arrive(square_copies)
    all_rows = square_x[0]
    for r in range(1, nx):
        all_rows += square_x[r]
    total_square = jnp.sum(jnp.where(on_lane, all_rows[0:1], 0.0), axis=1, keepdims=True)
    scale = lax.rsqrt(total_square / width + norm_eps)
    layer_out[...] = (stream_part + combined * scale).astype(jnp.bfloat16)

    arrive(at_end)
    for copy in small_out:
        copy.wait()


def run_layer(sizes, p):
    nz, ny, nc, nx, cap = sizes
    np_ = ny * nc
    toks, width = p.resid.shape
    own, quarter = toks // nx, width // nx
    hz = nz // 2
    bf16, f32 = jnp.bfloat16, jnp.float32
    share = p.expert_gate.shape[2]
    hid = p.dense_gate.shape[0]
    channels = p.conv_state.shape[3]
    state_dim = p.scan_state.shape[3]

    def tall(a):
        return a.reshape(-1, LANES)

    g = SimpleNamespace(**vars(p))
    g.mix_gain, g.post_gain, g.ffn_gain = tall(p.mix_gain), tall(p.post_gain), tall(p.ffn_gain)
    g.dense_switch, g.inner_gain = tall(p.dense_switch), tall(p.inner_gain)
    g.out_gain = tall(p.out_gain)
    g.proj_step, g.expert_router = p.proj_step.T, p.expert_router.T
    g.group_router, g.route_experts = p.group_router.T, p.route_experts.T
    g.resid = p.resid.reshape(nx, own, width)
    g.conv_state = p.conv_state.transpose(1, 2, 0, 3)
    g.scan_state = p.scan_state.reshape(toks, channels, state_dim)
    g.step_bias, g.decay_rate = p.step_bias.reshape(1, -1), p.decay_rate.reshape(1, -1)
    g.expert_gate = p.expert_gate.reshape(nx, quarter, share)
    g.expert_up = p.expert_up.reshape(nx, quarter, share)
    g.expert_down = p.expert_down.reshape(share, width)
    names = tuple(vars(g))
    operands = list(vars(g).values())
    s = SimpleNamespace(**{k: pltpu.VMEM(v.shape, v.dtype) for k, v in vars(g).items()})
    s.dense_gate = s.dense_up = s.dense_down = pltpu.VMEM((np_, hid, quarter), bf16)
    s.expert_down = pltpu.VMEM((nx, share, quarter), bf16)
    s.proj_x = s.proj_b = s.proj_c = s.proj_z = pltpu.VMEM((8, LANES), f32)
    s.proj = pltpu.VMEM((width, 4 * channels), bf16)
    s.fresh = pltpu.VMEM((3, toks, channels), bf16)
    state_rows = (p.scan_state.shape[1] + 1, toks, channels)
    s.rows_ref = pltpu.VMEM(state_rows, f32)
    s.cols_ref = pltpu.VMEM((channels, channels), f32)
    s.c_ref = s.old_read = pltpu.VMEM((toks, channels), f32)
    s.mixed_f = pltpu.VMEM((nx, own, width), f32)
    s.mixed_b = pltpu.VMEM((nx, own, width), bf16)
    s.mixed_in = pltpu.VMEM((nx - 1, own, width), bf16)
    s.feed_out = s.feed_in = s.far_in = pltpu.VMEM((nx, own, quarter), bf16)
    s.stream_out = s.stream_in = pltpu.VMEM((nx, own, quarter), bf16)
    s.pick_in = pltpu.VMEM((nx, own, LANES), f32)
    s.pick_z = pltpu.VMEM((nz, toks, LANES), f32)
    s.code_z = pltpu.VMEM((nz, toks, LANES), bf16)
    s.feed_z = s.far_z = pltpu.VMEM((nz, toks, quarter), bf16)
    s.rows_out = s.rows_in = s.far_out = pltpu.VMEM((2, np_, hz * cap, quarter), bf16)
    s.back_out = s.back_in = pltpu.VMEM((2, np_, hz * cap, quarter), bf16)
    s.rows_x = pltpu.VMEM((2, 3, np_, hz * cap, quarter), bf16)
    s.pre_out = pltpu.VMEM((2, nx, hz * own, 2 * np_ * hid), bf16)
    s.pre_in = pltpu.VMEM((2, nx - 1, hz * own, 2 * np_ * hid), bf16)
    s.hidden_x = pltpu.VMEM((2, nx, hz * own, np_ * hid), bf16)
    s.sum_out = s.sum_in = pltpu.VMEM((2, 6, np_ * hz * cap // 2, quarter), bf16)
    s.last_out = pltpu.VMEM((nz, toks, quarter), bf16)
    s.last_in = pltpu.VMEM((nz, toks, quarter), bf16)
    s.square_x = pltpu.VMEM((nx, 8, LANES), f32)
    plan = names, tuple(vars(s))
    groups = 44
    shapes = [
        pltpu.SemaphoreType.DMA((groups,)),
        pltpu.SemaphoreType.DMA((groups + 2 * (np_ - 2),)),
        pltpu.SemaphoreType.DMA((len(names),)),
        *vars(s).values(),
    ]
    anyw = pl.BlockSpec(memory_space=pl.ANY)
    return pl.pallas_call(
        functools.partial(layer, sizes, plan),
        out_shape=(
            pltpu.VMEM((toks, quarter), bf16),
            pltpu.VMEM(state_rows, f32),
            pltpu.VMEM((channels, channels), f32),
            pltpu.VMEM((3, toks, channels), bf16),
        ),
        in_specs=[anyw] * len(operands),
        out_specs=(pl.BlockSpec(memory_space=pltpu.VMEM), anyw, anyw, anyw),
        scratch_shapes=shapes,
        compiler_params=pltpu.CompilerParams(
            collective_id=0, has_side_effects=True, vmem_limit_bytes=56 * 1024 * 1024
        ),
        name="layer",
    )(*operands)


def finish_step(
    rows, cols, fresh, conv, result, state, new_state, new_conv, layer_out, state_v, sem
):
    used = [0]

    def move(src, dst):
        copy = pltpu.make_async_copy(src, dst, sem.at[used[0]])
        used[0] += 1
        copy.start()
        return copy

    toks = state.shape[0]
    heads = rows.shape[0] - 1
    head_dim = cols.shape[0] // heads
    block = 4
    out = [
        move(result, layer_out),
        move(conv.at[:, pl.ds(1, 2)], new_conv.at[:, pl.ds(0, 2)]),
        move(fresh, new_conv.at[:, 2]),
    ]
    for i in range(0, toks, block):
        for t in range(i, i + block):
            new = slice(t, t + 1)
            for h in range(heads):
                part = slice(h * head_dim, (h + 1) * head_dim)
                added = cols[part, new] * rows[heads, new]
                state_v[t, part] = rows[h, new] * state[t, part] + added
        out.append(move(state_v.at[pl.ds(i, block)], new_state.at[pl.ds(i, block)]))
    for copy in out:
        copy.wait()


def finish(result, rows, cols, fresh, p):
    toks, heads, head_dim, state_dim = p.scan_state.shape
    channels = heads * head_dim
    conv = p.conv_state.transpose(1, 2, 0, 3)
    state = p.scan_state.reshape(toks, channels, state_dim)
    anyw = pl.BlockSpec(memory_space=pl.ANY)
    vmem = pl.BlockSpec(memory_space=pltpu.VMEM)
    new_state, new_conv, layer_out = pl.pallas_call(
        finish_step,
        out_shape=tuple(jax.ShapeDtypeStruct(a.shape, a.dtype) for a in (state, conv, result)),
        in_specs=[vmem] * 6,
        out_specs=(anyw,) * 3,
        scratch_shapes=[
            pltpu.VMEM(state.shape, state.dtype),
            pltpu.SemaphoreType.DMA((3 + toks // 4,)),
        ],
        compiler_params=pltpu.CompilerParams(vmem_limit_bytes=8 * 1024 * 1024),
        name="finish",
    )(rows, cols, fresh, conv, result, state)
    return (
        layer_out,
        new_state.reshape(p.scan_state.shape),
        new_conv.transpose(2, 0, 1, 3),
    )


def on_device(
    resid,
    mix_gain,
    proj_x,
    proj_z,
    proj_b,
    proj_c,
    proj_step,
    step_bias,
    decay_rate,
    conv_taps,
    conv_state,
    scan_state,
    inner_gain,
    proj_out,
    post_gain,
    ffn_gain,
    group_router,
    expert_router,
    route_experts,
    expert_gate,
    expert_up,
    expert_down,
    dense_switch,
    dense_gate,
    dense_up,
    dense_down,
    out_gain,
):
    params = SimpleNamespace(**locals())
    sizes = tuple(lax.axis_size(a) for a in EP) + (lax.axis_size("tp"), CAPACITY)
    return finish(*run_layer(sizes, params), params)


TORUS = (8, 4, 2)


def solution(mesh):
    torus = Mesh(mesh.devices.reshape(*TORUS, mesh.shape["tp"]), EP + ("tp",))
    in_specs = (
        P(EP, None),
        P(),
        P(None, "tp"),
        P(None, "tp"),
        P(None, "tp"),
        P(None, "tp"),
        P(),
        P("tp"),
        P("tp"),
        P(None, None, "tp"),
        P(EP, None, None, "tp"),
        P(EP, "tp", None, None),
        P("tp"),
        P("tp", None),
        P(),
        P(),
        P(),
        P(),
        P(EP, None),
        P(EP, None, "tp"),
        P(EP, None, "tp"),
        P(EP, "tp", None),
        P(),
        P(EP, "tp"),
        P(EP, "tp"),
        P(EP, "tp"),
        P("tp"),
    )
    out_specs = (P(EP, "tp"), P(EP, "tp", None, None), P(EP, None, None, "tp"))
    return jax.shard_map(
        on_device, mesh=torus, in_specs=in_specs, out_specs=out_specs, check_vma=False
    )
```
